32 devices in a mesh: sp: 8 (over z, x), tp: 4 (over y, core).
Axes of the slice: x: 2, y: 2, z: 4, core: 2. Of those that a mesh axis runs over, the one named last changes fastest.
Arguments:
- queries: bfloat16 [1024, 2048], P('sp', 'tp'), may hold values from -18 to 90
- projected_key_rows: bfloat16 [1024, 1024], P('sp', 'tp'), may hold values from -18 to 90
- projected_value_rows: bfloat16 [1024, 1024], P('sp', 'tp'), may hold values from -6 to 6
- query_gain: float32 [64], replicated, may hold values from 1 to 6
- key_norm_gain: float32 [64], replicated, may hold values from 1 to 6
- residual: bfloat16 [1024, 2048], P('sp', 'tp'), may hold values from -54 to 54
- out_weight: bfloat16 [2048, 2048], P('tp'), may hold values from -1 to 1
- norm_gain: float32 [2048], P('tp'), may hold values from 0.28 to 4.68
- expert_ids: int32 [1024, 2], P('sp'), may hold values from 0 to 7, as said below
- route_weights: float32 [1024, 2], P('sp'), may hold values from 0.2 to 1
- gate_weight: bfloat16 [8, 2048, 4096], P('sp', None, 'tp'), may hold values from -0.125 to 0.125
- up_weight: bfloat16 [8, 2048, 4096], P('sp', None, 'tp'), may hold values from -0.125 to 0.125
- down_weight: bfloat16 [8, 4096, 2048], P('sp', 'tp'), may hold values from -0.25 to 0.25
- final_gain: float32 [2048], P('tp'), may hold values from 0.1 to 1.9
Outputs:
- layer_out: bfloat16 [1024, 2048], P('sp', 'tp')
The draws below stay inside these ranges and needn't reach their ends.
Inputs may be any that keep to these rules, and one draw needn't show every extreme that they name: `expert_ids`: each row names two different experts of one group, the group of expert e being e // 4. In every aligned block of 128 rows each group is named by the same number of rows, no expert is named by more than 64 rows, one expert of every group is named by exactly 64 rows, and one expert is named by 64 rows of every block.
All inputs are finite; a program needn't handle non-finite values.
Results may differ from the reference program's by a relative error of at most 0.019.
The reference program's roundings to bfloat16 on the way count: a program that leaves them out, or rounds other values in their place, can miss the bound.
Values may be sent and summed in bfloat16 or wider, within the bound.
A program may use at most 64 MiB of HBM per device.

```python
import jax
import jax.numpy as jnp
from jax import lax

D = 2048
QUERY_HEAD_COUNT = 32
KEY_VALUE_HEADS = 16
HEAD_DIM = 64
GRID_W = 64
FFE = 4096
EXP_GROUP = 4
TOPK = 2
TOK_SP = 128
SEQUENCE_TOKENS = 1024
EXPERTS = 8
CAP = 64
UNIT_BLOCKS = 4


def draw_rows_by_head(key, head_count):
    normal_part = jnp.clip(jax.random.normal(jax.random.fold_in(key, 1), (SEQUENCE_TOKENS, head_count, HEAD_DIM), jnp.float32), -6.0, 6.0)
    return normal_part.reshape(SEQUENCE_TOKENS, head_count * HEAD_DIM)


def draw_queries(key, part):
    return draw_rows_by_head(jax.random.fold_in(key, 101), QUERY_HEAD_COUNT).astype(jnp.bfloat16)


def draw_projected_key_rows(key, part):
    return draw_rows_by_head(jax.random.fold_in(key, 102), KEY_VALUE_HEADS).astype(jnp.bfloat16)


def draw_gain_row(key):
    base_gain = jax.random.uniform(jax.random.fold_in(key, 1), (HEAD_DIM,), jnp.float32, 1.0, 1.8)
    return base_gain


def draw_query_gain(key, part):
    return draw_gain_row(jax.random.fold_in(key, 103))


def draw_key_norm_gain(key, part):
    return draw_gain_row(jax.random.fold_in(key, 104))


def draw_residual(key, part):
    normal_part = jnp.clip(jax.random.normal(jax.random.fold_in(key, 105), (SEQUENCE_TOKENS, D), jnp.float32), -6.0, 6.0)
    columns = jnp.arange(D, dtype=jnp.float32) / D
    return (normal_part * 0.5 * 3.0 ** columns[None, :]).astype(jnp.bfloat16)


def draw_norm_gain(key, part):
    base_gain = jax.random.uniform(jax.random.fold_in(key, 107), (D,), jnp.float32, 0.7, 1.3)
    columns = jnp.arange(D, dtype=jnp.float32) / D
    return base_gain * 0.6 * 3.0 ** columns


def draw_expert_ids(key, part):
    block_count = SEQUENCE_TOKENS // TOK_SP
    group_count = EXPERTS // EXP_GROUP
    group_rows = TOK_SP // group_count
    mean_load = 2 * group_rows // EXP_GROUP
    hot_first = jax.random.randint(jax.random.fold_in(key, 21), (), 0, EXP_GROUP)
    lane_index = jnp.arange(EXP_GROUP, dtype=jnp.int32)
    list_index = jnp.arange(2 * group_rows, dtype=jnp.int32)

    def one_group(group_key, group_number):
        heights = jax.random.randint(group_key, (EXP_GROUP,), 0, mean_load + 1)
        peak_at = jax.random.randint(jax.random.fold_in(group_key, 1), (), 0, EXP_GROUP)
        peak_at = jnp.where(group_number == 0, hot_first, peak_at)
        heights = jnp.where(lane_index == peak_at, mean_load, heights)
        heights = jnp.where(lane_index == (peak_at + EXP_GROUP - 1) % EXP_GROUP, 0, heights)
        loads = mean_load + heights - jnp.roll(heights, 1)
        ends = jnp.cumsum(loads)
        listing = jnp.sum((ends[None, :] <= list_index[:, None]).astype(jnp.int32), 1)
        return jnp.stack([listing[:group_rows], listing[group_rows:]], 1) + group_number * EXP_GROUP

    def one_block(block_key):
        group_keys = jax.random.split(block_key, group_count)
        pairs = jax.vmap(one_group)(group_keys, jnp.arange(group_count, dtype=jnp.int32)).reshape(TOK_SP, TOPK)
        order = jax.random.permutation(jax.random.fold_in(block_key, 7), TOK_SP)
        pairs = pairs[order]
        flipped = jax.random.randint(jax.random.fold_in(block_key, 8), (TOK_SP, 1), 0, 2)
        return jnp.where(flipped == 1, pairs[:, ::-1], pairs)
    block_keys = jax.random.split(jax.random.fold_in(key, 20), block_count)
    return jax.vmap(one_block)(block_keys).reshape(SEQUENCE_TOKENS, TOPK).astype(jnp.int32)


def raised(array, own_key, source, target, shards_of, factor):
    owner, partner = [(jnp.arange(array.shape[axis_at]) // (array.shape[axis_at] // shards_of)).reshape([-1 if axis == axis_at else 1 for axis in range(array.ndim)]) for axis_at in (source, target)]
    chosen = jax.random.permutation(own_key, shards_of)[partner]
    strong = (owner == chosen) | (owner == (partner + shards_of // 2) % shards_of)
    return jnp.where(strong, factor * array, array)


def levels(stream_key, extent, cuts, low, top_value):
    gain, own = 1.0, jax.random.fold_in(stream_key, 6)
    for axis_at, shards_of in cuts:
        steps = jnp.exp(jax.random.uniform(jax.random.fold_in(own, axis_at), (shards_of,), jnp.float32, low / len(cuts), top_value / len(cuts)))
        gain = gain * jnp.repeat(steps, extent[axis_at] // shards_of).reshape([-1 if axis == axis_at else 1 for axis in range(len(extent))])
    return gain


def normal_values(own_key, shape, width, most, cuts=(), kind=jnp.bfloat16):
    array = jax.random.normal(own_key, shape, jnp.float32) * width
    if len(cuts) > 0:
        array = levels(own_key, shape, cuts, -0.22, 0.18) * array
    return jnp.clip(array, min=-most, max=most).astype(kind)


def gaussian_with(own_key, dims, deviation, bound, shards, heavy, kind=jnp.bfloat16):
    entries = deviation * jax.random.normal(own_key, dims, jnp.float32)
    if shards:
        entries = entries * levels(own_key, dims, shards, -0.22, 0.18)
    return jnp.clip(raised(entries, jax.random.fold_in(own_key, 3), *heavy), -bound, bound).astype(kind)


def setup_inputs(seed: int = 0) -> dict:
    key_of = jax.random.split(jax.random.key(seed), 15)
    queries = draw_queries(jax.random.fold_in(key_of[14], 71), 0)
    projected_key_rows = draw_projected_key_rows(jax.random.fold_in(key_of[14], 71), 0)
    projected_value_rows = normal_values(key_of[2], (SEQUENCE_TOKENS, KEY_VALUE_HEADS * HEAD_DIM), 1.0, 6.0, ((0, 8), (1, 4)))
    query_gain = draw_query_gain(jax.random.fold_in(key_of[14], 71), 0)
    key_norm_gain = draw_key_norm_gain(jax.random.fold_in(key_of[14], 71), 0)
    residual = draw_residual(jax.random.fold_in(key_of[14], 71), 0)
    out_weight = gaussian_with(key_of[6], (QUERY_HEAD_COUNT * HEAD_DIM, D), (QUERY_HEAD_COUNT * HEAD_DIM // 32) ** -0.5, 1.0, ((0, 4),), (0, 1, 4, 2.0))
    norm_gain = draw_norm_gain(jax.random.fold_in(key_of[14], 71), 0)
    expert_ids = draw_expert_ids(jax.random.fold_in(key_of[14], 71), 0)
    route_weights = jnp.clip(0.2 + 0.8 * jax.random.uniform(key_of[9], (SEQUENCE_TOKENS, TOPK), jnp.float32) ** levels(key_of[9], (SEQUENCE_TOKENS, TOPK), ((0, 8),), -0.2, 0.2), 0.2, 1.0)
    gate_weight = normal_values(key_of[10], (EXPERTS, D, FFE), D ** -0.5, 0.125, ((0, 8), (2, 4)))
    up_weight = normal_values(key_of[11], (EXPERTS, D, FFE), D ** -0.5, 0.125, ((0, 8), (2, 4)))
    down_weight = gaussian_with(key_of[12], (EXPERTS, FFE, D), (FFE // 4) ** -0.5, 0.25, ((0, 8), (1, 4)), (1, 2, 4, 2.0))
    final_gain = jnp.clip(1.0 + 0.18 * jax.random.normal(key_of[13], (D,), jnp.float32), 0.1, 1.9)
    return dict(queries=queries, projected_key_rows=projected_key_rows, projected_value_rows=projected_value_rows, query_gain=query_gain, key_norm_gain=key_norm_gain, residual=residual, out_weight=out_weight, norm_gain=norm_gain, expert_ids=expert_ids, route_weights=route_weights, gate_weight=gate_weight, up_weight=up_weight, down_weight=down_weight, final_gain=final_gain)


theta_base = 10000.0
norm_epsilon = 1e-06
residual_scale = 8.0 ** 0.25

def rope_line(halves, angles):
    pair_count = angles.shape[-1]
    first_half = halves[..., :pair_count]
    second_half = halves[..., pair_count:]
    cosine = jnp.cos(angles)[:, None, :]
    sine_part = jnp.sin(angles)[:, None, :]
    return jnp.concatenate([first_half * cosine - second_half * sine_part, first_half * sine_part + second_half * cosine], -1)

def rotary_over_grid(rows_by_head, token_positions):
    head_size = rows_by_head.shape[-1]
    frequency = theta_base ** (-jnp.arange(0, head_size // 2, 2, dtype=jnp.float32) / (head_size // 2))
    grid_row = (token_positions // GRID_W).astype(jnp.float32)
    grid_col = (token_positions % GRID_W).astype(jnp.float32)
    row_part = rope_line(rows_by_head[..., :head_size // 2], grid_row[:, None] * frequency[None, :])
    col_part = rope_line(rows_by_head[..., head_size // 2:], grid_col[:, None] * frequency[None, :])
    return jnp.concatenate([row_part, col_part], -1)

def normalize_heads(token_rows, gain_row, head_count):
    shaped = token_rows.astype(jnp.float32).reshape(token_rows.shape[0], head_count, -1)
    scaled = shaped * lax.rsqrt(lax.optimization_barrier(jnp.mean(shaped * shaped, -1, keepdims=True)) + norm_epsilon)
    return scaled * gain_row[None, None, :]

def layer_norm(stream):
    center = lax.optimization_barrier(jnp.mean(stream, -1, keepdims=True))
    spread = lax.optimization_barrier(jnp.mean(jnp.square(stream - center), -1, keepdims=True))
    return (stream - center) * lax.rsqrt(spread + norm_epsilon)

def attend_group(operands):
    head_queries, head_keys, head_values = operands
    scores = jnp.einsum('gqd,kd->gqk', head_queries.astype(jnp.float32), head_keys.astype(jnp.float32)) * HEAD_DIM ** (-0.5)
    weights = jnp.exp(scores - lax.optimization_barrier(jnp.max(scores, -1, keepdims=True)))
    row_total = lax.optimization_barrier(jnp.sum(weights, -1, keepdims=True))
    rounded = lax.optimization_barrier(weights.astype(jnp.bfloat16)).astype(jnp.float32)
    gathered = jnp.einsum('gqk,kd->gqd', rounded, head_values.astype(jnp.float32))
    return (gathered / row_total).astype(jnp.bfloat16)

def block_slots(block_ids):
    onehot = (block_ids[:, None] == jnp.arange(EXPERTS, dtype=jnp.int32)[None, :]).astype(jnp.int32)
    earlier = jnp.cumsum(onehot, 0) - onehot
    return lax.optimization_barrier(jnp.sum(earlier * onehot, 1))

def expert_rows(operands):
    token_rows, gate_mat, up_mat, down_mat = operands
    gate_sum = jnp.dot(token_rows, gate_mat, preferred_element_type=jnp.float32)
    up_sum = jnp.dot(token_rows, up_mat, preferred_element_type=jnp.float32)
    hidden = (jax.nn.silu(gate_sum) * up_sum).astype(jnp.bfloat16)
    split_hidden = hidden.reshape(hidden.shape[0], UNIT_BLOCKS, -1).astype(jnp.float32)
    split_down = down_mat.reshape(UNIT_BLOCKS, -1, down_mat.shape[-1]).astype(jnp.float32)
    partial_sums = jnp.einsum('rtf,tfd->trd', split_hidden, split_down)
    rounded = lax.optimization_barrier(partial_sums.astype(jnp.bfloat16)).astype(jnp.float32)
    return lax.optimization_barrier(jnp.sum(rounded, 0)).astype(jnp.bfloat16)

def reference(queries, projected_key_rows, projected_value_rows, query_gain, key_norm_gain, residual, out_weight, norm_gain, expert_ids, route_weights, gate_weight, up_weight, down_weight, final_gain):
    token_positions = jnp.arange(SEQUENCE_TOKENS, dtype=jnp.int32)
    queries_per_group = QUERY_HEAD_COUNT // KEY_VALUE_HEADS
    queries_after_rotation = rotary_over_grid(normalize_heads(queries, query_gain, QUERY_HEAD_COUNT), token_positions).astype(jnp.bfloat16)
    keys_after_rotation = rotary_over_grid(normalize_heads(projected_key_rows, key_norm_gain, KEY_VALUE_HEADS), token_positions).astype(jnp.bfloat16)
    grouped_query_heads = queries_after_rotation.reshape(SEQUENCE_TOKENS, KEY_VALUE_HEADS, queries_per_group, HEAD_DIM).transpose(1, 2, 0, 3)
    key_heads = keys_after_rotation.transpose(1, 0, 2)
    value_per_head = projected_value_rows.reshape(SEQUENCE_TOKENS, KEY_VALUE_HEADS, HEAD_DIM).transpose(1, 0, 2)
    attended = lax.map(attend_group, (grouped_query_heads, key_heads, value_per_head))
    attended = attended.transpose(2, 0, 1, 3).reshape(SEQUENCE_TOKENS, QUERY_HEAD_COUNT * HEAD_DIM)
    mixed_rows = jnp.dot(attended, out_weight, preferred_element_type=jnp.float32)
    pre_norm = residual_scale * residual.astype(jnp.float32) + mixed_rows
    normed = (layer_norm(pre_norm) * norm_gain[None, :]).astype(jnp.bfloat16)
    block_count = SEQUENCE_TOKENS // TOK_SP
    slots = jax.vmap(block_slots)(expert_ids.reshape(block_count, TOK_SP * TOPK)).reshape(SEQUENCE_TOKENS, TOPK)
    blocks = (jnp.arange(SEQUENCE_TOKENS, dtype=jnp.int32) // TOK_SP)[:, None]
    places = expert_ids * (block_count * CAP) + blocks * CAP + slots
    routed = jnp.zeros((EXPERTS * block_count * CAP, D), jnp.bfloat16)
    routed = routed.at[places.reshape(-1)].set(jnp.repeat(normed, TOPK, axis=0))
    expert_out = lax.map(expert_rows, (routed.reshape(EXPERTS, block_count * CAP, D), gate_weight, up_weight, down_weight))
    flat_out = expert_out.reshape(-1, D)
    combined = jnp.zeros((SEQUENCE_TOKENS, D), jnp.float32)
    for route_rank in range(TOPK):
        combined = combined + route_weights[:, route_rank:route_rank + 1] * flat_out[places[:, route_rank]].astype(jnp.float32)
    second_sum = residual_scale * normed.astype(jnp.float32) + combined
    return (layer_norm(second_sum) * final_gain[None, :]).astype(jnp.bfloat16)
```

```python
import contextlib

import jax
import jax.numpy as jnp
import numpy as np
from jax import lax
from jax.experimental import pallas as pl
from jax.experimental.pallas import tpu as pltpu
from jax.sharding import PartitionSpec as P

D = 2048
HEAD_DIM = 64
GRID_W = 64
TOPK = 2


theta_base = 10000.0
norm_epsilon = 1e-06
residual_scale = 8.0**0.25
far_below = -1e30
MESH = pl.DeviceIdType.MESH
SCOPES = False


def scope(name):
    return jax.named_scope(name) if SCOPES else contextlib.nullcontext()


def rotary_tables(grid_rows):
    quarter = HEAD_DIM // 4
    lane = np.arange(2 * HEAD_DIM)
    frequency = theta_base ** (-(lane % quarter) * 2.0 / (HEAD_DIM // 2))
    sign = np.where(lane % (2 * quarter) < quarter, -1.0, 1.0)
    by_row = lane % HEAD_DIM < HEAD_DIM // 2

    def tables(positions):
        angles = positions[:, None] * frequency[None, :].astype(np.float32).astype(np.float64)
        return np.stack([np.cos(angles), np.sin(angles) * sign[None, :]]).astype(np.float32)

    rows = np.where(by_row[None, None, :], tables(np.arange(grid_rows)), 0.0)
    columns = np.where(by_row[None, None, :], 0.0, tables(np.arange(GRID_W)))
    return rows.astype(np.float32), columns.astype(np.float32)


def place_of(index, group, group_minor):
    major = group // group_minor
    high, low = index // group_minor, lax.rem(index, group_minor)
    if group_minor == 1:
        return high
    back = major - 1 - high
    odd = lax.rem(back, 2)
    inner = (low - 1) * (1 - odd) + (group_minor - 1 - low) * odd
    first = jnp.where(low == 0, 1, 0)
    return first * high + (1 - first) * (major + back * (group_minor - 1) + inner)


def device_at(place, group, group_minor):
    major = group // group_minor
    if group_minor == 1:
        return place
    first = jnp.where(place < major, 1, 0)
    rest = jnp.maximum(place - major, 0)
    back = rest // (group_minor - 1)
    inner = lax.rem(rest, group_minor - 1)
    odd = lax.rem(back, 2)
    low = 1 + inner * (1 - odd) + (group_minor - 2 - inner) * odd
    other = (major - 1 - back) * group_minor + low
    return first * (place * group_minor) + (1 - first) * other


def layer(
    queries, key_rows, value_rows, row_table, column_table, query_gain, key_gain, out_weight, residual,
    norm_gain, expert_ids, route_weights, gate_weight, up_weight, down_weight, final_gain, experts,
    shards,
):
    token_count, width = residual.shape
    key_heads = key_rows.shape[1] // HEAD_DIM
    pair_width = 2 * HEAD_DIM
    query_rows = 2 * token_count
    ring_minor = 1 << ((experts.bit_length() - 1) // 2)
    ring_half = experts // 2
    pieces = 4
    piece = token_count // pieces
    lines = shards // 2
    row_total = TOPK * 2 * token_count
    capacity = row_total // experts
    groups = 4
    group_rows = row_total // groups
    group_experts = experts // groups
    halves = groups
    half_rows = row_total // halves
    hidden_units = gate_weight.shape[2]
    tile = min(256, hidden_units)
    feature_total = width * shards
    bf16, f32 = jnp.bfloat16, jnp.float32

    def kernel(
        row_hbm, column_hbm, q_gain_hbm, k_gain_hbm, gain_hbm, ids_hbm, rw_hbm, last_gain_hbm,
        q_hbm, k_hbm, v_hbm, res_hbm, ow_hbm, gate_hbm, up_hbm, down_hbm, out_ref,
        row_ref, column_ref, q_gain_ref, k_gain_ref, gain_ref, ids_ref, rw_ref, last_gain_ref,
        small_sem, q_v, k_v, v_v, res_ref, ow_ref, gate_v, up_v, down_v, weight_sem,
        ring_ref, ring_send, ring_recv, q_pad, flash_out, flash_max, flash_sum, att_ref,
        mix_send, mix_pair, line_send, line_recv, mix_sem, line_sem,
        stat_send, stat_recv, stat_sem,
        outgoing, routed, out_sem, fwd_sem, cross_sem, relay_sem,
        hidden, part_send, part_pair, sum_send, sum_recv, own_sum, other_sum, part_sem, sum_sem,
        result, returned, back_sem,
    ):
        me_s = lax.axis_index("sp")
        me_t = lax.axis_index("tp")
        line = me_t // 2
        core = lax.rem(me_t, 2)
        partner = line * 2 + 1 - core

        def line_at(step):
            return lax.rem(line + step, lines)

        barrier = pltpu.get_barrier_semaphore()
        for step in range(1, experts):
            pl.semaphore_signal(
                barrier, inc=1, device_id={"sp": lax.rem(me_s + step, experts)},
                device_id_type=MESH,
            )
        for step in range(1, shards):
            pl.semaphore_signal(
                barrier, inc=1, device_id={"tp": lax.rem(me_t + step, shards)},
                device_id_type=MESH,
            )
        loads = [
            pltpu.make_async_copy(src, dst, weight_sem.at[i])
            for i, (src, dst) in enumerate(
                (
                    (k_hbm, k_v), (v_hbm, v_v), (q_hbm, q_v), (ow_hbm, ow_ref), (res_hbm, res_ref),
                    (gate_hbm.at[0], gate_v), (up_hbm.at[0], up_v), (down_hbm.at[0], down_v),
                )
            )
        ]
        small_loads = [
            pltpu.make_async_copy(src, dst, small_sem.at[i])
            for i, (src, dst) in enumerate(
                (
                    (row_hbm, row_ref), (column_hbm, column_ref), (q_gain_hbm, q_gain_ref),
                    (k_gain_hbm, k_gain_ref), (gain_hbm, gain_ref), (ids_hbm, ids_ref),
                    (rw_hbm, rw_ref), (last_gain_hbm, last_gain_ref),
                )
            )
        ]
        for load in loads[:3] + small_loads + loads[3:]:
            load.start()
        sent = []

        def push(source, target, sems, index, device):
            copy = pltpu.make_async_remote_copy(
                src_ref=source, dst_ref=target,
                send_sem=sems.at[(0,) + index], recv_sem=sems.at[(1,) + index],
                device_id=device, device_id_type=MESH,
            )
            copy.start()
            sent.append(copy)
            return copy

        lane_pair = lax.broadcasted_iota(jnp.int32, (token_count, pair_width), 1)
        low_half = lane_pair < HEAD_DIM
        quarter = HEAD_DIM // 4
        turn_low = lane_pair % (2 * quarter) < quarter
        same_head = jnp.where(
            lax.broadcasted_iota(jnp.int32, (pair_width, pair_width), 0) // HEAD_DIM
            == lax.broadcasted_iota(jnp.int32, (pair_width, pair_width), 1) // HEAD_DIM,
            1.0, 0.0,
        ).astype(bf16)
        for load in small_loads:
            load.wait()

        def rotary(part):
            blocks = []
            for line_of_grid in range(token_count // GRID_W):
                row = row_ref[part, pl.ds(me_s * (token_count // GRID_W) + line_of_grid, 1)]
                blocks.append(column_ref[part] + row)
            return jnp.concatenate(blocks, 0)

        cosine, sine = rotary(0), rotary(1)
        both_gains = [
            jnp.concatenate([ref[...]] * 2, 1) for ref in (q_gain_ref, k_gain_ref)
        ]

        def rotated(rows, gain):
            square = rows * rows
            high = square.astype(bf16)
            rest = (square - high.astype(f32)).astype(bf16)
            total = jnp.dot(high, same_head, preferred_element_type=f32) + jnp.dot(
                rest, same_head, preferred_element_type=f32
            )
            scaled = rows * lax.rsqrt(total / HEAD_DIM + norm_epsilon) * gain
            turned = jnp.where(
                turn_low,
                pltpu.roll(scaled, pair_width - quarter, 1),
                pltpu.roll(scaled, quarter, 1),
            )
            return scaled * cosine + turned * sine

        def swap(rows):
            return pltpu.roll(rows, HEAD_DIM, 1)

        loads[0].wait()
        loads[1].wait()
        for pair in range((key_heads + 1) // 2):
            if key_heads == 1:
                key_pair = jnp.concatenate([k_v[...]] * 2, 1).astype(f32)
                value_pair = jnp.concatenate([v_v[...]] * 2, 1).astype(f32)
            else:
                lanes = pl.ds(pair * pair_width, pair_width)
                key_pair = k_v[:, lanes].astype(f32)
                value_pair = v_v[:, lanes].astype(f32)
            key_pair = rotated(key_pair, both_gains[1])
            ring_ref[0, :, pl.ds(2 * pair * pair_width, pair_width)] = jnp.where(
                low_half, key_pair, swap(value_pair)
            ).astype(bf16)
            if key_heads > 1:
                ring_ref[0, :, pl.ds((2 * pair + 1) * pair_width, pair_width)] = jnp.where(
                    low_half, swap(key_pair), value_pair
                ).astype(bf16)
        spot = place_of(me_s, experts, ring_minor)
        right = device_at(lax.rem(spot + 1, experts), experts, ring_minor)
        left = device_at(lax.rem(spot + experts - 1, experts), experts, ring_minor)
        with scope("barrier"):
            pl.semaphore_wait(barrier, experts + shards - 2)

        ring = {}

        def pass_on(hop, part):
            for way in range(2):
                if hop == ring_half and (part < pieces // 2) != (way == 0):
                    continue
                if hop > 1:
                    ring[way, hop - 1, part].wait_recv()
                span = pl.ds(part * piece, piece)
                source_slot = (hop - 1) if way == 0 else (experts - hop + 1) % experts
                target_slot = hop if way == 0 else experts - hop
                copy = pltpu.make_async_remote_copy(
                    src_ref=ring_ref.at[source_slot, span], dst_ref=ring_ref.at[target_slot, span],
                    send_sem=ring_send.at[way, hop - 1, part],
                    recv_sem=ring_recv.at[way, hop - 1, part],
                    device_id={"sp": right if way == 0 else left}, device_id_type=MESH,
                )
                copy.start()
                sent.append(copy)
                ring[way, hop, part] = copy

        def attend(slot, head, first):
            block = ring_ref[slot, :, pl.ds(head * pair_width, pair_width)]
            scores = lax.dot_general(
                block, q_pad[head], (((1,), (1,)), ((), ())), preferred_element_type=f32
            )
            peak = jnp.max(scores, 0, keepdims=True)
            if not first:
                peak = jnp.maximum(flash_max[head], peak)
            weights = jnp.exp(scores - peak)
            mass = jnp.sum(weights, 0, keepdims=True)
            gathered = lax.dot_general(
                block, weights.astype(bf16), (((0,), (0,)), ((), ())), preferred_element_type=f32
            )[HEAD_DIM:]
            if not first:
                fade = jnp.exp(flash_max[head] - peak)
                mass = mass + flash_sum[head] * fade
                gathered = gathered + flash_out[head] * fade
            flash_max[head] = peak
            flash_sum[head] = mass
            flash_out[head] = gathered

        def prepare(head):
            rows = rotated(
                q_v[:, pl.ds(head * pair_width, pair_width)].astype(f32), both_gains[0]
            ) * HEAD_DIM ** (-0.5)
            q_pad[head, pl.ds(0, token_count)] = jnp.where(low_half, rows, 0.0).astype(bf16)
            q_pad[head, pl.ds(token_count, token_count)] = jnp.where(
                low_half, swap(rows), 0.0
            ).astype(bf16)

        waiting = []
        for part in range(pieces):
            pass_on(1, part)
        loads[2].wait()
        for head in range(key_heads):
            prepare(head)
        waiting += [(0, head, True) for head in range(key_heads)]
        for hop in range(2, ring_half + 1):
            for part in range(pieces):
                pass_on(hop, part)
                for _ in range(-(-len(waiting) // (pieces - part))):
                    attend(*waiting.pop(0))
            if hop < ring_half:
                for slot in (hop - 1, experts - hop + 1):
                    waiting += [(slot, head, False) for head in range(key_heads)]
        with scope("ring_tail"):
            for way in range(2):
                for part in range(pieces):
                    if (way, ring_half, part) not in ring:
                        ring[way, ring_half - 1, part].wait_recv()
        for slot in (ring_half - 1, ring_half + 1):
            for head in range(key_heads):
                attend(slot, head, False)
        with scope("ring_last"):
            for way in range(2):
                for part in range(pieces):
                    if (way, ring_half, part) in ring:
                        ring[way, ring_half, part].wait_recv()
        for head in range(key_heads):
            attend(ring_half, head, False)
            result_rows = flash_out[head] / flash_sum[head]
            att_ref[:, pl.ds(head * pair_width, pair_width)] = (
                jnp.concatenate([result_rows[:, :token_count], result_rows[:, token_count:]], 0)
                .T.astype(bf16)
            )
        attended_rows = att_ref[...]
        loads[3].wait()

        def mix(shard):
            return jnp.dot(
                attended_rows,
                ow_ref[:, pl.ds(pl.multiple_of(shard * width, width), width)],
                preferred_element_type=f32,
            )

        for step in range(lines):
            mix_send[step] = mix(line_at(step) * 2 + 1 - core).astype(bf16)
        pair = {}
        for step in list(range(1, lines)) + [0]:
            pair[step] = push(
                mix_send.at[step], mix_pair.at[step], mix_sem, (step,), {"tp": partner}
            )
        across = {}
        for step in range(1, lines):
            mine = mix(line_at(step) * 2 + core)
            pair[step].wait_recv()
            line_send[step - 1] = (mine + mix_pair[step].astype(f32)).astype(bf16)
            across[step] = push(
                line_send.at[step - 1], line_recv.at[step - 1], line_sem, (step - 1,),
                {"tp": line_at(step) * 2 + core},
            )
        total = mix(me_t)
        pair[0].wait_recv()
        total = total + mix_pair[0].astype(f32)
        loads[4].wait()
        total = total + residual_scale * res_ref[...].astype(f32)
        for step in range(1, lines):
            across[step].wait_recv()
            total = total + line_recv[step - 1].astype(f32)

        lane = lax.broadcasted_iota(jnp.int32, (token_count, 128), 1)

        before = jnp.where(
            lax.broadcasted_iota(jnp.int32, (token_count, token_count), 1)
            < lax.broadcasted_iota(jnp.int32, (token_count, token_count), 0),
            1.0, 0.0,
        ).astype(bf16)

        def columns_of(rows):
            return jnp.concatenate([rows] * (token_count // TOPK), 0).T

        ids = columns_of(ids_ref[...].astype(f32)).astype(jnp.int32)
        routing = columns_of(rw_ref[...])
        marked = [jnp.where(lane == ids[:, k : k + 1], 1.0, 0.0) for k in range(TOPK)]
        earlier = jnp.dot(before, (marked[0] + marked[1]).astype(bf16), preferred_element_type=f32)
        at = []
        for k in range(TOPK):
            away = lax.rem(ids[:, k : k + 1] - me_s + experts, experts)
            at.append(
                (away * capacity).astype(f32) + jnp.sum(earlier * marked[k], 1, keepdims=True)
            )
        across = jnp.where(lane == 0, at[0], jnp.where(lane == 1, at[1], 0.0)).T.astype(jnp.int32)
        at = [column.astype(jnp.int32) for column in at]

        def normalize(values, gain, turn):
            sums = jnp.sum(values, 1, keepdims=True)
            squares = jnp.sum(values * values, 1, keepdims=True)
            both = jnp.where(lane == 0, sums, jnp.where(lane == 1, squares, 0.0)).T[:8]
            stat_send[turn] = both
            stats = [
                push(
                    stat_send.at[turn], stat_recv.at[turn, step - 1], stat_sem,
                    (turn, step - 1), {"tp": lax.rem(me_t + step, shards)},
                )
                for step in range(1, shards)
            ]
            for step in range(1, shards):
                stats[step - 1].wait_recv()
                both = both + stat_recv[turn, step - 1]
            columns = jnp.concatenate([both] * 16, 0).T
            center = columns[:, 0:1] / feature_total
            spread = columns[:, 1:2] / feature_total - center * center
            return (values - center) * lax.rsqrt(spread + norm_epsilon) * gain

        normed = normalize(total, gain_ref[...], 0).astype(bf16)
        row_index = lax.broadcasted_iota(jnp.int32, (row_total, token_count), 0)
        picks = jnp.where(
            (row_index == across[0:1, :]) | (row_index == across[1:2, :]), 1.0, 0.0
        ).astype(bf16)
        spread_rows = jnp.dot(picks, normed, preferred_element_type=f32).astype(bf16)
        outgoing[...] = spread_rows
        routed[me_t, pl.ds(0, capacity)] = spread_rows[:capacity]
        arrivals = {}
        for step in range(1, experts):
            rows = pl.ds(step * capacity, capacity)
            arrivals[step] = push(
                outgoing.at[rows], routed.at[me_t, rows], out_sem, (step,),
                {"sp": lax.rem(me_s + step, experts)},
            )
        forwards, crossings, relays = {}, {}, {}

        def forward(group):
            for step in range(group * group_experts, (group + 1) * group_experts):
                if step > 0:
                    arrivals[step].wait_recv()
            rows = pl.ds(group * group_rows, group_rows)
            block = routed.at[me_t, rows]
            for step in range(1, lines):
                crossings[group, step] = push(
                    block, block, cross_sem, (group, step - 1),
                    {"tp": line_at(step) * 2 + core},
                )
            forwards[group] = push(block, block, fwd_sem, (group,), {"tp": partner})

        def relay(group):
            rows = pl.ds(group * group_rows, group_rows)
            for step in range(1, lines):
                crossings[group, step].wait_recv()
                block = routed.at[line_at(lines - step) * 2 + core, rows]
                relays[group, step] = push(
                    block, block, relay_sem, (group, step - 1), {"tp": partner}
                )

        def settle(group):
            forwards[group].wait_recv()
            for step in range(1, lines):
                relays[group, step].wait_recv()

        def expand(half):
            rows = pl.ds(half * half_rows, half_rows)

            def one_tile(index, carry):
                cols = pl.ds(pl.multiple_of(index * tile, tile), tile)
                gate_sum = jnp.zeros((half_rows, tile), f32)
                up_sum = jnp.zeros((half_rows, tile), f32)
                for shard in range(shards):
                    block = routed[shard, rows]
                    deep = pl.ds(shard * width, width)
                    gate_sum += jnp.dot(block, gate_v[deep, cols], preferred_element_type=f32)
                    up_sum += jnp.dot(block, up_v[deep, cols], preferred_element_type=f32)
                hidden[rows, cols] = (
                    gate_sum / (1.0 + jnp.exp(-gate_sum)) * up_sum
                ).astype(bf16)
                return carry

            lax.fori_loop(0, hidden_units // tile, one_tile, 0)

        def down(half, shard):
            return jnp.dot(
                hidden[pl.ds(half * half_rows, half_rows)],
                down_v[:, pl.ds(pl.multiple_of(shard * width, width), width)],
                preferred_element_type=f32,
            )

        parts, sums = {}, {}

        def shrink(half):
            for step in list(range(1, lines)) + [0]:
                part_send[half, step] = down(half, line_at(step) * 2 + 1 - core).astype(bf16)
                parts[half, step] = push(
                    part_send.at[half, step], part_pair.at[half, step], part_sem, (half, step),
                    {"tp": partner},
                )
            for step in range(1, lines):
                other_sum[half, step - 1] = down(half, line_at(step) * 2 + core)
            own_sum[half] = down(half, me_t)

        def join(half):
            for step in range(1, lines):
                parts[half, step].wait_recv()
                sum_send[half, step - 1] = (
                    other_sum[half, step - 1] + part_pair[half, step].astype(f32)
                ).astype(bf16)
                sums[half, step] = push(
                    sum_send.at[half, step - 1], sum_recv.at[half, step - 1], sum_sem,
                    (half, step - 1), {"tp": line_at(step) * 2 + core},
                )

        backs = {}

        def finish(half):
            parts[half, 0].wait_recv()
            value = own_sum[half] + part_pair[half, 0].astype(f32)
            for step in range(1, lines):
                sums[half, step].wait_recv()
                value = value + sum_recv[half, step - 1].astype(f32)
            value = value.astype(bf16)
            result[pl.ds(half * half_rows, half_rows)] = value
            first = half * (experts // halves)
            if half == 0:
                returned[pl.ds(0, capacity)] = value[:capacity]
            for step in range(max(first, 1), first + experts // halves):
                rows = pl.ds(step * capacity, capacity)
                backs[step] = push(
                    result.at[rows], returned.at[rows], back_sem, (step,),
                    {"sp": lax.rem(me_s + experts - step, experts)},
                )

        forward(0)
        forward(1)
        relay(0)
        for load in loads[5:7]:
            load.wait()
        settle(0)
        expand(0)
        forward(2)
        relay(1)
        loads[7].wait()
        shrink(0)
        forward(3)
        settle(1)
        join(0)
        expand(1)
        relay(2)
        shrink(1)
        settle(2)
        join(1)
        finish(0)
        expand(2)
        relay(3)
        shrink(2)
        settle(3)
        join(2)
        finish(1)
        expand(3)
        shrink(3)
        join(3)
        finish(2)
        finish(3)
        slot_index = lax.broadcasted_iota(jnp.int32, (token_count, row_total), 1)
        choose = [
            jnp.where(slot_index == at[k], 1.0, 0.0).astype(bf16)
            for k in range(TOPK)
        ]
        for step in range(1, experts):
            backs[step].wait_recv()
        second_sum = residual_scale * normed.astype(f32)
        back_rows = returned[...]
        for k in range(TOPK):
            second_sum = second_sum + routing[:, k : k + 1] * jnp.dot(
                choose[k], back_rows, preferred_element_type=f32
            )
        out_ref[...] = normalize(second_sum, last_gain_ref[...], 1).astype(bf16)
        for copy in sent:
            copy.wait_send()

    vmem = pl.BlockSpec(memory_space=pltpu.VMEM)
    hbm = pl.BlockSpec(memory_space=pltpu.HBM)
    dma = pltpu.SemaphoreType.DMA
    other = max(lines - 1, 1)
    return pl.pallas_call(
        kernel,
        out_shape=jax.ShapeDtypeStruct((token_count, width), bf16),
        in_specs=[hbm] * 16,
        out_specs=vmem,
        scratch_shapes=[
            pltpu.VMEM(row_table.shape, f32),
            pltpu.VMEM(column_table.shape, f32),
            pltpu.VMEM((1, HEAD_DIM), f32),
            pltpu.VMEM((1, HEAD_DIM), f32),
            pltpu.VMEM((1, width), f32),
            pltpu.VMEM((TOPK, token_count), jnp.int32),
            pltpu.VMEM((TOPK, token_count), f32),
            pltpu.VMEM((1, width), f32),
            dma((8,)),
            pltpu.VMEM(queries.shape, bf16),
            pltpu.VMEM(key_rows.shape, bf16),
            pltpu.VMEM(value_rows.shape, bf16),
            pltpu.VMEM(residual.shape, bf16),
            pltpu.VMEM(out_weight.shape, bf16),
            pltpu.VMEM(gate_weight.shape[1:], bf16),
            pltpu.VMEM(up_weight.shape[1:], bf16),
            pltpu.VMEM(down_weight.shape[1:], bf16),
            dma((8,)),
            pltpu.VMEM((experts, token_count, key_heads * pair_width), bf16),
            dma((2, ring_half, pieces)),
            dma((2, ring_half, pieces)),
            pltpu.VMEM((key_heads, query_rows, pair_width), bf16),
            pltpu.VMEM((key_heads, HEAD_DIM, query_rows), f32),
            pltpu.VMEM((key_heads, 1, query_rows), f32),
            pltpu.VMEM((key_heads, 1, query_rows), f32),
            pltpu.VMEM((token_count, key_heads * pair_width), bf16),
            pltpu.VMEM((lines, token_count, width), bf16),
            pltpu.VMEM((lines, token_count, width), bf16),
            pltpu.VMEM((other, token_count, width), bf16),
            pltpu.VMEM((other, token_count, width), bf16),
            dma((2, lines)),
            dma((2, other)),
            pltpu.VMEM((2, 8, token_count), f32),
            pltpu.VMEM((2, shards - 1, 8, token_count), f32),
            dma((2, 2, shards - 1)),
            pltpu.VMEM((row_total, width), bf16),
            pltpu.VMEM((shards, row_total, width), bf16),
            dma((2, experts)),
            dma((2, groups)),
            dma((2, groups, other)),
            dma((2, groups, other)),
            pltpu.VMEM((row_total, hidden_units), bf16),
            pltpu.VMEM((halves, lines, half_rows, width), bf16),
            pltpu.VMEM((halves, lines, half_rows, width), bf16),
            pltpu.VMEM((halves, other, half_rows, width), bf16),
            pltpu.VMEM((halves, other, half_rows, width), bf16),
            pltpu.VMEM((halves, half_rows, width), f32),
            pltpu.VMEM((halves, other, half_rows, width), f32),
            dma((2, halves, lines)),
            dma((2, halves, other)),
            pltpu.VMEM((row_total, width), bf16),
            pltpu.VMEM((row_total, width), bf16),
            dma((2, experts)),
        ],
        compiler_params=pltpu.CompilerParams(
            collective_id=0, has_side_effects=True, vmem_limit_bytes=58 << 20
        ),
    )(
        row_table, column_table, query_gain.reshape(1, -1), key_gain.reshape(1, -1),
        norm_gain.reshape(1, -1), expert_ids.T, route_weights.T,
        final_gain.reshape(1, -1), queries, key_rows, value_rows, residual, out_weight,
        gate_weight, up_weight, down_weight,
    )


def per_device(
    queries,
    projected_key_rows,
    projected_value_rows,
    query_gain,
    key_norm_gain,
    residual,
    out_weight,
    norm_gain,
    expert_ids,
    route_weights,
    gate_weight,
    up_weight,
    down_weight,
    final_gain,
):
    token_total = queries.shape[0] * lax.axis_size("sp")
    row_table, column_table = rotary_tables(-(-token_total // GRID_W))
    return layer(
        queries,
        projected_key_rows,
        projected_value_rows,
        row_table,
        column_table,
        query_gain,
        key_norm_gain,
        out_weight,
        residual,
        norm_gain,
        expert_ids,
        route_weights,
        gate_weight,
        up_weight,
        down_weight,
        final_gain,
        lax.axis_size("sp"),
        lax.axis_size("tp"),
    )


def solution(mesh):
    in_specs = (
        P("sp", "tp"),
        P("sp", "tp"),
        P("sp", "tp"),
        P(),
        P(),
        P("sp", "tp"),
        P("tp", None),
        P("tp"),
        P("sp", None),
        P("sp", None),
        P("sp", None, "tp"),
        P("sp", None, "tp"),
        P("sp", "tp", None),
        P("tp"),
    )
    out_specs = P("sp", "tp")
    return jax.shard_map(
        per_device, mesh=mesh, in_specs=in_specs, out_specs=out_specs, check_vma=False
    )
```

```python
import contextlib

import jax
import jax.numpy as jnp
import numpy as np
from jax import lax
from jax.experimental import pallas as pl
from jax.experimental.pallas import tpu as pltpu
from jax.sharding import PartitionSpec as P

D = 2048
HEAD_DIM = 64
GRID_W = 64
EXP_GROUP = 4
TOPK = 2


theta_base = 10000.0
norm_epsilon = 1e-06
residual_scale = 8.0**0.25
far_below = -1e30
MESH = pl.DeviceIdType.MESH
SCOPES = False


def scope(name):
    return jax.named_scope(name) if SCOPES else contextlib.nullcontext()


def rotary_tables(grid_rows):
    quarter = HEAD_DIM // 4
    lane = np.arange(2 * HEAD_DIM)
    frequency = theta_base ** (-(lane % quarter) * 2.0 / (HEAD_DIM // 2))
    sign = np.where(lane % (2 * quarter) < quarter, -1.0, 1.0)
    by_row = lane % HEAD_DIM < HEAD_DIM // 2

    def tables(positions):
        angles = positions[:, None] * frequency[None, :].astype(np.float32).astype(np.float64)
        return np.stack([np.cos(angles), np.sin(angles) * sign[None, :]]).astype(np.float32)

    rows = np.where(by_row[None, None, :], tables(np.arange(grid_rows)), 0.0)
    columns = np.where(by_row[None, None, :], 0.0, tables(np.arange(GRID_W)))
    return rows.astype(np.float32), columns.astype(np.float32)


def place_of(index, group, group_minor):
    major = group // group_minor
    high, low = index // group_minor, lax.rem(index, group_minor)
    if group_minor == 1:
        return high
    back = major - 1 - high
    odd = lax.rem(back, 2)
    inner = (low - 1) * (1 - odd) + (group_minor - 1 - low) * odd
    first = jnp.where(low == 0, 1, 0)
    return first * high + (1 - first) * (major + back * (group_minor - 1) + inner)


def device_at(place, group, group_minor):
    major = group // group_minor
    if group_minor == 1:
        return place
    first = jnp.where(place < major, 1, 0)
    rest = jnp.maximum(place - major, 0)
    back = rest // (group_minor - 1)
    inner = lax.rem(rest, group_minor - 1)
    odd = lax.rem(back, 2)
    low = 1 + inner * (1 - odd) + (group_minor - 2 - inner) * odd
    other = (major - 1 - back) * group_minor + low
    return first * (place * group_minor) + (1 - first) * other


def layer(
    queries, key_rows, value_rows, row_table, column_table, query_gain, key_gain, out_weight, residual,
    norm_gain, expert_ids, route_weights, gate_weight, up_weight, down_weight, final_gain, experts,
    shards,
):
    token_count, width = residual.shape
    key_heads = key_rows.shape[1] // HEAD_DIM
    pair_width = 2 * HEAD_DIM
    query_rows = 2 * token_count
    ring_minor = 1 << ((experts.bit_length() - 1) // 2)
    ring_half = experts // 2
    pieces = 4
    piece = token_count // pieces
    lines = shards // 2
    groups = experts // EXP_GROUP
    capacity = token_count // groups
    sets = (1, groups - 1) if groups > 1 else (1,)
    set_rows = [EXP_GROUP * blocks * capacity for blocks in sets]
    row_total = sum(set_rows)
    hidden_units = gate_weight.shape[2]
    tile = min(256, hidden_units)
    feature_total = width * shards
    bf16, f32 = jnp.bfloat16, jnp.float32

    def kernel(
        row_hbm, column_hbm, q_gain_hbm, k_gain_hbm, gain_hbm, ids_hbm, rw_hbm, last_gain_hbm,
        q_hbm, k_hbm, v_hbm, res_hbm, ow_hbm, gate_hbm, up_hbm, down_hbm, out_ref,
        row_ref, column_ref, q_gain_ref, k_gain_ref, gain_ref, ids_ref, rw_ref, last_gain_ref,
        small_sem, q_v, k_v, v_v, res_ref, ow_ref, gate_v, up_v, down_v, weight_sem,
        ring_ref, ring_send, ring_recv, q_pad, flash_out, flash_max, flash_sum, att_ref,
        mix_send, mix_pair, line_send, line_recv, mix_sem, line_sem,
        stat_send, stat_recv, stat_sem,
        perm_ref, back_ref, weight_send, weight_recv, share_sem, scale_ref, outgoing, hidden,
        cross_sem, home, returned_ref, back_sem, *per_set,
    ):
        count = len(sets)
        (
            routed, spread_sem, mirror_sem, part_send, part_recv, part_sem, give, take, return_sem,
            kept,
        ) = [per_set[i * count : (i + 1) * count] for i in range(10)]
        me_s = lax.axis_index("sp")
        me_t = lax.axis_index("tp")
        line = me_t // 2
        core = lax.rem(me_t, 2)
        partner = line * 2 + 1 - core

        def line_at(step):
            return lax.rem(line + step, lines)

        me_g = me_s // EXP_GROUP
        me_m = lax.rem(me_s, EXP_GROUP)

        def member(turn):
            if turn == 0:
                return me_m
            if turn == 1:
                return me_m + 1 - 2 * lax.rem(me_m, 2)
            if turn == 2:
                return me_m + 2 - 4 * (me_m // 2)
            return EXP_GROUP - 1 - me_m

        def line_before(step):
            return lax.rem(line + lines - step, lines)

        def group_device(step):
            return {"sp": lax.rem(me_g + step + groups, groups) * EXP_GROUP + me_m}

        def square_device(turn, step):
            return {"sp": me_g * EXP_GROUP + member(turn), "tp": line_at(step) * 2 + core}

        barrier = pltpu.get_barrier_semaphore()
        for step in range(1, experts):
            pl.semaphore_signal(
                barrier, inc=1, device_id={"sp": lax.rem(me_s + step, experts)},
                device_id_type=MESH,
            )
        for step in range(1, shards):
            pl.semaphore_signal(
                barrier, inc=1, device_id={"tp": lax.rem(me_t + step, shards)},
                device_id_type=MESH,
            )
        for turn in range(1, EXP_GROUP):
            for step in range(1, lines):
                pl.semaphore_signal(
                    barrier, inc=1, device_id=square_device(turn, step), device_id_type=MESH
                )
        greeted = experts - 1 + shards - 1 + (EXP_GROUP - 1) * (lines - 1)
        loads = [
            pltpu.make_async_copy(src, dst, weight_sem.at[i])
            for i, (src, dst) in enumerate(
                (
                    (k_hbm, k_v), (v_hbm, v_v), (q_hbm, q_v), (ow_hbm, ow_ref), (res_hbm, res_ref),
                    (gate_hbm.at[0], gate_v), (up_hbm.at[0], up_v), (down_hbm.at[0], down_v),
                )
            )
        ]
        small_loads = [
            pltpu.make_async_copy(src, dst, small_sem.at[i])
            for i, (src, dst) in enumerate(
                (
                    (row_hbm, row_ref), (column_hbm, column_ref), (q_gain_hbm, q_gain_ref),
                    (k_gain_hbm, k_gain_ref), (gain_hbm, gain_ref), (ids_hbm, ids_ref),
                    (rw_hbm, rw_ref), (last_gain_hbm, last_gain_ref),
                )
            )
        ]
        for load in loads[:3] + small_loads + loads[3:]:
            load.start()
        sent = []

        def push(source, target, sems, index, device):
            copy = pltpu.make_async_remote_copy(
                src_ref=source, dst_ref=target,
                send_sem=sems.at[(0,) + index], recv_sem=sems.at[(1,) + index],
                device_id=device, device_id_type=MESH,
            )
            copy.start()
            sent.append(copy)
            return copy

        lane_pair = lax.broadcasted_iota(jnp.int32, (token_count, pair_width), 1)
        low_half = lane_pair < HEAD_DIM
        quarter = HEAD_DIM // 4
        turn_low = lane_pair % (2 * quarter) < quarter
        same_head = jnp.where(
            lax.broadcasted_iota(jnp.int32, (pair_width, pair_width), 0) // HEAD_DIM
            == lax.broadcasted_iota(jnp.int32, (pair_width, pair_width), 1) // HEAD_DIM,
            1.0, 0.0,
        ).astype(bf16)
        for load in small_loads:
            load.wait()

        def rotary(part):
            blocks = []
            for line_of_grid in range(token_count // GRID_W):
                row = row_ref[part, pl.ds(me_s * (token_count // GRID_W) + line_of_grid, 1)]
                blocks.append(column_ref[part] + row)
            return jnp.concatenate(blocks, 0)

        cosine, sine = rotary(0), rotary(1)
        both_gains = [
            jnp.concatenate([ref[...]] * 2, 1) for ref in (q_gain_ref, k_gain_ref)
        ]

        def rotated(rows, gain):
            square = rows * rows
            high = square.astype(bf16)
            rest = (square - high.astype(f32)).astype(bf16)
            total = jnp.dot(high, same_head, preferred_element_type=f32) + jnp.dot(
                rest, same_head, preferred_element_type=f32
            )
            scaled = rows * lax.rsqrt(total / HEAD_DIM + norm_epsilon) * gain
            turned = jnp.where(
                turn_low,
                pltpu.roll(scaled, pair_width - quarter, 1),
                pltpu.roll(scaled, quarter, 1),
            )
            return scaled * cosine + turned * sine

        def swap(rows):
            return pltpu.roll(rows, HEAD_DIM, 1)

        loads[0].wait()
        loads[1].wait()
        for pair in range((key_heads + 1) // 2):
            if key_heads == 1:
                key_pair = jnp.concatenate([k_v[...]] * 2, 1).astype(f32)
                value_pair = jnp.concatenate([v_v[...]] * 2, 1).astype(f32)
            else:
                lanes = pl.ds(pair * pair_width, pair_width)
                key_pair = k_v[:, lanes].astype(f32)
                value_pair = v_v[:, lanes].astype(f32)
            key_pair = rotated(key_pair, both_gains[1])
            ring_ref[0, :, pl.ds(2 * pair * pair_width, pair_width)] = jnp.where(
                low_half, key_pair, swap(value_pair)
            ).astype(bf16)
            if key_heads > 1:
                ring_ref[0, :, pl.ds((2 * pair + 1) * pair_width, pair_width)] = jnp.where(
                    low_half, swap(key_pair), value_pair
                ).astype(bf16)
        spot = place_of(me_s, experts, ring_minor)
        right = device_at(lax.rem(spot + 1, experts), experts, ring_minor)
        left = device_at(lax.rem(spot + experts - 1, experts), experts, ring_minor)
        with scope("barrier"):
            pl.semaphore_wait(barrier, greeted)

        ring = {}

        def pass_on(hop, part):
            for way in range(2):
                if hop == ring_half and (part < pieces // 2) != (way == 0):
                    continue
                if hop > 1:
                    ring[way, hop - 1, part].wait_recv()
                span = pl.ds(part * piece, piece)
                source_slot = (hop - 1) if way == 0 else (experts - hop + 1) % experts
                target_slot = hop if way == 0 else experts - hop
                copy = pltpu.make_async_remote_copy(
                    src_ref=ring_ref.at[source_slot, span], dst_ref=ring_ref.at[target_slot, span],
                    send_sem=ring_send.at[way, hop - 1, part],
                    recv_sem=ring_recv.at[way, hop - 1, part],
                    device_id={"sp": right if way == 0 else left}, device_id_type=MESH,
                )
                copy.start()
                sent.append(copy)
                ring[way, hop, part] = copy

        def attend(slot, head, first):
            block = ring_ref[slot, :, pl.ds(head * pair_width, pair_width)]
            scores = lax.dot_general(
                block, q_pad[head], (((1,), (1,)), ((), ())), preferred_element_type=f32
            )
            peak = jnp.max(scores, 0, keepdims=True)
            if not first:
                peak = jnp.maximum(flash_max[head], peak)
            weights = jnp.exp(scores - peak)
            mass = jnp.sum(weights, 0, keepdims=True)
            gathered = lax.dot_general(
                block, weights.astype(bf16), (((0,), (0,)), ((), ())), preferred_element_type=f32
            )[HEAD_DIM:]
            if not first:
                fade = jnp.exp(flash_max[head] - peak)
                mass = mass + flash_sum[head] * fade
                gathered = gathered + flash_out[head] * fade
            flash_max[head] = peak
            flash_sum[head] = mass
            flash_out[head] = gathered

        def prepare(head):
            rows = rotated(
                q_v[:, pl.ds(head * pair_width, pair_width)].astype(f32), both_gains[0]
            ) * HEAD_DIM ** (-0.5)
            q_pad[head, pl.ds(0, token_count)] = jnp.where(low_half, rows, 0.0).astype(bf16)
            q_pad[head, pl.ds(token_count, token_count)] = jnp.where(
                low_half, swap(rows), 0.0
            ).astype(bf16)

        def columns_of(rows):
            return jnp.concatenate([rows] * (token_count // TOPK), 0).T

        lane = lax.broadcasted_iota(jnp.int32, (token_count, 128), 1)
        before = jnp.where(
            lax.broadcasted_iota(jnp.int32, (token_count, token_count), 1)
            < lax.broadcasted_iota(jnp.int32, (token_count, token_count), 0),
            1.0, 0.0,
        ).astype(bf16)

        def route():
            ids = columns_of(ids_ref[...].astype(f32)).astype(jnp.int32)
            routing = columns_of(rw_ref[...])
            group_of = ids[:, 0:1] // EXP_GROUP
            inside = jnp.where(lane == group_of, 1.0, 0.0)
            earlier = jnp.dot(before, inside.astype(bf16), preferred_element_type=f32)
            slot = jnp.sum(earlier * inside, 1, keepdims=True)
            away = lax.rem(group_of - me_g + groups, groups)
            place = (away * capacity).astype(f32) + slot
            place_row = jnp.where(lane == 0, place, 0.0).T[0:1].astype(jnp.int32)
            place = place.astype(jnp.int32)
            row_index = lax.broadcasted_iota(jnp.int32, (token_count, token_count), 0)
            picks = jnp.where(row_index == place_row, 1.0, 0.0)
            perm_ref[...] = picks.astype(bf16)
            back_ref[...] = jnp.where(
                lax.broadcasted_iota(jnp.int32, (token_count, token_count), 1) == place, 1.0, 0.0
            ).astype(bf16)
            by_expert = sum(
                jnp.where(lane == ids[:, k : k + 1], routing[:, k : k + 1], 0.0)
                for k in range(TOPK)
            )
            by_slot = jnp.dot(
                picks, by_expert, preferred_element_type=f32, precision=lax.Precision.HIGHEST
            ).T
            for expert in range(experts):
                weight_send[expert] = jnp.broadcast_to(
                    by_slot[expert : expert + 1], (8, token_count)
                )
            weight_recv[me_s] = weight_send[me_s]
            return {
                step: push(
                    weight_send.at[lax.rem(me_s + step, experts)], weight_recv.at[me_s], share_sem,
                    (step,), {"sp": lax.rem(me_s + step, experts)},
                )
                for step in range(1, experts)
            }

        waiting = []
        for part in range(pieces):
            pass_on(1, part)
        loads[2].wait()
        for head in range(key_heads):
            prepare(head)
        shares = route()
        waiting += [(0, head, True) for head in range(key_heads)]
        for hop in range(2, ring_half + 1):
            for part in range(pieces):
                pass_on(hop, part)
                for _ in range(-(-len(waiting) // (pieces - part))):
                    attend(*waiting.pop(0))
            if hop < ring_half:
                for slot in (hop - 1, experts - hop + 1):
                    waiting += [(slot, head, False) for head in range(key_heads)]
        with scope("ring_tail"):
            for way in range(2):
                for part in range(pieces):
                    if (way, ring_half, part) not in ring:
                        ring[way, ring_half - 1, part].wait_recv()
        for slot in (ring_half - 1, ring_half + 1):
            for head in range(key_heads):
                attend(slot, head, False)
        with scope("ring_last"):
            for way in range(2):
                for part in range(pieces):
                    if (way, ring_half, part) in ring:
                        ring[way, ring_half, part].wait_recv()
        for head in range(key_heads):
            attend(ring_half, head, False)
            result_rows = flash_out[head] / flash_sum[head]
            att_ref[:, pl.ds(head * pair_width, pair_width)] = (
                jnp.concatenate([result_rows[:, :token_count], result_rows[:, token_count:]], 0)
                .T.astype(bf16)
            )
        attended_rows = att_ref[...]
        loads[3].wait()

        def mix(shard):
            return jnp.dot(
                attended_rows,
                ow_ref[:, pl.ds(pl.multiple_of(shard * width, width), width)],
                preferred_element_type=f32,
            )

        with scope("mix"):
            pass
        for step in range(lines):
            mix_send[step] = mix(line_at(step) * 2 + 1 - core).astype(bf16)
        pair = {}
        for step in list(range(1, lines)) + [0]:
            pair[step] = push(
                mix_send.at[step], mix_pair.at[step], mix_sem, (step,), {"tp": partner}
            )
        across = {}
        for step in range(1, lines):
            mine = mix(line_at(step) * 2 + core)
            pair[step].wait_recv()
            line_send[step - 1] = (mine + mix_pair[step].astype(f32)).astype(bf16)
            across[step] = push(
                line_send.at[step - 1], line_recv.at[step - 1], line_sem, (step - 1,),
                {"tp": line_at(step) * 2 + core},
            )
        total = mix(me_t)
        pair[0].wait_recv()
        total = total + mix_pair[0].astype(f32)
        loads[4].wait()
        total = total + residual_scale * res_ref[...].astype(f32)
        for step in range(1, lines):
            across[step].wait_recv()
            total = total + line_recv[step - 1].astype(f32)

        def normalize(values, gain, turn):
            sums = jnp.sum(values, 1, keepdims=True)
            squares = jnp.sum(values * values, 1, keepdims=True)
            both = jnp.where(lane == 0, sums, jnp.where(lane == 1, squares, 0.0)).T[:8]
            stat_send[turn] = both
            stats = [
                push(
                    stat_send.at[turn], stat_recv.at[turn, step - 1], stat_sem,
                    (turn, step - 1), {"tp": lax.rem(me_t + step, shards)},
                )
                for step in range(1, shards)
            ]
            for step in range(1, shards):
                stats[step - 1].wait_recv()
                both = both + stat_recv[turn, step - 1]
            columns = jnp.concatenate([both] * 16, 0).T
            center = columns[:, 0:1] / feature_total
            spread = columns[:, 1:2] / feature_total - center * center
            return (values - center) * lax.rsqrt(spread + norm_epsilon) * gain

        with scope("norm1"):
            normed = normalize(total, gain_ref[...], 0).astype(bf16)
        spread_rows = jnp.dot(perm_ref[...], normed, preferred_element_type=f32).astype(bf16)
        outgoing[...] = spread_rows
        first_rows = pl.ds(pl.multiple_of(me_m * capacity, capacity), capacity)
        routed[0][me_t, first_rows] = spread_rows[:capacity]
        square = [(turn, step) for turn in range(EXP_GROUP) for step in range(lines)]
        square.sort(key=lambda pair: -(pair[0] + 1) // 2 - min(pair[1], lines - pair[1]))
        square.remove((0, 0))

        def chunk_rows(index, owner):
            count = sets[index] * capacity
            return pl.ds(pl.multiple_of(owner * count, count), count)

        crossings = {
            step: push(
                outgoing.at[pl.ds(step * capacity, capacity)],
                routed[1].at[
                    me_t,
                    pl.ds(
                        pl.multiple_of((me_m * sets[1] + step - 1) * capacity, capacity), capacity
                    ),
                ],
                cross_sem, (step - 1,), group_device(step),
            )
            for step in range(1, groups)
        }
        arrivals, mirrored = {}, {}

        def spread(index):
            rows = chunk_rows(index, me_m)
            source = outgoing.at[pl.ds(0, capacity)] if index == 0 else routed[1].at[me_t, rows]
            for turn, step in square:
                arrivals[index, turn, step] = push(
                    source, routed[index].at[me_t, rows], spread_sem[index], (turn, step),
                    square_device(turn, step),
                )
            mirrored[index, 0, 0] = push(
                source, routed[index].at[me_t, rows], mirror_sem[index], (0, 0), {"tp": partner}
            )

        def mirror(index):
            for turn, step in square:
                arrivals[index, turn, step].wait_recv()
                block = routed[index].at[
                    line_before(step) * 2 + core, chunk_rows(index, member(turn))
                ]
                mirrored[index, turn, step] = push(
                    block, block, mirror_sem[index], (turn, step), {"tp": partner}
                )

        def settle(index):
            for turn, step in [(0, 0)] + square:
                mirrored[index, turn, step].wait_recv()

        def expand(index):
            base = sum(set_rows[:index])
            rows = set_rows[index]

            def one_tile(number, carry):
                cols = pl.ds(pl.multiple_of(number * tile, tile), tile)
                gate_sum = jnp.zeros((rows, tile), f32)
                up_sum = jnp.zeros((rows, tile), f32)
                for shard in range(shards):
                    block = routed[index][shard]
                    deep = pl.ds(shard * width, width)
                    gate_sum += jnp.dot(block, gate_v[deep, cols], preferred_element_type=f32)
                    up_sum += jnp.dot(block, up_v[deep, cols], preferred_element_type=f32)
                hidden[pl.ds(base, rows), cols] = (
                    gate_sum / (1.0 + jnp.exp(-gate_sum)) * up_sum
                ).astype(bf16)
                return carry

            lax.fori_loop(0, hidden_units // tile, one_tile, 0)

        def down(index, shard):
            base = sum(set_rows[:index])
            return scale_ref[pl.ds(base, set_rows[index]), 0:1] * jnp.dot(
                hidden[pl.ds(base, set_rows[index])],
                down_v[:, pl.ds(pl.multiple_of(shard * width, width), width)],
                preferred_element_type=f32,
            )

        parts, returns = {}, {}
        line_order = list(range(1, lines)) + [0]

        def shrink(index):
            for step in line_order:
                part_send[index][step] = down(index, line_at(step) * 2 + 1 - core).astype(bf16)
                parts[index, step] = push(
                    part_send[index].at[step], part_recv[index].at[step], part_sem[index], (step,),
                    {"tp": partner},
                )
            for step in line_order:
                own = down(index, line_at(step) * 2 + core)
                parts[index, step].wait_recv()
                own = own + part_recv[index][step].astype(f32)
                give[index][step] = own.astype(bf16)
                for turn in (3, 2, 1, 0):
                    if turn == 0 and step == 0:
                        continue
                    returns[index, turn, step] = push(
                        give[index].at[step, chunk_rows(index, member(turn))],
                        take[index].at[turn, step], return_sem[index], (turn, step),
                        square_device(turn, step),
                    )
                if step == 0:
                    kept[index][...] = own

        def gather_up(index):
            total = kept[index][chunk_rows(index, me_m)]
            for turn, step in square:
                returns[index, turn, step].wait_recv()
                total = total + take[index][turn, step].astype(f32)
            return total

        with scope("weights_in"):
            for step in range(1, experts):
                shares[step].wait_recv()
        shared = [
            weight_recv[lax.rem(me_g - step + groups, groups) * EXP_GROUP + owner, 0:1]
            for step in range(groups)
            for owner in range(EXP_GROUP)
        ]
        shared.append(jnp.zeros((128 - experts, token_count), f32))
        shared = jnp.concatenate(shared, 0).T
        base = 0
        for index in range(len(sets)):
            for owner in range(EXP_GROUP):
                for step in [0] if index == 0 else range(1, groups):
                    column = step * EXP_GROUP + owner
                    scale_ref[pl.ds(base, capacity)] = jnp.broadcast_to(
                        shared[step * capacity : (step + 1) * capacity, column : column + 1],
                        (capacity, 128),
                    )
                    base += capacity
        with scope("spread0"):
            spread(0)
        if groups > 1:
            with scope("cross"):
                for step in range(1, groups):
                    crossings[step].wait_recv()
            spread(1)
        with scope("mirror0"):
            mirror(0)
        for load in loads[5:7]:
            load.wait()
        with scope("settle0"):
            settle(0)
        with scope("expand0"):
            expand(0)
        loads[7].wait()
        with scope("shrink0"):
            shrink(0)
        returned = []
        if groups > 1:
            with scope("mirror1"):
                mirror(1)
            with scope("settle1"):
                settle(1)
            with scope("expand1"):
                expand(1)
            with scope("shrink1"):
                shrink(1)
            with scope("gather0"):
                first = gather_up(0)
            with scope("gather1"):
                home[...] = gather_up(1).astype(bf16)
            backs = {
                step: push(
                    home.at[pl.ds((step - 1) * capacity, capacity)], returned_ref.at[step - 1],
                    back_sem, (step - 1,), group_device(-step),
                )
                for step in range(1, groups)
            }
            with scope("back"):
                for step in range(1, groups):
                    backs[step].wait_recv()
                    returned.append(returned_ref[step - 1].astype(f32))
        else:
            first = gather_up(0)
        second_sum = residual_scale * spread_rows.astype(f32) + jnp.concatenate([first] + returned, 0)
        with scope("norm2"):
            result_rows = normalize(second_sum, last_gain_ref[...], 1).astype(bf16)
        out_ref[...] = jnp.dot(back_ref[...], result_rows, preferred_element_type=f32).astype(bf16)
        for copy in sent:
            copy.wait_send()

    vmem = pl.BlockSpec(memory_space=pltpu.VMEM)
    hbm = pl.BlockSpec(memory_space=pltpu.HBM)
    dma = pltpu.SemaphoreType.DMA
    other = max(lines - 1, 1)
    return pl.pallas_call(
        kernel,
        out_shape=jax.ShapeDtypeStruct((token_count, width), bf16),
        in_specs=[hbm] * 16,
        out_specs=vmem,
        scratch_shapes=[
            pltpu.VMEM(row_table.shape, f32),
            pltpu.VMEM(column_table.shape, f32),
            pltpu.VMEM((1, HEAD_DIM), f32),
            pltpu.VMEM((1, HEAD_DIM), f32),
            pltpu.VMEM((1, width), f32),
            pltpu.VMEM((TOPK, token_count), jnp.int32),
            pltpu.VMEM((TOPK, token_count), f32),
            pltpu.VMEM((1, width), f32),
            dma((8,)),
            pltpu.VMEM(queries.shape, bf16),
            pltpu.VMEM(key_rows.shape, bf16),
            pltpu.VMEM(value_rows.shape, bf16),
            pltpu.VMEM(residual.shape, bf16),
            pltpu.VMEM(out_weight.shape, bf16),
            pltpu.VMEM(gate_weight.shape[1:], bf16),
            pltpu.VMEM(up_weight.shape[1:], bf16),
            pltpu.VMEM(down_weight.shape[1:], bf16),
            dma((8,)),
            pltpu.VMEM((experts, token_count, key_heads * pair_width), bf16),
            dma((2, ring_half, pieces)),
            dma((2, ring_half, pieces)),
            pltpu.VMEM((key_heads, query_rows, pair_width), bf16),
            pltpu.VMEM((key_heads, HEAD_DIM, query_rows), f32),
            pltpu.VMEM((key_heads, 1, query_rows), f32),
            pltpu.VMEM((key_heads, 1, query_rows), f32),
            pltpu.VMEM((token_count, key_heads * pair_width), bf16),
            pltpu.VMEM((lines, token_count, width), bf16),
            pltpu.VMEM((lines, token_count, width), bf16),
            pltpu.VMEM((other, token_count, width), bf16),
            pltpu.VMEM((other, token_count, width), bf16),
            dma((2, lines)),
            dma((2, other)),
            pltpu.VMEM((2, 8, token_count), f32),
            pltpu.VMEM((2, shards - 1, 8, token_count), f32),
            dma((2, 2, shards - 1)),
            pltpu.VMEM((token_count, token_count), bf16),
            pltpu.VMEM((token_count, token_count), bf16),
            pltpu.VMEM((experts, 8, token_count), f32),
            pltpu.VMEM((experts, 8, token_count), f32),
            dma((2, experts)),
            pltpu.VMEM((row_total, 128), f32),
            pltpu.VMEM((token_count, width), bf16),
            pltpu.VMEM((row_total, hidden_units), bf16),
            dma((2, max(groups - 1, 1))),
            pltpu.VMEM((sets[-1] * capacity, width), bf16),
            pltpu.VMEM((max(groups - 1, 1), capacity, width), bf16),
            dma((2, max(groups - 1, 1))),
        ]
        + [pltpu.VMEM((shards, rows, width), bf16) for rows in set_rows]
        + [dma((2, EXP_GROUP, lines))] * len(sets)
        + [dma((2, EXP_GROUP, lines))] * len(sets)
        + [pltpu.VMEM((lines, rows, width), bf16) for rows in set_rows]
        + [pltpu.VMEM((lines, rows, width), bf16) for rows in set_rows]
        + [dma((2, lines))] * len(sets)
        + [pltpu.VMEM((lines, rows, width), bf16) for rows in set_rows]
        + [
            pltpu.VMEM((EXP_GROUP, lines, blocks * capacity, width), bf16) for blocks in sets
        ]
        + [dma((2, EXP_GROUP, lines))] * len(sets)
        + [pltpu.VMEM((rows, width), f32) for rows in set_rows],
        compiler_params=pltpu.CompilerParams(
            collective_id=0, has_side_effects=True, vmem_limit_bytes=58 << 20
        ),
    )(
        row_table, column_table, query_gain.reshape(1, -1), key_gain.reshape(1, -1),
        norm_gain.reshape(1, -1), expert_ids.T, route_weights.T,
        final_gain.reshape(1, -1), queries, key_rows, value_rows, residual, out_weight,
        gate_weight, up_weight, down_weight,
    )


def per_device(
    queries,
    projected_key_rows,
    projected_value_rows,
    query_gain,
    key_norm_gain,
    residual,
    out_weight,
    norm_gain,
    expert_ids,
    route_weights,
    gate_weight,
    up_weight,
    down_weight,
    final_gain,
):
    token_total = queries.shape[0] * lax.axis_size("sp")
    row_table, column_table = rotary_tables(-(-token_total // GRID_W))
    return layer(
        queries,
        projected_key_rows,
        projected_value_rows,
        row_table,
        column_table,
        query_gain,
        key_norm_gain,
        out_weight,
        residual,
        norm_gain,
        expert_ids,
        route_weights,
        gate_weight,
        up_weight,
        down_weight,
        final_gain,
        lax.axis_size("sp"),
        lax.axis_size("tp"),
    )


def solution(mesh):
    in_specs = (
        P("sp", "tp"),
        P("sp", "tp"),
        P("sp", "tp"),
        P(),
        P(),
        P("sp", "tp"),
        P("tp", None),
        P("tp"),
        P("sp", None),
        P("sp", None),
        P("sp", None, "tp"),
        P("sp", None, "tp"),
        P("sp", "tp", None),
        P("tp"),
    )
    out_specs = P("sp", "tp")
    return jax.shard_map(
        per_device, mesh=mesh, in_specs=in_specs, out_specs=out_specs, check_vma=False
    )
```

```python
import contextlib

import jax
import jax.numpy as jnp
import numpy as np
from jax import lax
from jax.experimental import pallas as pl
from jax.experimental.pallas import tpu as pltpu
from jax.sharding import PartitionSpec as P

D = 2048
HEAD_DIM = 64
GRID_W = 64
EXP_GROUP = 4
TOPK = 2


theta_base = 10000.0
norm_epsilon = 1e-06
residual_scale = 8.0**0.25
far_below = -1e30
MESH = pl.DeviceIdType.MESH
SCOPES = False


def scope(name):
    return jax.named_scope(name) if SCOPES else contextlib.nullcontext()


def rotary_tables(grid_rows):
    quarter = HEAD_DIM // 4
    lane = np.arange(2 * HEAD_DIM)
    frequency = theta_base ** (-(lane % quarter) * 2.0 / (HEAD_DIM // 2))
    sign = np.where(lane % (2 * quarter) < quarter, -1.0, 1.0)
    by_row = lane % HEAD_DIM < HEAD_DIM // 2

    def tables(positions):
        angles = positions[:, None] * frequency[None, :].astype(np.float32).astype(np.float64)
        return np.stack([np.cos(angles), np.sin(angles) * sign[None, :]]).astype(np.float32)

    rows = np.where(by_row[None, None, :], tables(np.arange(grid_rows)), 0.0)
    columns = np.where(by_row[None, None, :], 0.0, tables(np.arange(GRID_W)))
    return rows.astype(np.float32), columns.astype(np.float32)


def place_of(index, group, group_minor):
    major = group // group_minor
    high, low = index // group_minor, lax.rem(index, group_minor)
    if group_minor == 1:
        return high
    back = major - 1 - high
    odd = lax.rem(back, 2)
    inner = (low - 1) * (1 - odd) + (group_minor - 1 - low) * odd
    first = jnp.where(low == 0, 1, 0)
    return first * high + (1 - first) * (major + back * (group_minor - 1) + inner)


def device_at(place, group, group_minor):
    major = group // group_minor
    if group_minor == 1:
        return place
    first = jnp.where(place < major, 1, 0)
    rest = jnp.maximum(place - major, 0)
    back = rest // (group_minor - 1)
    inner = lax.rem(rest, group_minor - 1)
    odd = lax.rem(back, 2)
    low = 1 + inner * (1 - odd) + (group_minor - 2 - inner) * odd
    other = (major - 1 - back) * group_minor + low
    return first * (place * group_minor) + (1 - first) * other


def layer(
    queries, key_rows, value_rows, row_table, column_table, query_gain, key_gain, out_weight, residual,
    norm_gain, expert_ids, route_weights, gate_weight, up_weight, down_weight, final_gain, experts,
    shards,
):
    token_count, width = residual.shape
    key_heads = key_rows.shape[1] // HEAD_DIM
    pair_width = 2 * HEAD_DIM
    query_rows = 2 * token_count
    ring_minor = 1 << ((experts.bit_length() - 1) // 2)
    ring_half = experts // 2
    pieces = 8
    piece = token_count // pieces
    lines = shards // 2
    groups = experts // EXP_GROUP
    capacity = token_count // groups
    splits = 2 if capacity % 32 == 0 else 1
    stretch = capacity // splits
    sets = [([0], part) for part in range(splits)]
    if groups > 1:
        sets += [(list(range(1, groups)), part) for part in range(splits)]
    away_sets = range(splits, len(sets))
    member_rows = [len(steps) * stretch for steps, _ in sets]
    set_rows = [EXP_GROUP * rows for rows in member_rows]
    row_total = sum(set_rows)
    hidden_units = gate_weight.shape[2]
    tile = min(256, hidden_units)
    feature_total = width * shards
    bf16, f32 = jnp.bfloat16, jnp.float32

    def kernel(
        row_hbm, column_hbm, q_gain_hbm, k_gain_hbm, gain_hbm, ids_hbm, rw_hbm, last_gain_hbm,
        q_hbm, k_hbm, v_hbm, res_hbm, ow_hbm, gate_hbm, up_hbm, down_hbm, out_ref,
        row_ref, column_ref, q_gain_ref, k_gain_ref, gain_ref, ids_ref, rw_ref, last_gain_ref,
        small_sem, q_v, k_v, v_v, res_ref, ow_ref, gate_v, up_v, down_v, weight_sem,
        send_sem, ring_ref, ring_recv, q_pad, flash_out, flash_max, flash_sum, att_ref,
        mix_send, mix_pair, line_send, line_recv, mix_sem, line_sem,
        stat_send, stat_recv, stat_sem,
        perm_ref, back_ref, weight_send, weight_recv, share_sem, scale_ref, outgoing, hidden,
        cross_sem, spread_sem, mirror_sem, part_sem, return_sem, home, returned_ref, back_sem,
        *per_set,
    ):
        count = len(sets)
        routed, part_send, part_recv, give, take, kept = [
            per_set[i * count : (i + 1) * count] for i in range(6)
        ]
        me_s = lax.axis_index("sp")
        me_t = lax.axis_index("tp")
        line = me_t // 2
        core = lax.rem(me_t, 2)
        partner = line * 2 + 1 - core

        def line_at(step):
            return lax.rem(line + step, lines)

        me_g = me_s // EXP_GROUP
        me_m = lax.rem(me_s, EXP_GROUP)

        def member(turn):
            if turn == 0:
                return me_m
            if turn == 1:
                return me_m + 1 - 2 * lax.rem(me_m, 2)
            if turn == 2:
                return me_m + 2 - 4 * (me_m // 2)
            return EXP_GROUP - 1 - me_m

        def line_before(step):
            return lax.rem(line + lines - step, lines)

        def group_device(step):
            return {"sp": lax.rem(me_g + step + groups, groups) * EXP_GROUP + me_m}

        def square_device(turn, step):
            return {"sp": me_g * EXP_GROUP + member(turn), "tp": line_at(step) * 2 + core}

        barrier = pltpu.get_barrier_semaphore()
        for step in range(1, experts):
            pl.semaphore_signal(
                barrier, inc=1, device_id={"sp": lax.rem(me_s + step, experts)},
                device_id_type=MESH,
            )
        for step in range(1, shards):
            pl.semaphore_signal(
                barrier, inc=1, device_id={"tp": lax.rem(me_t + step, shards)},
                device_id_type=MESH,
            )
        for turn in range(1, EXP_GROUP):
            for step in range(1, lines):
                pl.semaphore_signal(
                    barrier, inc=1, device_id=square_device(turn, step), device_id_type=MESH
                )
        greeted = experts - 1 + shards - 1 + (EXP_GROUP - 1) * (lines - 1)
        loads = [
            pltpu.make_async_copy(src, dst, weight_sem.at[i])
            for i, (src, dst) in enumerate(
                (
                    (k_hbm, k_v), (v_hbm, v_v), (q_hbm, q_v), (ow_hbm, ow_ref), (res_hbm, res_ref),
                    (gate_hbm.at[0], gate_v), (up_hbm.at[0], up_v), (down_hbm.at[0], down_v),
                )
            )
        ]
        small_loads = [
            pltpu.make_async_copy(src, dst, small_sem.at[i])
            for i, (src, dst) in enumerate(
                (
                    (row_hbm, row_ref), (column_hbm, column_ref), (q_gain_hbm, q_gain_ref),
                    (k_gain_hbm, k_gain_ref), (gain_hbm, gain_ref), (ids_hbm, ids_ref),
                    (rw_hbm, rw_ref), (last_gain_hbm, last_gain_ref),
                )
            )
        ]
        for load in loads[:3] + small_loads:
            load.start()
        sent_bytes = dict.fromkeys(range(8), 0)

        def push(source, target, phase, recv_sem, device):
            copy = pltpu.make_async_remote_copy(
                src_ref=source, dst_ref=target, send_sem=send_sem.at[phase], recv_sem=recv_sem,
                device_id=device, device_id_type=MESH,
            )
            copy.start()
            sent_bytes[phase] += int(np.prod(source.shape)) * jnp.dtype(source.dtype).itemsize
            return copy

        def stretch_of(size):
            rows = size // (2 * hidden_units)
            assert rows * 2 * hidden_units == size and rows % 8 == 0 and rows <= feature_total
            return gate_v.at[pl.ds(0, rows)]

        def waiter(region, sems):
            return pltpu.make_async_remote_copy(
                src_ref=region, dst_ref=region, send_sem=sems, recv_sem=sems,
                device_id={"tp": partner}, device_id_type=MESH,
            )

        lane_pair = lax.broadcasted_iota(jnp.int32, (token_count, pair_width), 1)
        low_half = lane_pair < HEAD_DIM
        quarter = HEAD_DIM // 4
        turn_low = lane_pair % (2 * quarter) < quarter
        same_head = jnp.where(
            lax.broadcasted_iota(jnp.int32, (pair_width, pair_width), 0) // HEAD_DIM
            == lax.broadcasted_iota(jnp.int32, (pair_width, pair_width), 1) // HEAD_DIM,
            1.0, 0.0,
        ).astype(bf16)
        for load in small_loads:
            load.wait()
        for load in loads[:3]:
            load.wait()
        for load in loads[3:]:
            load.start()

        def rotary(part):
            blocks = []
            for line_of_grid in range(token_count // GRID_W):
                row = row_ref[part, pl.ds(me_s * (token_count // GRID_W) + line_of_grid, 1)]
                blocks.append(column_ref[part] + row)
            return jnp.concatenate(blocks, 0)

        cosine, sine = rotary(0), rotary(1)
        both_gains = [
            jnp.concatenate([ref[...]] * 2, 1) for ref in (q_gain_ref, k_gain_ref)
        ]

        def rotated(rows, gain):
            square = rows * rows
            high = square.astype(bf16)
            rest = (square - high.astype(f32)).astype(bf16)
            total = jnp.dot(high, same_head, preferred_element_type=f32) + jnp.dot(
                rest, same_head, preferred_element_type=f32
            )
            scaled = rows * lax.rsqrt(total / HEAD_DIM + norm_epsilon) * gain
            turned = jnp.where(
                turn_low,
                pltpu.roll(scaled, pair_width - quarter, 1),
                pltpu.roll(scaled, quarter, 1),
            )
            return scaled * cosine + turned * sine

        def swap(rows):
            return pltpu.roll(rows, HEAD_DIM, 1)

        for pair in range((key_heads + 1) // 2):
            if key_heads == 1:
                key_pair = jnp.concatenate([k_v[...]] * 2, 1).astype(f32)
                value_pair = jnp.concatenate([v_v[...]] * 2, 1).astype(f32)
            else:
                lanes = pl.ds(pair * pair_width, pair_width)
                key_pair = k_v[:, lanes].astype(f32)
                value_pair = v_v[:, lanes].astype(f32)
            key_pair = rotated(key_pair, both_gains[1])
            ring_ref[0, :, pl.ds(2 * pair * pair_width, pair_width)] = jnp.where(
                low_half, key_pair, swap(value_pair)
            ).astype(bf16)
            if key_heads > 1:
                ring_ref[0, :, pl.ds((2 * pair + 1) * pair_width, pair_width)] = jnp.where(
                    low_half, swap(key_pair), value_pair
                ).astype(bf16)
        spot = place_of(me_s, experts, ring_minor)
        right = device_at(lax.rem(spot + 1, experts), experts, ring_minor)
        left = device_at(lax.rem(spot + experts - 1, experts), experts, ring_minor)
        with scope("barrier"):
            pl.semaphore_wait(barrier, greeted)

        ring = {}

        def pass_on(hop, part):
            for way in range(2):
                if hop == ring_half and (part < pieces // 2) != (way == 0):
                    continue
                if hop > 1:
                    ring[way, hop - 1, part].wait_recv()
                span = pl.ds(part * piece, piece)
                source_slot = (hop - 1) if way == 0 else (experts - hop + 1) % experts
                target_slot = hop if way == 0 else experts - hop
                copy = push(
                    ring_ref.at[source_slot, span], ring_ref.at[target_slot, span], 0,
                    ring_recv.at[way, hop - 1, part], {"sp": right if way == 0 else left},
                )
                ring[way, hop, part] = copy

        def attend(slot, head, first):
            block = ring_ref[slot, :, pl.ds(head * pair_width, pair_width)]
            scores = lax.dot_general(
                block, q_pad[head], (((1,), (1,)), ((), ())), preferred_element_type=f32
            )
            peak = jnp.max(scores, 0, keepdims=True)
            if not first:
                peak = jnp.maximum(flash_max[head], peak)
            weights = jnp.exp(scores - peak)
            mass = jnp.sum(weights, 0, keepdims=True)
            gathered = lax.dot_general(
                block, weights.astype(bf16), (((0,), (0,)), ((), ())), preferred_element_type=f32
            )[HEAD_DIM:]
            if not first:
                fade = jnp.exp(flash_max[head] - peak)
                mass = mass + flash_sum[head] * fade
                gathered = gathered + flash_out[head] * fade
            flash_max[head] = peak
            flash_sum[head] = mass
            flash_out[head] = gathered

        def prepare(head):
            rows = rotated(
                q_v[:, pl.ds(head * pair_width, pair_width)].astype(f32), both_gains[0]
            ) * HEAD_DIM ** (-0.5)
            q_pad[head, pl.ds(0, token_count)] = jnp.where(low_half, rows, 0.0).astype(bf16)
            q_pad[head, pl.ds(token_count, token_count)] = jnp.where(
                low_half, swap(rows), 0.0
            ).astype(bf16)

        def columns_of(rows):
            return jnp.concatenate([rows] * (token_count // TOPK), 0).T

        lane = lax.broadcasted_iota(jnp.int32, (token_count, 128), 1)
        before = jnp.where(
            lax.broadcasted_iota(jnp.int32, (token_count, token_count), 1)
            < lax.broadcasted_iota(jnp.int32, (token_count, token_count), 0),
            1.0, 0.0,
        ).astype(bf16)

        def route():
            ids = columns_of(ids_ref[...].astype(f32)).astype(jnp.int32)
            routing = columns_of(rw_ref[...])
            group_of = ids[:, 0:1] // EXP_GROUP
            inside = jnp.where(lane == group_of, 1.0, 0.0)
            earlier = jnp.dot(before, inside.astype(bf16), preferred_element_type=f32)
            slot = jnp.sum(earlier * inside, 1, keepdims=True)
            away = lax.rem(group_of - me_g + groups, groups)
            place = (away * capacity).astype(f32) + slot
            place_row = jnp.where(lane == 0, place, 0.0).T[0:1].astype(jnp.int32)
            place = place.astype(jnp.int32)
            row_index = lax.broadcasted_iota(jnp.int32, (token_count, token_count), 0)
            picks = jnp.where(row_index == place_row, 1.0, 0.0)
            perm_ref[...] = picks.astype(bf16)
            back_ref[...] = jnp.where(
                lax.broadcasted_iota(jnp.int32, (token_count, token_count), 1) == place, 1.0, 0.0
            ).astype(bf16)
            by_expert = sum(
                jnp.where(lane == ids[:, k : k + 1], routing[:, k : k + 1], 0.0)
                for k in range(TOPK)
            )
            by_slot = jnp.dot(
                picks, by_expert, preferred_element_type=f32, precision=lax.Precision.HIGHEST
            ).T
            for expert in range(experts):
                weight_send[expert] = jnp.broadcast_to(
                    by_slot[expert : expert + 1], (8, token_count)
                )
            weight_recv[me_s] = weight_send[me_s]
            for step in range(1, experts):
                push(
                    weight_send.at[lax.rem(me_s + step, experts)], weight_recv.at[me_s], 1,
                    share_sem, {"sp": lax.rem(me_s + step, experts)},
                )

        waiting = []
        for part in range(pieces):
            pass_on(1, part)
        for head in range(key_heads):
            prepare(head)
        route()
        waiting += [(0, head, True) for head in range(key_heads)]
        for hop in range(2, ring_half + 1):
            for part in range(pieces):
                pass_on(hop, part)
                for _ in range(-(-len(waiting) // (pieces - part))):
                    attend(*waiting.pop(0))
            if hop < ring_half:
                for slot in (hop - 1, experts - hop + 1):
                    waiting += [(slot, head, False) for head in range(key_heads)]
        with scope("ring_tail"):
            for way in range(2):
                for part in range(pieces):
                    if (way, ring_half, part) not in ring:
                        ring[way, ring_half - 1, part].wait_recv()
        for slot in (ring_half - 1, ring_half + 1):
            for head in range(key_heads):
                attend(slot, head, False)
        with scope("ring_last"):
            for way in range(2):
                for part in range(pieces):
                    if (way, ring_half, part) in ring:
                        ring[way, ring_half, part].wait_recv()
        for head in range(key_heads):
            attend(ring_half, head, False)
        for head in range(key_heads):
            result_rows = flash_out[head] / flash_sum[head]
            att_ref[:, pl.ds(head * pair_width, pair_width)] = (
                jnp.concatenate([result_rows[:, :token_count], result_rows[:, token_count:]], 0)
                .T.astype(bf16)
            )
        attended_rows = att_ref[...]
        loads[3].wait()

        def mix(shard):
            return jnp.dot(
                attended_rows,
                ow_ref[:, pl.ds(pl.multiple_of(shard * width, width), width)],
                preferred_element_type=f32,
            )

        with scope("mix"):
            pass
        for step in range(lines):
            mix_send[step] = mix(line_at(step) * 2 + 1 - core).astype(bf16)
        pair = {}
        for step in list(range(1, lines)) + [0]:
            pair[step] = push(
                mix_send.at[step], mix_pair.at[step], 2, mix_sem.at[step], {"tp": partner}
            )
        across = {}
        for step in range(1, lines):
            mine = mix(line_at(step) * 2 + core)
            pair[step].wait_recv()
            line_send[step - 1] = (mine + mix_pair[step].astype(f32)).astype(bf16)
            across[step] = push(
                line_send.at[step - 1], line_recv.at[step - 1], 2, line_sem.at[step - 1],
                {"tp": line_at(step) * 2 + core},
            )
        total = mix(me_t)
        pair[0].wait_recv()
        total = total + mix_pair[0].astype(f32)
        loads[4].wait()
        total = total + residual_scale * res_ref[...].astype(f32)
        for step in range(1, lines):
            across[step].wait_recv()
            total = total + line_recv[step - 1].astype(f32)

        def normalize(values, gain, turn):
            sums = jnp.sum(values, 1, keepdims=True)
            squares = jnp.sum(values * values, 1, keepdims=True)
            both = jnp.where(lane == 0, sums, jnp.where(lane == 1, squares, 0.0)).T[:8]
            stat_send[turn] = both
            for step in range(1, shards):
                push(
                    stat_send.at[turn], stat_recv.at[turn, step - 1], 3, stat_sem.at[turn],
                    {"tp": lax.rem(me_t + step, shards)},
                )
            waiter(stat_recv.at[turn], stat_sem.at[turn]).wait_recv()
            for step in range(1, shards):
                both = both + stat_recv[turn, step - 1]
            columns = jnp.concatenate([both] * 16, 0).T
            center = columns[:, 0:1] / feature_total
            spread = columns[:, 1:2] / feature_total - center * center
            return (values - center) * lax.rsqrt(spread + norm_epsilon) * gain

        with scope("norm1"):
            normed = normalize(total, gain_ref[...], 0).astype(bf16)
        spread_rows = jnp.dot(perm_ref[...], normed, preferred_element_type=f32).astype(bf16)
        outgoing[...] = spread_rows
        square = [(turn, step) for turn in range(EXP_GROUP) for step in range(lines)]
        square.sort(key=lambda pair: -(pair[0] + 1) // 2 - min(pair[1], lines - pair[1]))
        square.remove((0, 0))

        def member_span(index, owner):
            count = member_rows[index]
            return pl.ds(pl.multiple_of(owner * count, count), count)

        crossings = {}
        for index in away_sets:
            for place, step in enumerate(sets[index][0]):
                crossings[index, step] = push(
                    outgoing.at[pl.ds(step * capacity + sets[index][1] * stretch, stretch)],
                    routed[index].at[
                        me_t,
                        pl.ds(
                            pl.multiple_of(
                                me_m * member_rows[index] + place * stretch, stretch
                            ),
                            stretch,
                        ),
                    ],
                    4, cross_sem.at[index - splits, place], group_device(step),
                )
        arrivals = {}

        def spread(index):
            rows = member_span(index, me_m)
            if index < splits:
                span = slice(index * stretch, (index + 1) * stretch)
                routed[index][me_t, rows] = spread_rows[span]
                source = outgoing.at[pl.ds(index * stretch, stretch)]
            else:
                for step in sets[index][0]:
                    crossings[index, step].wait_recv()
                source = routed[index].at[me_t, rows]
            for turn, step in square:
                arrivals[index, turn, step] = push(
                    source, routed[index].at[me_t, rows], 4, spread_sem.at[index, turn, step],
                    square_device(turn, step),
                )
            push(
                source, routed[index].at[me_t, rows], 5, mirror_sem.at[index], {"tp": partner}
            )

        def mirror(index):
            for turn, step in square:
                arrivals[index, turn, step].wait_recv()
                block = routed[index].at[
                    line_before(step) * 2 + core, member_span(index, member(turn))
                ]
                push(block, block, 5, mirror_sem.at[index], {"tp": partner})

        def settle(index):
            size = lines * set_rows[index] * width * 2
            waiter(stretch_of(size), mirror_sem.at[index]).wait_recv()

        def expand(index):
            base = sum(set_rows[:index])
            rows = set_rows[index]

            def one_tile(number, carry):
                cols = pl.ds(pl.multiple_of(number * tile, tile), tile)
                gate_sum = jnp.zeros((rows, tile), f32)
                up_sum = jnp.zeros((rows, tile), f32)
                for shard in range(shards):
                    block = routed[index][shard]
                    deep = pl.ds(shard * width, width)
                    gate_sum += jnp.dot(block, gate_v[deep, cols], preferred_element_type=f32)
                    up_sum += jnp.dot(block, up_v[deep, cols], preferred_element_type=f32)
                hidden[pl.ds(base, rows), cols] = (
                    gate_sum / (1.0 + jnp.exp(-gate_sum)) * up_sum
                ).astype(bf16)
                return carry

            lax.fori_loop(0, hidden_units // tile, one_tile, 0)

        def down(index, shard):
            base = sum(set_rows[:index])
            return scale_ref[pl.ds(base, set_rows[index]), 0:1] * jnp.dot(
                hidden[pl.ds(base, set_rows[index])],
                down_v[:, pl.ds(pl.multiple_of(shard * width, width), width)],
                preferred_element_type=f32,
            )

        parts = {}
        line_order = list(range(1, lines)) + [0]

        def shrink(index):
            for step in line_order:
                part_send[index][step] = down(index, line_at(step) * 2 + 1 - core).astype(bf16)
                parts[index, step] = push(
                    part_send[index].at[step], part_recv[index].at[step], 6,
                    part_sem.at[index, step], {"tp": partner},
                )
            for step in line_order:
                own = down(index, line_at(step) * 2 + core)
                parts[index, step].wait_recv()
                own = own + part_recv[index][step].astype(f32)
                give[index][step] = own.astype(bf16)
                for turn in (3, 2, 1, 0):
                    if turn == 0 and step == 0:
                        continue
                    push(
                        give[index].at[step, member_span(index, member(turn))],
                        take[index].at[turn, step], 7, return_sem.at[index],
                        square_device(turn, step),
                    )
                if step == 0:
                    kept[index][...] = own

        def gather_up(index):
            total = kept[index][member_span(index, me_m)]
            size = len(square) * member_rows[index] * width * 2
            waiter(stretch_of(size), return_sem.at[index]).wait_recv()
            for turn, step in square:
                total = total + take[index][turn, step].astype(f32)
            return total

        for index in range(splits):
            spread(index)
        with scope("weights_in"):
            waiter(weight_recv.at[pl.ds(0, experts - 1)], share_sem).wait_recv()
        shared = [
            weight_recv[lax.rem(me_g - step + groups, groups) * EXP_GROUP + owner, 0:1]
            for step in range(groups)
            for owner in range(EXP_GROUP)
        ]
        shared.append(jnp.zeros((128 - experts, token_count), f32))
        shared = jnp.concatenate(shared, 0).T
        base = 0
        for steps, part in sets:
            for owner in range(EXP_GROUP):
                for step in steps:
                    column = step * EXP_GROUP + owner
                    top = step * capacity + part * stretch
                    scale_ref[pl.ds(base, stretch)] = jnp.broadcast_to(
                        shared[top : top + stretch, column : column + 1], (stretch, 128)
                    )
                    base += stretch
        for index in away_sets:
            with scope(f"cross{index}"):
                spread(index)
        with scope("mirror0"):
            mirror(0)
        with scope("weights"):
            for load in loads[5:]:
                load.wait()
        for index in range(len(sets)):
            with scope(f"settle{index}"):
                settle(index)
            with scope(f"expand{index}"):
                expand(index)
            if index + 1 < len(sets):
                with scope(f"mirror{index + 1}"):
                    mirror(index + 1)
            with scope(f"shrink{index}"):
                shrink(index)
        with scope("gatherA"):
            combined = [gather_up(index) for index in range(splits)]
        backs = {}
        for index in away_sets:
            with scope(f"gather{index}"):
                home[index - splits] = gather_up(index).astype(bf16)
            for place, step in enumerate(sets[index][0]):
                backs[step, sets[index][1]] = push(
                    home.at[index - splits, pl.ds(place * stretch, stretch)],
                    returned_ref.at[step - 1, pl.ds(sets[index][1] * stretch, stretch)],
                    7, back_sem.at[index - splits, place], group_device(-step),
                )
        with scope("back"):
            for step in range(1, groups):
                for part in range(splits):
                    backs[step, part].wait_recv()
                combined.append(returned_ref[step - 1].astype(f32))
        second_sum = residual_scale * spread_rows.astype(f32) + jnp.concatenate(combined, 0)
        with scope("norm2"):
            result_rows = normalize(second_sum, last_gain_ref[...], 1).astype(bf16)
        out_ref[...] = jnp.dot(back_ref[...], result_rows, preferred_element_type=f32).astype(bf16)
        with scope("sendwait"):
            regions = {
                0: ring_ref.at[pl.ds(1, experts - 1)], 1: weight_recv.at[pl.ds(1, experts - 1)],
                3: stat_recv,
            }
            for phase in range(8):
                region = regions[phase] if phase in regions else stretch_of(sent_bytes[phase])
                size = int(np.prod(region.shape)) * jnp.dtype(region.dtype).itemsize
                assert size == sent_bytes[phase]
                waiter(region, send_sem.at[phase]).wait_send()

    vmem = pl.BlockSpec(memory_space=pltpu.VMEM)
    hbm = pl.BlockSpec(memory_space=pltpu.HBM)
    dma = pltpu.SemaphoreType.DMA
    other = max(lines - 1, 1)
    return pl.pallas_call(
        kernel,
        out_shape=pltpu.VMEM((token_count, width), bf16),
        in_specs=[hbm] * 16,
        out_specs=vmem,
        scratch_shapes=[
            pltpu.VMEM(row_table.shape, f32),
            pltpu.VMEM(column_table.shape, f32),
            pltpu.VMEM((1, HEAD_DIM), f32),
            pltpu.VMEM((1, HEAD_DIM), f32),
            pltpu.VMEM((1, width), f32),
            pltpu.VMEM((TOPK, token_count), jnp.int32),
            pltpu.VMEM((TOPK, token_count), f32),
            pltpu.VMEM((1, width), f32),
            dma((8,)),
            pltpu.VMEM(queries.shape, bf16),
            pltpu.VMEM(key_rows.shape, bf16),
            pltpu.VMEM(value_rows.shape, bf16),
            pltpu.VMEM(residual.shape, bf16),
            pltpu.VMEM(out_weight.shape, bf16),
            pltpu.VMEM(gate_weight.shape[1:], bf16),
            pltpu.VMEM(up_weight.shape[1:], bf16),
            pltpu.VMEM(down_weight.shape[1:], bf16),
            dma((8,)),
            dma((8,)),
            pltpu.VMEM((experts, token_count, key_heads * pair_width), bf16),
            dma((2, ring_half, pieces)),
            pltpu.VMEM((key_heads, query_rows, pair_width), bf16),
            pltpu.VMEM((key_heads, HEAD_DIM, query_rows), f32),
            pltpu.VMEM((key_heads, 1, query_rows), f32),
            pltpu.VMEM((key_heads, 1, query_rows), f32),
            pltpu.VMEM((token_count, key_heads * pair_width), bf16),
            pltpu.VMEM((lines, token_count, width), bf16),
            pltpu.VMEM((lines, token_count, width), bf16),
            pltpu.VMEM((other, token_count, width), bf16),
            pltpu.VMEM((other, token_count, width), bf16),
            dma((lines,)),
            dma((other,)),
            pltpu.VMEM((2, 8, token_count), f32),
            pltpu.VMEM((2, shards - 1, 8, token_count), f32),
            dma((2,)),
            pltpu.VMEM((token_count, token_count), bf16),
            pltpu.VMEM((token_count, token_count), bf16),
            pltpu.VMEM((experts, 8, token_count), f32),
            pltpu.VMEM((experts, 8, token_count), f32),
            dma,
            pltpu.VMEM((row_total, 128), f32),
            pltpu.VMEM((token_count, width), bf16),
            pltpu.VMEM((row_total, hidden_units), bf16),
            dma((splits, max(groups - 1, 1))),
            dma((len(sets), EXP_GROUP, lines)),
            dma((len(sets),)),
            dma((len(sets), lines)),
            dma((len(sets),)),
            pltpu.VMEM((splits, member_rows[-1], width), bf16),
            pltpu.VMEM((max(groups - 1, 1), capacity, width), bf16),
            dma((splits, max(groups - 1, 1))),
        ]
        + [pltpu.VMEM((shards, rows, width), bf16) for rows in set_rows]
        + [pltpu.VMEM((lines, rows, width), bf16) for rows in set_rows] * 3
        + [pltpu.VMEM((EXP_GROUP, lines, rows, width), bf16) for rows in member_rows]
        + [pltpu.VMEM((rows, width), f32) for rows in set_rows],
        compiler_params=pltpu.CompilerParams(
            collective_id=0, has_side_effects=True, vmem_limit_bytes=48 << 20
        ),
    )(
        *(
            pltpu.with_memory_space_constraint(array, pltpu.HBM)
            for array in (
                jnp.asarray(row_table), jnp.asarray(column_table), query_gain.reshape(1, -1),
                key_gain.reshape(1, -1), norm_gain.reshape(1, -1), expert_ids.T, route_weights.T,
                final_gain.reshape(1, -1), queries, key_rows, value_rows, residual, out_weight,
                gate_weight, up_weight, down_weight,
            )
        )
    )


def per_device(
    queries,
    projected_key_rows,
    projected_value_rows,
    query_gain,
    key_norm_gain,
    residual,
    out_weight,
    norm_gain,
    expert_ids,
    route_weights,
    gate_weight,
    up_weight,
    down_weight,
    final_gain,
):
    token_total = queries.shape[0] * lax.axis_size("sp")
    row_table, column_table = rotary_tables(-(-token_total // GRID_W))
    return layer(
        queries,
        projected_key_rows,
        projected_value_rows,
        row_table,
        column_table,
        query_gain,
        key_norm_gain,
        out_weight,
        residual,
        norm_gain,
        expert_ids,
        route_weights,
        gate_weight,
        up_weight,
        down_weight,
        final_gain,
        lax.axis_size("sp"),
        lax.axis_size("tp"),
    )


def solution(mesh):
    in_specs = (
        P("sp", "tp"),
        P("sp", "tp"),
        P("sp", "tp"),
        P(),
        P(),
        P("sp", "tp"),
        P("tp", None),
        P("tp"),
        P("sp", None),
        P("sp", None),
        P("sp", None, "tp"),
        P("sp", None, "tp"),
        P("sp", "tp", None),
        P("tp"),
    )
    out_specs = P("sp", "tp")
    return jax.shard_map(
        per_device, mesh=mesh, in_specs=in_specs, out_specs=out_specs, check_vma=False
    )
```

```python
import contextlib

import jax
import jax.numpy as jnp
import numpy as np
from jax import lax
from jax.experimental import pallas as pl
from jax.experimental.pallas import tpu as pltpu
from jax.sharding import PartitionSpec as P

D = 2048
HEAD_DIM = 64
GRID_W = 64
EXP_GROUP = 4
TOPK = 2


theta_base = 10000.0
norm_epsilon = 1e-06
residual_scale = 8.0**0.25
far_below = -1e30
MESH = pl.DeviceIdType.MESH
SCOPES = False


def scope(name):
    return jax.named_scope(name) if SCOPES else contextlib.nullcontext()


def rotary_tables(grid_rows):
    quarter = HEAD_DIM // 4
    lane = np.arange(2 * HEAD_DIM)
    frequency = theta_base ** (-(lane % quarter) * 2.0 / (HEAD_DIM // 2))
    sign = np.where(lane % (2 * quarter) < quarter, -1.0, 1.0)
    by_row = lane % HEAD_DIM < HEAD_DIM // 2

    def tables(positions):
        angles = positions[:, None] * frequency[None, :].astype(np.float32).astype(np.float64)
        return np.stack([np.cos(angles), np.sin(angles) * sign[None, :]]).astype(np.float32)

    rows = np.where(by_row[None, None, :], tables(np.arange(grid_rows)), 0.0)
    columns = np.where(by_row[None, None, :], 0.0, tables(np.arange(GRID_W)))
    return rows.astype(np.float32), columns.astype(np.float32)


def place_of(index, group, group_minor):
    major = group // group_minor
    high, low = index // group_minor, lax.rem(index, group_minor)
    if group_minor == 1:
        return high
    back = major - 1 - high
    odd = lax.rem(back, 2)
    inner = (low - 1) * (1 - odd) + (group_minor - 1 - low) * odd
    first = jnp.where(low == 0, 1, 0)
    return first * high + (1 - first) * (major + back * (group_minor - 1) + inner)


def device_at(place, group, group_minor):
    major = group // group_minor
    if group_minor == 1:
        return place
    first = jnp.where(place < major, 1, 0)
    rest = jnp.maximum(place - major, 0)
    back = rest // (group_minor - 1)
    inner = lax.rem(rest, group_minor - 1)
    odd = lax.rem(back, 2)
    low = 1 + inner * (1 - odd) + (group_minor - 2 - inner) * odd
    other = (major - 1 - back) * group_minor + low
    return first * (place * group_minor) + (1 - first) * other


def layer(
    queries, key_rows, value_rows, row_table, column_table, query_gain, key_gain, out_weight, residual,
    norm_gain, expert_ids, route_weights, gate_weight, up_weight, down_weight, final_gain, experts,
    shards,
):
    token_count, width = residual.shape
    key_heads = key_rows.shape[1] // HEAD_DIM
    pair_width = 2 * HEAD_DIM
    query_rows = 2 * token_count
    ring_minor = 1 << ((experts.bit_length() - 1) // 2)
    ring_half = experts // 2
    pieces = 8
    piece = token_count // pieces
    lines = shards // 2
    groups = experts // EXP_GROUP
    capacity = token_count // groups
    splits = 2 if capacity % 32 == 0 else 1
    stretch = capacity // splits
    near_sets = [([0], part) for part in range(splits)]
    far_sets = [(list(range(1, groups)), part) for part in range(splits)] if groups > 1 else []
    sets = near_sets[:1] + far_sets + near_sets[1:]
    home_sets = [index for index, (steps, _) in enumerate(sets) if steps == [0]]
    away_sets = [index for index, (steps, _) in enumerate(sets) if steps != [0]]
    far_rows = (groups - 1) * stretch if groups > 1 else stretch
    member_rows = [len(steps) * stretch for steps, _ in sets]
    set_rows = [EXP_GROUP * rows for rows in member_rows]
    row_total = sum(set_rows)
    hidden_units = gate_weight.shape[2]
    tile = min(256, hidden_units)
    feature_total = width * shards
    bf16, f32 = jnp.bfloat16, jnp.float32

    def kernel(
        row_hbm, column_hbm, q_gain_hbm, k_gain_hbm, gain_hbm, ids_hbm, rw_hbm, last_gain_hbm,
        q_hbm, k_hbm, v_hbm, res_hbm, ow_hbm, gate_hbm, up_hbm, down_hbm, out_ref,
        row_ref, column_ref, q_gain_ref, k_gain_ref, gain_ref, ids_ref, rw_ref, last_gain_ref,
        small_sem, q_v, k_v, v_v, res_ref, ow_ref, gate_v, up_v, down_v, weight_sem,
        send_sem, ring_ref, ring_recv, q_pad, flash_out, flash_max, flash_sum, att_ref,
        mix_send, mix_pair, line_send, line_recv, mix_sem, line_sem,
        stat_send, stat_recv, stat_sem,
        perm_ref, back_ref, weight_send, weight_recv, share_sem, scale_ref, outgoing, hidden,
        cross_sem, spread_sem, mirror_sem, part_sem, return_sem, home, returned_ref, back_sem,
        *per_set,
    ):
        count = len(sets)
        routed, part_send, part_recv, give, take, kept, own_sum = [
            per_set[i * count : (i + 1) * count] for i in range(7)
        ]
        me_s = lax.axis_index("sp")
        me_t = lax.axis_index("tp")
        line = me_t // 2
        core = lax.rem(me_t, 2)
        partner = line * 2 + 1 - core

        def line_at(step):
            return lax.rem(line + step, lines)

        me_g = me_s // EXP_GROUP
        me_m = lax.rem(me_s, EXP_GROUP)

        def member(turn):
            if turn == 0:
                return me_m
            if turn == 1:
                return me_m + 1 - 2 * lax.rem(me_m, 2)
            if turn == 2:
                return me_m + 2 - 4 * (me_m // 2)
            return EXP_GROUP - 1 - me_m

        def line_before(step):
            return lax.rem(line + lines - step, lines)

        def group_device(step):
            return {"sp": lax.rem(me_g + step + groups, groups) * EXP_GROUP + me_m}

        def square_device(turn, step):
            return {"sp": me_g * EXP_GROUP + member(turn), "tp": line_at(step) * 2 + core}

        barrier = pltpu.get_barrier_semaphore()
        for step in range(1, experts):
            pl.semaphore_signal(
                barrier, inc=1, device_id={"sp": lax.rem(me_s + step, experts)},
                device_id_type=MESH,
            )
        for step in range(1, shards):
            pl.semaphore_signal(
                barrier, inc=1, device_id={"tp": lax.rem(me_t + step, shards)},
                device_id_type=MESH,
            )
        for turn in range(1, EXP_GROUP):
            for step in range(1, lines):
                pl.semaphore_signal(
                    barrier, inc=1, device_id=square_device(turn, step), device_id_type=MESH
                )
        greeted = experts - 1 + shards - 1 + (EXP_GROUP - 1) * (lines - 1)
        loads = [
            pltpu.make_async_copy(src, dst, weight_sem.at[i])
            for i, (src, dst) in enumerate(
                (
                    (k_hbm, k_v), (v_hbm, v_v), (q_hbm, q_v), (ow_hbm, ow_ref), (res_hbm, res_ref),
                    (gate_hbm.at[0], gate_v), (up_hbm.at[0], up_v), (down_hbm.at[0], down_v),
                )
            )
        ]
        small_loads = [
            pltpu.make_async_copy(src, dst, small_sem.at[i])
            for i, (src, dst) in enumerate(
                (
                    (row_hbm, row_ref), (column_hbm, column_ref), (q_gain_hbm, q_gain_ref),
                    (k_gain_hbm, k_gain_ref), (gain_hbm, gain_ref), (ids_hbm, ids_ref),
                    (rw_hbm, rw_ref), (last_gain_hbm, last_gain_ref),
                )
            )
        ]
        for load in loads[:3] + small_loads:
            load.start()
        sent_bytes = dict.fromkeys(range(8), 0)

        def push(source, target, phase, recv_sem, device):
            copy = pltpu.make_async_remote_copy(
                src_ref=source, dst_ref=target, send_sem=send_sem.at[phase], recv_sem=recv_sem,
                device_id=device, device_id_type=MESH,
            )
            copy.start()
            sent_bytes[phase] += int(np.prod(source.shape)) * jnp.dtype(source.dtype).itemsize
            return copy

        def stretch_of(size):
            rows = size // (2 * hidden_units)
            assert rows * 2 * hidden_units == size and rows % 8 == 0 and rows <= feature_total
            return gate_v.at[pl.ds(0, rows)]

        def waiter(region, sems):
            return pltpu.make_async_remote_copy(
                src_ref=region, dst_ref=region, send_sem=sems, recv_sem=sems,
                device_id={"tp": partner}, device_id_type=MESH,
            )

        lane_pair = lax.broadcasted_iota(jnp.int32, (token_count, pair_width), 1)
        low_half = lane_pair < HEAD_DIM
        quarter = HEAD_DIM // 4
        turn_low = lane_pair % (2 * quarter) < quarter
        same_head = jnp.where(
            lax.broadcasted_iota(jnp.int32, (pair_width, pair_width), 0) // HEAD_DIM
            == lax.broadcasted_iota(jnp.int32, (pair_width, pair_width), 1) // HEAD_DIM,
            1.0, 0.0,
        ).astype(bf16)
        for load in small_loads:
            load.wait()
        for load in loads[:3]:
            load.wait()
        for load in loads[3:]:
            load.start()

        def rotary(part):
            blocks = []
            for line_of_grid in range(token_count // GRID_W):
                row = row_ref[part, pl.ds(me_s * (token_count // GRID_W) + line_of_grid, 1)]
                blocks.append(column_ref[part] + row)
            return jnp.concatenate(blocks, 0)

        cosine, sine = rotary(0), rotary(1)
        both_gains = [
            jnp.concatenate([ref[...]] * 2, 1) for ref in (q_gain_ref, k_gain_ref)
        ]

        def rotated(rows, gain):
            square = rows * rows
            high = square.astype(bf16)
            rest = (square - high.astype(f32)).astype(bf16)
            total = jnp.dot(high, same_head, preferred_element_type=f32) + jnp.dot(
                rest, same_head, preferred_element_type=f32
            )
            scaled = rows * lax.rsqrt(total / HEAD_DIM + norm_epsilon) * gain
            turned = jnp.where(
                turn_low,
                pltpu.roll(scaled, pair_width - quarter, 1),
                pltpu.roll(scaled, quarter, 1),
            )
            return scaled * cosine + turned * sine

        def swap(rows):
            return pltpu.roll(rows, HEAD_DIM, 1)

        for pair in range((key_heads + 1) // 2):
            if key_heads == 1:
                key_pair = jnp.concatenate([k_v[...]] * 2, 1).astype(f32)
                value_pair = jnp.concatenate([v_v[...]] * 2, 1).astype(f32)
            else:
                lanes = pl.ds(pair * pair_width, pair_width)
                key_pair = k_v[:, lanes].astype(f32)
                value_pair = v_v[:, lanes].astype(f32)
            key_pair = rotated(key_pair, both_gains[1])
            ring_ref[0, :, pl.ds(2 * pair * pair_width, pair_width)] = jnp.where(
                low_half, key_pair, swap(value_pair)
            ).astype(bf16)
            if key_heads > 1:
                ring_ref[0, :, pl.ds((2 * pair + 1) * pair_width, pair_width)] = jnp.where(
                    low_half, swap(key_pair), value_pair
                ).astype(bf16)
        spot = place_of(me_s, experts, ring_minor)
        right = device_at(lax.rem(spot + 1, experts), experts, ring_minor)
        left = device_at(lax.rem(spot + experts - 1, experts), experts, ring_minor)
        with scope("barrier"):
            pl.semaphore_wait(barrier, greeted)

        ring = {}

        def pass_on(hop, part):
            for way in range(2):
                if hop == ring_half and (part < pieces // 2) != (way == 0):
                    continue
                if hop > 1:
                    ring[way, hop - 1, part].wait_recv()
                span = pl.ds(part * piece, piece)
                source_slot = (hop - 1) if way == 0 else (experts - hop + 1) % experts
                target_slot = hop if way == 0 else experts - hop
                copy = push(
                    ring_ref.at[source_slot, span], ring_ref.at[target_slot, span], 0,
                    ring_recv.at[way, hop - 1, part], {"sp": right if way == 0 else left},
                )
                ring[way, hop, part] = copy

        def attend(slot, head, first):
            block = ring_ref[slot, :, pl.ds(head * pair_width, pair_width)]
            scores = lax.dot_general(
                block, q_pad[head], (((1,), (1,)), ((), ())), preferred_element_type=f32
            )
            peak = jnp.max(scores, 0, keepdims=True)
            if not first:
                peak = jnp.maximum(flash_max[head], peak)
            weights = jnp.exp(scores - peak)
            mass = jnp.sum(weights, 0, keepdims=True)
            gathered = lax.dot_general(
                block, weights.astype(bf16), (((0,), (0,)), ((), ())), preferred_element_type=f32
            )[HEAD_DIM:]
            if not first:
                fade = jnp.exp(flash_max[head] - peak)
                mass = mass + flash_sum[head] * fade
                gathered = gathered + flash_out[head] * fade
            flash_max[head] = peak
            flash_sum[head] = mass
            flash_out[head] = gathered

        def prepare(head):
            rows = rotated(
                q_v[:, pl.ds(head * pair_width, pair_width)].astype(f32), both_gains[0]
            ) * HEAD_DIM ** (-0.5)
            q_pad[head, pl.ds(0, token_count)] = jnp.where(low_half, rows, 0.0).astype(bf16)
            q_pad[head, pl.ds(token_count, token_count)] = jnp.where(
                low_half, swap(rows), 0.0
            ).astype(bf16)

        def columns_of(rows):
            return jnp.concatenate([rows] * (token_count // TOPK), 0).T

        lane = lax.broadcasted_iota(jnp.int32, (token_count, 128), 1)
        before = jnp.where(
            lax.broadcasted_iota(jnp.int32, (token_count, token_count), 1)
            < lax.broadcasted_iota(jnp.int32, (token_count, token_count), 0),
            1.0, 0.0,
        ).astype(bf16)

        def route():
            ids = columns_of(ids_ref[...].astype(f32)).astype(jnp.int32)
            routing = columns_of(rw_ref[...])
            group_of = ids[:, 0:1] // EXP_GROUP
            inside = jnp.where(lane == group_of, 1.0, 0.0)
            earlier = jnp.dot(before, inside.astype(bf16), preferred_element_type=f32)
            slot = jnp.sum(earlier * inside, 1, keepdims=True)
            away = lax.rem(group_of - me_g + groups, groups)
            place = (away * capacity).astype(f32) + slot
            place_row = jnp.where(lane == 0, place, 0.0).T[0:1].astype(jnp.int32)
            place = place.astype(jnp.int32)
            row_index = lax.broadcasted_iota(jnp.int32, (token_count, token_count), 0)
            picks = jnp.where(row_index == place_row, 1.0, 0.0)
            perm_ref[...] = picks.astype(bf16)
            back_ref[...] = jnp.where(
                lax.broadcasted_iota(jnp.int32, (token_count, token_count), 1) == place, 1.0, 0.0
            ).astype(bf16)
            by_expert = sum(
                jnp.where(lane == ids[:, k : k + 1], routing[:, k : k + 1], 0.0)
                for k in range(TOPK)
            )
            by_slot = jnp.dot(
                picks, by_expert, preferred_element_type=f32, precision=lax.Precision.HIGHEST
            ).T
            for expert in range(experts):
                weight_send[expert] = jnp.broadcast_to(
                    by_slot[expert : expert + 1], (8, token_count)
                )
            weight_recv[me_s] = weight_send[me_s]
            for step in range(1, experts):
                push(
                    weight_send.at[lax.rem(me_s + step, experts)], weight_recv.at[me_s], 1,
                    share_sem, {"sp": lax.rem(me_s + step, experts)},
                )

        waiting = []
        for part in range(pieces):
            pass_on(1, part)
        for head in range(key_heads):
            prepare(head)
        route()
        waiting += [(0, head, True) for head in range(key_heads)]
        for hop in range(2, ring_half + 1):
            for part in range(pieces):
                pass_on(hop, part)
                for _ in range(-(-len(waiting) // (pieces - part))):
                    attend(*waiting.pop(0))
            if hop < ring_half:
                for slot in (hop - 1, experts - hop + 1):
                    waiting += [(slot, head, False) for head in range(key_heads)]
        with scope("ring_tail"):
            for way in range(2):
                for part in range(pieces):
                    if (way, ring_half, part) not in ring:
                        ring[way, ring_half - 1, part].wait_recv()
        for slot in (ring_half - 1, ring_half + 1):
            for head in range(key_heads):
                attend(slot, head, False)
        with scope("ring_last"):
            for way in range(2):
                for part in range(pieces):
                    if (way, ring_half, part) in ring:
                        ring[way, ring_half, part].wait_recv()
        for head in range(key_heads):
            attend(ring_half, head, False)
        for head in range(key_heads):
            result_rows = flash_out[head] / flash_sum[head]
            att_ref[:, pl.ds(head * pair_width, pair_width)] = (
                jnp.concatenate([result_rows[:, :token_count], result_rows[:, token_count:]], 0)
                .T.astype(bf16)
            )
        attended_rows = att_ref[...]
        loads[3].wait()

        def mix(shard):
            return jnp.dot(
                attended_rows,
                ow_ref[:, pl.ds(pl.multiple_of(shard * width, width), width)],
                preferred_element_type=f32,
            )

        across = {}
        pair = {}

        def send_pair(step):
            mix_send[step] = mix(line_at(step) * 2 + 1 - core).astype(bf16)
            pair[step] = push(
                mix_send.at[step], mix_pair.at[step], 2, mix_sem.at[step], {"tp": partner}
            )

        for step in range(1, lines):
            send_pair(step)
        for step in range(1, lines):
            mine = mix(line_at(step) * 2 + core)
            with scope("pairwait"):
                pair[step].wait_recv()
            line_send[step - 1] = (mine + mix_pair[step].astype(f32)).astype(bf16)
            across[step] = push(
                line_send.at[step - 1], line_recv.at[step - 1], 2, line_sem.at[step - 1],
                {"tp": line_at(step) * 2 + core},
            )
        send_pair(0)
        total = mix(me_t)
        pair[0].wait_recv()
        total = total + mix_pair[0].astype(f32)
        loads[4].wait()
        total = total + residual_scale * res_ref[...].astype(f32)
        for step in range(1, lines):
            with scope("acrosswait"):
                across[step].wait_recv()
            total = total + line_recv[step - 1].astype(f32)

        def normalize(values, gain, turn):
            sums = jnp.sum(values, 1, keepdims=True)
            squares = jnp.sum(values * values, 1, keepdims=True)
            both = jnp.where(lane == 0, sums, jnp.where(lane == 1, squares, 0.0)).T[:8]
            stat_send[turn] = both
            for step in range(1, shards):
                push(
                    stat_send.at[turn], stat_recv.at[turn, step - 1], 3, stat_sem.at[turn],
                    {"tp": lax.rem(me_t + step, shards)},
                )
            waiter(stat_recv.at[turn], stat_sem.at[turn]).wait_recv()
            for step in range(1, shards):
                both = both + stat_recv[turn, step - 1]
            columns = jnp.concatenate([both] * 16, 0).T
            center = columns[:, 0:1] / feature_total
            spread = columns[:, 1:2] / feature_total - center * center
            return (values - center) * lax.rsqrt(spread + norm_epsilon) * gain

        with scope("norm1"):
            normed = normalize(total, gain_ref[...], 0).astype(bf16)
        spread_rows = jnp.dot(perm_ref[...], normed, preferred_element_type=f32).astype(bf16)
        outgoing[...] = spread_rows
        square = [(turn, step) for turn in range(EXP_GROUP) for step in range(lines)]
        square.sort(key=lambda pair: -(pair[0] + 1) // 2 - min(pair[1], lines - pair[1]))
        square.remove((0, 0))

        def member_span(index, owner):
            count = member_rows[index]
            return pl.ds(pl.multiple_of(owner * count, count), count)

        crossings = {}

        def cross(index):
            for place, step in enumerate(sets[index][0]):
                crossings[index, step] = push(
                    outgoing.at[pl.ds(step * capacity + sets[index][1] * stretch, stretch)],
                    routed[index].at[
                        me_t,
                        pl.ds(
                            pl.multiple_of(
                                me_m * member_rows[index] + place * stretch, stretch
                            ),
                            stretch,
                        ),
                    ],
                    4, cross_sem.at[away_sets.index(index), place], group_device(step),
                )

        arrivals = {}

        def spread(index):
            rows = member_span(index, me_m)
            if index in home_sets:
                top = sets[index][1] * stretch
                routed[index][me_t, rows] = spread_rows[top : top + stretch]
                source = outgoing.at[pl.ds(top, stretch)]
            else:
                for step in sets[index][0]:
                    crossings[index, step].wait_recv()
                source = routed[index].at[me_t, rows]
            for turn, step in square:
                arrivals[index, turn, step] = push(
                    source, routed[index].at[me_t, rows], 4, spread_sem.at[index, turn, step],
                    square_device(turn, step),
                )
            push(
                source, routed[index].at[me_t, rows], 5, mirror_sem.at[index], {"tp": partner}
            )

        def mirror(index):
            for turn, step in square:
                arrivals[index, turn, step].wait_recv()
                block = routed[index].at[
                    line_before(step) * 2 + core, member_span(index, member(turn))
                ]
                push(block, block, 5, mirror_sem.at[index], {"tp": partner})

        def settle(index):
            size = lines * set_rows[index] * width * 2
            waiter(stretch_of(size), mirror_sem.at[index]).wait_recv()

        def expand(index):
            base = sum(set_rows[:index])
            rows = set_rows[index]

            def one_tile(number, carry):
                cols = pl.ds(pl.multiple_of(number * tile, tile), tile)
                gate_sum = jnp.zeros((rows, tile), f32)
                up_sum = jnp.zeros((rows, tile), f32)
                for shard in range(shards):
                    block = routed[index][shard]
                    deep = pl.ds(shard * width, width)
                    gate_sum += jnp.dot(block, gate_v[deep, cols], preferred_element_type=f32)
                    up_sum += jnp.dot(block, up_v[deep, cols], preferred_element_type=f32)
                hidden[pl.ds(base, rows), cols] = (
                    gate_sum / (1.0 + jnp.exp(-gate_sum)) * up_sum
                ).astype(bf16)
                return carry

            lax.fori_loop(0, hidden_units // tile, one_tile, 0)

        def down(index, shard):
            base = sum(set_rows[:index])
            return scale_ref[pl.ds(base, set_rows[index]), 0:1] * jnp.dot(
                hidden[pl.ds(base, set_rows[index])],
                down_v[:, pl.ds(pl.multiple_of(shard * width, width), width)],
                preferred_element_type=f32,
            )

        parts = {}
        line_order = list(range(1, lines)) + [0]

        def shrink(index):
            for step in line_order:
                part_send[index][step] = down(index, line_at(step) * 2 + 1 - core).astype(bf16)
                parts[index, step] = push(
                    part_send[index].at[step], part_recv[index].at[step], 6,
                    part_sem.at[index, step], {"tp": partner},
                )
            for step in line_order:
                own_sum[index][step] = down(index, line_at(step) * 2 + core)

        def join(index):
            for step in line_order:
                parts[index, step].wait_recv()
                own = own_sum[index][step] + part_recv[index][step].astype(f32)
                give[index][step] = own.astype(bf16)
                for turn in (3, 2, 1, 0):
                    if turn == 0 and step == 0:
                        continue
                    push(
                        give[index].at[step, member_span(index, member(turn))],
                        take[index].at[turn, step], 7, return_sem.at[index],
                        square_device(turn, step),
                    )
                if step == 0:
                    kept[index][...] = own

        def gather_up(index):
            total = kept[index][member_span(index, me_m)]
            size = len(square) * member_rows[index] * width * 2
            waiter(stretch_of(size), return_sem.at[index]).wait_recv()
            for turn, step in square:
                total = total + take[index][turn, step].astype(f32)
            return total

        for index in away_sets[:1]:
            cross(index)
        spread(0)
        for index in away_sets[1:]:
            cross(index)
        with scope("weights_in"):
            waiter(weight_recv.at[pl.ds(0, experts - 1)], share_sem).wait_recv()
        shared = [
            weight_recv[lax.rem(me_g - step + groups, groups) * EXP_GROUP + owner, 0:1]
            for step in range(groups)
            for owner in range(EXP_GROUP)
        ]
        shared.append(jnp.zeros((128 - experts, token_count), f32))
        shared = jnp.concatenate(shared, 0).T
        base = 0
        for steps, part in sets:
            for owner in range(EXP_GROUP):
                for step in steps:
                    column = step * EXP_GROUP + owner
                    top = step * capacity + part * stretch
                    scale_ref[pl.ds(base, stretch)] = jnp.broadcast_to(
                        shared[top : top + stretch, column : column + 1], (stretch, 128)
                    )
                    base += stretch
        for index in away_sets + home_sets[1:]:
            with scope(f"cross{index}"):
                spread(index)
        with scope("mirror0"):
            mirror(0)
        with scope("weights"):
            for load in loads[5:]:
                load.wait()
        for index in range(len(sets)):
            with scope(f"settle{index}"):
                settle(index)
            with scope(f"expand{index}"):
                expand(index)
            if index + 1 < len(sets):
                with scope(f"mirror{index + 1}"):
                    mirror(index + 1)
            if index == 1:
                with scope("join0"):
                    join(0)
            with scope(f"shrink{index}"):
                shrink(index)
            if index > 0 or len(sets) == 1:
                with scope(f"join{index}"):
                    join(index)
        backs = {}
        for order, index in enumerate(away_sets):
            with scope(f"gather{index}"):
                home[order] = gather_up(index).astype(bf16)
            for place, step in enumerate(sets[index][0]):
                backs[step, sets[index][1]] = push(
                    home.at[order, pl.ds(place * stretch, stretch)],
                    returned_ref.at[step - 1, pl.ds(sets[index][1] * stretch, stretch)],
                    7, back_sem.at[order, place], group_device(-step),
                )
        with scope("gatherA"):
            combined = [gather_up(index) for index in home_sets]
        with scope("back"):
            for step in range(1, groups):
                for part in range(splits):
                    backs[step, part].wait_recv()
                combined.append(returned_ref[step - 1].astype(f32))
        second_sum = residual_scale * spread_rows.astype(f32) + jnp.concatenate(combined, 0)
        with scope("norm2"):
            result_rows = normalize(second_sum, last_gain_ref[...], 1).astype(bf16)
        out_ref[...] = jnp.dot(back_ref[...], result_rows, preferred_element_type=f32).astype(bf16)
        with scope("sendwait"):
            regions = {
                0: ring_ref.at[pl.ds(1, experts - 1)], 1: weight_recv.at[pl.ds(1, experts - 1)],
                3: stat_recv,
            }
            for phase in range(8):
                region = regions[phase] if phase in regions else stretch_of(sent_bytes[phase])
                size = int(np.prod(region.shape)) * jnp.dtype(region.dtype).itemsize
                assert size == sent_bytes[phase]
                waiter(region, send_sem.at[phase]).wait_send()

    vmem = pl.BlockSpec(memory_space=pltpu.VMEM)
    hbm = pl.BlockSpec(memory_space=pltpu.HBM)
    dma = pltpu.SemaphoreType.DMA
    other = max(lines - 1, 1)
    return pl.pallas_call(
        kernel,
        out_shape=pltpu.VMEM((token_count, width), bf16),
        in_specs=[hbm] * 16,
        out_specs=vmem,
        scratch_shapes=[
            pltpu.VMEM(row_table.shape, f32),
            pltpu.VMEM(column_table.shape, f32),
            pltpu.VMEM((1, HEAD_DIM), f32),
            pltpu.VMEM((1, HEAD_DIM), f32),
            pltpu.VMEM((1, width), f32),
            pltpu.VMEM((TOPK, token_count), jnp.int32),
            pltpu.VMEM((TOPK, token_count), f32),
            pltpu.VMEM((1, width), f32),
            dma((8,)),
            pltpu.VMEM(queries.shape, bf16),
            pltpu.VMEM(key_rows.shape, bf16),
            pltpu.VMEM(value_rows.shape, bf16),
            pltpu.VMEM(residual.shape, bf16),
            pltpu.VMEM(out_weight.shape, bf16),
            pltpu.VMEM(gate_weight.shape[1:], bf16),
            pltpu.VMEM(up_weight.shape[1:], bf16),
            pltpu.VMEM(down_weight.shape[1:], bf16),
            dma((8,)),
            dma((8,)),
            pltpu.VMEM((experts, token_count, key_heads * pair_width), bf16),
            dma((2, ring_half, pieces)),
            pltpu.VMEM((key_heads, query_rows, pair_width), bf16),
            pltpu.VMEM((key_heads, HEAD_DIM, query_rows), f32),
            pltpu.VMEM((key_heads, 1, query_rows), f32),
            pltpu.VMEM((key_heads, 1, query_rows), f32),
            pltpu.VMEM((token_count, key_heads * pair_width), bf16),
            pltpu.VMEM((lines, token_count, width), bf16),
            pltpu.VMEM((lines, token_count, width), bf16),
            pltpu.VMEM((other, token_count, width), bf16),
            pltpu.VMEM((other, token_count, width), bf16),
            dma((lines,)),
            dma((other,)),
            pltpu.VMEM((2, 8, token_count), f32),
            pltpu.VMEM((2, shards - 1, 8, token_count), f32),
            dma((2,)),
            pltpu.VMEM((token_count, token_count), bf16),
            pltpu.VMEM((token_count, token_count), bf16),
            pltpu.VMEM((experts, 8, token_count), f32),
            pltpu.VMEM((experts, 8, token_count), f32),
            dma,
            pltpu.VMEM((row_total, 128), f32),
            pltpu.VMEM((token_count, width), bf16),
            pltpu.VMEM((row_total, hidden_units), bf16),
            dma((splits, max(groups - 1, 1))),
            dma((len(sets), EXP_GROUP, lines)),
            dma((len(sets),)),
            dma((len(sets), lines)),
            dma((len(sets),)),
            pltpu.VMEM((splits, far_rows, width), bf16),
            pltpu.VMEM((max(groups - 1, 1), capacity, width), bf16),
            dma((splits, max(groups - 1, 1))),
        ]
        + [pltpu.VMEM((shards, rows, width), bf16) for rows in set_rows]
        + [pltpu.VMEM((lines, rows, width), bf16) for rows in set_rows] * 3
        + [pltpu.VMEM((EXP_GROUP, lines, rows, width), bf16) for rows in member_rows]
        + [pltpu.VMEM((rows, width), f32) for rows in set_rows]
        + [pltpu.VMEM((lines, rows, width), f32) for rows in set_rows],
        compiler_params=pltpu.CompilerParams(
            collective_id=0, has_side_effects=True, vmem_limit_bytes=48 << 20
        ),
    )(
        *(
            pltpu.with_memory_space_constraint(array, pltpu.HBM)
            for array in (
                jnp.asarray(row_table), jnp.asarray(column_table), query_gain.reshape(1, -1),
                key_gain.reshape(1, -1), norm_gain.reshape(1, -1), expert_ids.T, route_weights.T,
                final_gain.reshape(1, -1), queries, key_rows, value_rows, residual, out_weight,
                gate_weight, up_weight, down_weight,
            )
        )
    )


def per_device(
    queries,
    projected_key_rows,
    projected_value_rows,
    query_gain,
    key_norm_gain,
    residual,
    out_weight,
    norm_gain,
    expert_ids,
    route_weights,
    gate_weight,
    up_weight,
    down_weight,
    final_gain,
):
    token_total = queries.shape[0] * lax.axis_size("sp")
    row_table, column_table = rotary_tables(-(-token_total // GRID_W))
    return layer(
        queries,
        projected_key_rows,
        projected_value_rows,
        row_table,
        column_table,
        query_gain,
        key_norm_gain,
        out_weight,
        residual,
        norm_gain,
        expert_ids,
        route_weights,
        gate_weight,
        up_weight,
        down_weight,
        final_gain,
        lax.axis_size("sp"),
        lax.axis_size("tp"),
    )


def solution(mesh):
    in_specs = (
        P("sp", "tp"),
        P("sp", "tp"),
        P("sp", "tp"),
        P(),
        P(),
        P("sp", "tp"),
        P("tp", None),
        P("tp"),
        P("sp", None),
        P("sp", None),
        P("sp", None, "tp"),
        P("sp", None, "tp"),
        P("sp", "tp", None),
        P("tp"),
    )
    out_specs = P("sp", "tp")
    return jax.shard_map(
        per_device, mesh=mesh, in_specs=in_specs, out_specs=out_specs, check_vma=False
    )
```

```python
import contextlib

import jax
import jax.numpy as jnp
import numpy as np
from jax import lax
from jax.experimental import pallas as pl
from jax.experimental.pallas import tpu as pltpu
from jax.sharding import PartitionSpec as P

D = 2048
HEAD_DIM = 64
GRID_W = 64
EXP_GROUP = 4
TOPK = 2


theta_base = 10000.0
norm_epsilon = 1e-06
residual_scale = 8.0**0.25
far_below = -1e30
MESH = pl.DeviceIdType.MESH
SCOPES = False


def scope(name):
    return jax.named_scope(name) if SCOPES else contextlib.nullcontext()


def rotary_tables(grid_rows):
    quarter = HEAD_DIM // 4
    lane = np.arange(2 * HEAD_DIM)
    frequency = theta_base ** (-(lane % quarter) * 2.0 / (HEAD_DIM // 2))
    sign = np.where(lane % (2 * quarter) < quarter, -1.0, 1.0)
    by_row = lane % HEAD_DIM < HEAD_DIM // 2

    def tables(positions):
        angles = positions[:, None] * frequency[None, :].astype(np.float32).astype(np.float64)
        return np.stack([np.cos(angles), np.sin(angles) * sign[None, :]]).astype(np.float32)

    rows = np.where(by_row[None, None, :], tables(np.arange(grid_rows)), 0.0)
    columns = np.where(by_row[None, None, :], 0.0, tables(np.arange(GRID_W)))
    return rows.astype(np.float32), columns.astype(np.float32)


def place_of(index, group, group_minor):
    major = group // group_minor
    high, low = index // group_minor, lax.rem(index, group_minor)
    if group_minor == 1:
        return high
    back = major - 1 - high
    odd = lax.rem(back, 2)
    inner = (low - 1) * (1 - odd) + (group_minor - 1 - low) * odd
    first = jnp.where(low == 0, 1, 0)
    return first * high + (1 - first) * (major + back * (group_minor - 1) + inner)


def device_at(place, group, group_minor):
    major = group // group_minor
    if group_minor == 1:
        return place
    first = jnp.where(place < major, 1, 0)
    rest = jnp.maximum(place - major, 0)
    back = rest // (group_minor - 1)
    inner = lax.rem(rest, group_minor - 1)
    odd = lax.rem(back, 2)
    low = 1 + inner * (1 - odd) + (group_minor - 2 - inner) * odd
    other = (major - 1 - back) * group_minor + low
    return first * (place * group_minor) + (1 - first) * other


def layer(
    queries, key_rows, value_rows, row_table, column_table, query_gain, key_gain, out_weight, residual,
    norm_gain, expert_ids, route_weights, gate_weight, up_weight, down_weight, final_gain, experts,
    shards,
):
    token_count, width = residual.shape
    key_heads = key_rows.shape[1] // HEAD_DIM
    pair_width = 2 * HEAD_DIM
    query_rows = 2 * token_count
    ring_minor = 1 << ((experts.bit_length() - 1) // 2)
    ring_half = experts // 2
    pieces = 8
    piece = token_count // pieces
    lines = shards // 2
    groups = experts // EXP_GROUP
    capacity = token_count // groups
    splits = 2 if capacity % 32 == 0 else 1
    stretch = capacity // splits
    near_sets = [([0], part) for part in range(splits)]
    far_sets = [(list(range(1, groups)), part) for part in range(splits)] if groups > 1 else []
    sets = near_sets[:1] + far_sets + near_sets[1:]
    home_sets = [index for index, (steps, _) in enumerate(sets) if steps == [0]]
    away_sets = [index for index, (steps, _) in enumerate(sets) if steps != [0]]
    far_rows = (groups - 1) * stretch if groups > 1 else stretch
    member_rows = [len(steps) * stretch for steps, _ in sets]
    set_rows = [EXP_GROUP * rows for rows in member_rows]
    row_total = sum(set_rows)
    hidden_units = gate_weight.shape[2]
    tile = min(256, hidden_units)
    feature_total = width * shards
    bf16, f32 = jnp.bfloat16, jnp.float32

    def kernel(
        row_hbm, column_hbm, q_gain_hbm, k_gain_hbm, gain_hbm, ids_hbm, rw_hbm, last_gain_hbm,
        q_hbm, k_hbm, v_hbm, res_hbm, ow_hbm, gate_hbm, up_hbm, down_hbm, out_ref,
        row_ref, column_ref, q_gain_ref, k_gain_ref, gain_ref, ids_ref, rw_ref, last_gain_ref,
        small_sem, q_v, k_v, v_v, res_ref, ow_ref, gate_v, up_v, down_v, weight_sem,
        send_sem, ring_ref, ring_recv, q_pad, flash_out, flash_max, flash_sum, att_ref,
        mix_send, mix_pair, line_send, line_recv, mix_sem, line_sem,
        stat_send, stat_recv, stat_sem,
        perm_ref, back_ref, weight_send, weight_recv, share_sem, scale_ref, outgoing, hidden,
        cross_sem, spread_sem, later_sem, mirror_sem, part_sem, return_sem, home, returned_ref, back_sem,
        *per_set,
    ):
        count = len(sets)
        routed, part_send, part_recv, give, take, kept, own_sum = [
            per_set[i * count : (i + 1) * count] for i in range(7)
        ]
        me_s = lax.axis_index("sp")
        me_t = lax.axis_index("tp")
        line = me_t // 2
        core = lax.rem(me_t, 2)
        partner = line * 2 + 1 - core

        def line_at(step):
            return lax.rem(line + step, lines)

        me_g = me_s // EXP_GROUP
        me_m = lax.rem(me_s, EXP_GROUP)

        def member(turn):
            if turn == 0:
                return me_m
            if turn == 1:
                return me_m + 1 - 2 * lax.rem(me_m, 2)
            if turn == 2:
                return me_m + 2 - 4 * (me_m // 2)
            return EXP_GROUP - 1 - me_m

        def line_before(step):
            return lax.rem(line + lines - step, lines)

        def group_device(step):
            return {"sp": lax.rem(me_g + step + groups, groups) * EXP_GROUP + me_m}

        def square_device(turn, step):
            return {"sp": me_g * EXP_GROUP + member(turn), "tp": line_at(step) * 2 + core}

        barrier = pltpu.get_barrier_semaphore()
        for step in range(1, experts):
            pl.semaphore_signal(
                barrier, inc=1, device_id={"sp": lax.rem(me_s + step, experts)},
                device_id_type=MESH,
            )
        for step in range(1, shards):
            pl.semaphore_signal(
                barrier, inc=1, device_id={"tp": lax.rem(me_t + step, shards)},
                device_id_type=MESH,
            )
        for turn in range(1, EXP_GROUP):
            for step in range(1, lines):
                pl.semaphore_signal(
                    barrier, inc=1, device_id=square_device(turn, step), device_id_type=MESH
                )
        greeted = experts - 1 + shards - 1 + (EXP_GROUP - 1) * (lines - 1)
        loads = [
            pltpu.make_async_copy(src, dst, weight_sem.at[i])
            for i, (src, dst) in enumerate(
                (
                    (k_hbm, k_v), (v_hbm, v_v), (q_hbm, q_v), (ow_hbm, ow_ref), (res_hbm, res_ref),
                    (gate_hbm.at[0], gate_v), (up_hbm.at[0], up_v), (down_hbm.at[0], down_v),
                )
            )
        ]
        small_loads = [
            pltpu.make_async_copy(src, dst, small_sem.at[i])
            for i, (src, dst) in enumerate(
                (
                    (row_hbm, row_ref), (column_hbm, column_ref), (q_gain_hbm, q_gain_ref),
                    (k_gain_hbm, k_gain_ref), (gain_hbm, gain_ref), (ids_hbm, ids_ref),
                    (rw_hbm, rw_ref), (last_gain_hbm, last_gain_ref),
                )
            )
        ]
        for load in loads[:3] + small_loads:
            load.start()
        sent_bytes = dict.fromkeys(range(8), 0)

        def push(source, target, phase, recv_sem, device):
            copy = pltpu.make_async_remote_copy(
                src_ref=source, dst_ref=target, send_sem=send_sem.at[phase], recv_sem=recv_sem,
                device_id=device, device_id_type=MESH,
            )
            copy.start()
            sent_bytes[phase] += int(np.prod(source.shape)) * jnp.dtype(source.dtype).itemsize
            return copy

        def stretch_of(size):
            rows = size // (2 * hidden_units)
            assert rows * 2 * hidden_units == size and rows % 8 == 0 and rows <= feature_total
            return gate_v.at[pl.ds(0, rows)]

        def waiter(region, sems):
            return pltpu.make_async_remote_copy(
                src_ref=region, dst_ref=region, send_sem=sems, recv_sem=sems,
                device_id={"tp": partner}, device_id_type=MESH,
            )

        lane_pair = lax.broadcasted_iota(jnp.int32, (token_count, pair_width), 1)
        low_half = lane_pair < HEAD_DIM
        quarter = HEAD_DIM // 4
        turn_low = lane_pair % (2 * quarter) < quarter
        same_head = jnp.where(
            lax.broadcasted_iota(jnp.int32, (pair_width, pair_width), 0) // HEAD_DIM
            == lax.broadcasted_iota(jnp.int32, (pair_width, pair_width), 1) // HEAD_DIM,
            1.0, 0.0,
        ).astype(bf16)
        for load in small_loads:
            load.wait()
        for load in loads[:3]:
            load.wait()
        for load in loads[3:]:
            load.start()

        def rotary(part):
            blocks = []
            for line_of_grid in range(token_count // GRID_W):
                row = row_ref[part, pl.ds(me_s * (token_count // GRID_W) + line_of_grid, 1)]
                blocks.append(column_ref[part] + row)
            return jnp.concatenate(blocks, 0)

        cosine, sine = rotary(0), rotary(1)
        both_gains = [
            jnp.concatenate([ref[...]] * 2, 1) for ref in (q_gain_ref, k_gain_ref)
        ]

        def rotated(rows, gain):
            square = rows * rows
            high = square.astype(bf16)
            rest = (square - high.astype(f32)).astype(bf16)
            total = jnp.dot(high, same_head, preferred_element_type=f32) + jnp.dot(
                rest, same_head, preferred_element_type=f32
            )
            scaled = rows * lax.rsqrt(total / HEAD_DIM + norm_epsilon) * gain
            turned = jnp.where(
                turn_low,
                pltpu.roll(scaled, pair_width - quarter, 1),
                pltpu.roll(scaled, quarter, 1),
            )
            return scaled * cosine + turned * sine

        def swap(rows):
            return pltpu.roll(rows, HEAD_DIM, 1)

        for pair in range((key_heads + 1) // 2):
            if key_heads == 1:
                key_pair = jnp.concatenate([k_v[...]] * 2, 1).astype(f32)
                value_pair = jnp.concatenate([v_v[...]] * 2, 1).astype(f32)
            else:
                lanes = pl.ds(pair * pair_width, pair_width)
                key_pair = k_v[:, lanes].astype(f32)
                value_pair = v_v[:, lanes].astype(f32)
            key_pair = rotated(key_pair, both_gains[1])
            ring_ref[0, :, pl.ds(2 * pair * pair_width, pair_width)] = jnp.where(
                low_half, key_pair, swap(value_pair)
            ).astype(bf16)
            if key_heads > 1:
                ring_ref[0, :, pl.ds((2 * pair + 1) * pair_width, pair_width)] = jnp.where(
                    low_half, swap(key_pair), value_pair
                ).astype(bf16)
        spot = place_of(me_s, experts, ring_minor)
        right = device_at(lax.rem(spot + 1, experts), experts, ring_minor)
        left = device_at(lax.rem(spot + experts - 1, experts), experts, ring_minor)
        with scope("barrier"):
            pl.semaphore_wait(barrier, greeted)

        ring = {}

        def pass_on(hop, part):
            for way in range(2):
                if hop == ring_half and (part < pieces // 2) != (way == 0):
                    continue
                if hop > 1:
                    ring[way, hop - 1, part].wait_recv()
                span = pl.ds(part * piece, piece)
                source_slot = (hop - 1) if way == 0 else (experts - hop + 1) % experts
                target_slot = hop if way == 0 else experts - hop
                copy = push(
                    ring_ref.at[source_slot, span], ring_ref.at[target_slot, span], 0,
                    ring_recv.at[way, hop - 1, part], {"sp": right if way == 0 else left},
                )
                ring[way, hop, part] = copy

        def attend(slot, head, first):
            block = ring_ref[slot, :, pl.ds(head * pair_width, pair_width)]
            scores = lax.dot_general(
                block, q_pad[head], (((1,), (1,)), ((), ())), preferred_element_type=f32
            )
            peak = jnp.max(scores, 0, keepdims=True)
            if not first:
                peak = jnp.maximum(flash_max[head], peak)
            weights = jnp.exp(scores - peak)
            mass = jnp.sum(weights, 0, keepdims=True)
            gathered = lax.dot_general(
                block, weights.astype(bf16), (((0,), (0,)), ((), ())), preferred_element_type=f32
            )[HEAD_DIM:]
            if not first:
                fade = jnp.exp(flash_max[head] - peak)
                mass = mass + flash_sum[head] * fade
                gathered = gathered + flash_out[head] * fade
            flash_max[head] = peak
            flash_sum[head] = mass
            flash_out[head] = gathered

        def prepare(head):
            rows = rotated(
                q_v[:, pl.ds(head * pair_width, pair_width)].astype(f32), both_gains[0]
            ) * HEAD_DIM ** (-0.5)
            rows = jnp.dot(perm_ref[...], rows.astype(bf16), preferred_element_type=f32)
            q_pad[head, pl.ds(0, token_count)] = jnp.where(low_half, rows, 0.0).astype(bf16)
            q_pad[head, pl.ds(token_count, token_count)] = jnp.where(
                low_half, swap(rows), 0.0
            ).astype(bf16)

        def columns_of(rows):
            return jnp.concatenate([rows] * (token_count // TOPK), 0).T

        lane = lax.broadcasted_iota(jnp.int32, (token_count, 128), 1)
        before = jnp.where(
            lax.broadcasted_iota(jnp.int32, (token_count, token_count), 1)
            < lax.broadcasted_iota(jnp.int32, (token_count, token_count), 0),
            1.0, 0.0,
        ).astype(bf16)

        def route():
            ids = columns_of(ids_ref[...].astype(f32)).astype(jnp.int32)
            routing = columns_of(rw_ref[...])
            group_of = ids[:, 0:1] // EXP_GROUP
            inside = jnp.where(lane == group_of, 1.0, 0.0)
            earlier = jnp.dot(before, inside.astype(bf16), preferred_element_type=f32)
            slot = jnp.sum(earlier * inside, 1, keepdims=True)
            away = lax.rem(group_of - me_g + groups, groups)
            place = (away * capacity).astype(f32) + slot
            place_row = jnp.where(lane == 0, place, 0.0).T[0:1].astype(jnp.int32)
            place = place.astype(jnp.int32)
            row_index = lax.broadcasted_iota(jnp.int32, (token_count, token_count), 0)
            picks = jnp.where(row_index == place_row, 1.0, 0.0)
            perm_ref[...] = picks.astype(bf16)
            back_ref[...] = jnp.where(
                lax.broadcasted_iota(jnp.int32, (token_count, token_count), 1) == place, 1.0, 0.0
            ).astype(bf16)
            by_expert = sum(
                jnp.where(lane == ids[:, k : k + 1], routing[:, k : k + 1], 0.0)
                for k in range(TOPK)
            )
            by_slot = jnp.dot(
                picks, by_expert, preferred_element_type=f32, precision=lax.Precision.HIGHEST
            ).T
            for expert in range(experts):
                weight_send[expert] = jnp.broadcast_to(
                    by_slot[expert : expert + 1], (8, token_count)
                )
            weight_recv[me_s] = weight_send[me_s]
            for step in range(1, experts):
                push(
                    weight_send.at[lax.rem(me_s + step, experts)], weight_recv.at[me_s], 1,
                    share_sem, {"sp": lax.rem(me_s + step, experts)},
                )

        waiting = []
        for part in range(pieces):
            pass_on(1, part)
        route()
        for head in range(key_heads):
            prepare(head)
        waiting += [(0, head, True) for head in range(key_heads)]
        for hop in range(2, ring_half + 1):
            if hop == 3:
                loads[4].wait()
                res_ref[...] = jnp.dot(
                    perm_ref[...], res_ref[...], preferred_element_type=f32
                ).astype(bf16)
            for part in range(pieces):
                pass_on(hop, part)
                for _ in range(-(-len(waiting) // (pieces - part))):
                    attend(*waiting.pop(0))
            if hop < ring_half:
                for slot in (hop - 1, experts - hop + 1):
                    waiting += [(slot, head, False) for head in range(key_heads)]
        with scope("ring_tail"):
            for way in range(2):
                for part in range(pieces):
                    if (way, ring_half, part) not in ring:
                        ring[way, ring_half - 1, part].wait_recv()
        for slot in (ring_half - 1, ring_half + 1):
            for head in range(key_heads):
                attend(slot, head, False)
        with scope("ring_last"):
            for way in range(2):
                for part in range(pieces):
                    if (way, ring_half, part) in ring:
                        ring[way, ring_half, part].wait_recv()
        for head in range(key_heads):
            attend(ring_half, head, False)
        for head in range(key_heads):
            result_rows = flash_out[head] / flash_sum[head]
            att_ref[:, pl.ds(head * pair_width, pair_width)] = (
                jnp.concatenate([result_rows[:, :token_count], result_rows[:, token_count:]], 0)
                .T.astype(bf16)
            )
        attended_rows = att_ref[...]
        loads[3].wait()

        def mix(shard):
            return jnp.dot(
                attended_rows,
                ow_ref[:, pl.ds(pl.multiple_of(shard * width, width), width)],
                preferred_element_type=f32,
            )

        across = {}
        pair = {}

        def send_pair(step):
            mix_send[step] = mix(line_at(step) * 2 + 1 - core).astype(bf16)
            pair[step] = push(
                mix_send.at[step], mix_pair.at[step], 2, mix_sem.at[step], {"tp": partner}
            )

        for step in range(1, lines):
            send_pair(step)
        for step in range(1, lines):
            mine = mix(line_at(step) * 2 + core)
            with scope("pairwait"):
                pair[step].wait_recv()
            line_send[step - 1] = (mine + mix_pair[step].astype(f32)).astype(bf16)
            across[step] = push(
                line_send.at[step - 1], line_recv.at[step - 1], 2, line_sem.at[step - 1],
                {"tp": line_at(step) * 2 + core},
            )
        send_pair(0)
        total = mix(me_t)
        pair[0].wait_recv()
        total = total + mix_pair[0].astype(f32)
        total = total + residual_scale * res_ref[...].astype(f32)
        for step in range(1, lines):
            with scope("acrosswait"):
                across[step].wait_recv()
            total = total + line_recv[step - 1].astype(f32)

        def normalize(values, gain, turn):
            sums = jnp.sum(values, 1, keepdims=True)
            squares = jnp.sum(values * values, 1, keepdims=True)
            both = jnp.where(lane == 0, sums, jnp.where(lane == 1, squares, 0.0)).T[:8]
            stat_send[turn] = both
            for step in range(1, shards):
                push(
                    stat_send.at[turn], stat_recv.at[turn, step - 1], 3, stat_sem.at[turn],
                    {"tp": lax.rem(me_t + step, shards)},
                )
            waiter(stat_recv.at[turn], stat_sem.at[turn]).wait_recv()
            for step in range(1, shards):
                both = both + stat_recv[turn, step - 1]
            columns = jnp.concatenate([both] * 16, 0).T
            center = columns[:, 0:1] / feature_total
            spread = columns[:, 1:2] / feature_total - center * center
            return (values - center) * lax.rsqrt(spread + norm_epsilon) * gain

        with scope("norm1"):
            normed = normalize(total, gain_ref[...], 0).astype(bf16)
        spread_rows = normed
        outgoing[...] = spread_rows
        square = [(turn, step) for turn in range(EXP_GROUP) for step in range(lines)]
        square.sort(key=lambda pair: -(pair[0] + 1) // 2 - min(pair[1], lines - pair[1]))
        square.remove((0, 0))

        def member_span(index, owner):
            count = member_rows[index]
            return pl.ds(pl.multiple_of(owner * count, count), count)

        crossings = {}

        def cross(index):
            for place, step in enumerate(sets[index][0]):
                crossings[index, step] = push(
                    outgoing.at[pl.ds(step * capacity + sets[index][1] * stretch, stretch)],
                    routed[index].at[
                        me_t,
                        pl.ds(
                            pl.multiple_of(
                                me_m * member_rows[index] + place * stretch, stretch
                            ),
                            stretch,
                        ),
                    ],
                    4, cross_sem.at[away_sets.index(index), place], group_device(step),
                )

        arrivals = {}

        def spread(index):
            rows = member_span(index, me_m)
            if index in home_sets:
                top = sets[index][1] * stretch
                routed[index][me_t, rows] = spread_rows[top : top + stretch]
                source = outgoing.at[pl.ds(top, stretch)]
            else:
                for step in sets[index][0]:
                    crossings[index, step].wait_recv()
                source = routed[index].at[me_t, rows]
            for turn, step in square:
                arrivals[index, turn, step] = push(
                    source, routed[index].at[me_t, rows], 4, spread_sem.at[turn, step] if index == 0 else later_sem.at[index],
                    square_device(turn, step),
                )
            push(
                source, routed[index].at[me_t, rows], 5, mirror_sem.at[index], {"tp": partner}
            )

        def mirror(index):
            if index > 0:
                size = len(square) * member_rows[index] * width * 2
                waiter(stretch_of(size), later_sem.at[index]).wait_recv()
            for turn, step in square:
                if index == 0:
                    arrivals[index, turn, step].wait_recv()
                block = routed[index].at[
                    line_before(step) * 2 + core, member_span(index, member(turn))
                ]
                push(block, block, 5, mirror_sem.at[index], {"tp": partner})

        def settle(index):
            size = lines * set_rows[index] * width * 2
            waiter(stretch_of(size), mirror_sem.at[index]).wait_recv()

        def expand(index, span):
            base = sum(set_rows[:index])
            rows = set_rows[index]

            def one_tile(number, carry):
                cols = pl.ds(pl.multiple_of(number * tile, tile), tile)
                block = jnp.concatenate([routed[index][shard] for shard in range(shards)], 1)
                gate_sum = jnp.dot(block, gate_v[:, cols], preferred_element_type=f32)
                up_sum = jnp.dot(block, up_v[:, cols], preferred_element_type=f32)
                hidden[pl.ds(base, rows), cols] = (
                    gate_sum / (1.0 + jnp.exp(-gate_sum)) * up_sum
                ).astype(bf16)
                return carry

            lax.fori_loop(*span, one_tile, 0)

        def down(index, shard):
            base = sum(set_rows[:index])
            return scale_ref[pl.ds(base, set_rows[index]), 0:1] * jnp.dot(
                hidden[pl.ds(base, set_rows[index])],
                down_v[:, pl.ds(pl.multiple_of(shard * width, width), width)],
                preferred_element_type=f32,
            )

        parts = {}
        line_order = list(range(1, lines)) + [0]

        def shrink(index):
            for step in line_order:
                part_send[index][step] = down(index, line_at(step) * 2 + 1 - core).astype(bf16)
                parts[index, step] = push(
                    part_send[index].at[step], part_recv[index].at[step], 6,
                    part_sem.at[index, step], {"tp": partner},
                )
            for step in line_order:
                own_sum[index][step] = down(index, line_at(step) * 2 + core)

        def join(index):
            for step in line_order:
                parts[index, step].wait_recv()
                own = own_sum[index][step] + part_recv[index][step].astype(f32)
                give[index][step] = own.astype(bf16)
                for turn in (3, 2, 1, 0):
                    if turn == 0 and step == 0:
                        continue
                    push(
                        give[index].at[step, member_span(index, member(turn))],
                        take[index].at[turn, step], 7, return_sem.at[index],
                        square_device(turn, step),
                    )
                if step == 0:
                    kept[index][...] = own

        def gather_up(index):
            total = kept[index][member_span(index, me_m)]
            size = len(square) * member_rows[index] * width * 2
            waiter(stretch_of(size), return_sem.at[index]).wait_recv()
            for turn, step in square:
                total = total + take[index][turn, step].astype(f32)
            return total

        for index in away_sets[:1]:
            cross(index)
        spread(0)
        for index in away_sets[1:]:
            cross(index)
        with scope("weights_in"):
            waiter(weight_recv.at[pl.ds(0, experts - 1)], share_sem).wait_recv()
        shared = [
            weight_recv[lax.rem(me_g - step + groups, groups) * EXP_GROUP + owner, 0:1]
            for step in range(groups)
            for owner in range(EXP_GROUP)
        ]
        shared.append(jnp.zeros((128 - experts, token_count), f32))
        shared = jnp.concatenate(shared, 0).T
        base = 0
        for steps, part in sets:
            for owner in range(EXP_GROUP):
                for step in steps:
                    column = step * EXP_GROUP + owner
                    top = step * capacity + part * stretch
                    scale_ref[pl.ds(base, stretch)] = jnp.broadcast_to(
                        shared[top : top + stretch, column : column + 1], (stretch, 128)
                    )
                    base += stretch
        for index in away_sets + home_sets[1:]:
            with scope(f"cross{index}"):
                spread(index)
        with scope("mirror0"):
            mirror(0)
        with scope("weights"):
            for load in loads[5:]:
                load.wait()
        tiles = hidden_units // tile
        for index in range(len(sets)):
            with scope(f"settle{index}"):
                settle(index)
            with scope(f"expand{index}a"):
                expand(index, (0, min(1, tiles)))
            if index > 0:
                with scope(f"join{index - 1}"):
                    join(index - 1)
            with scope(f"expand{index}b"):
                expand(index, (min(1, tiles), tiles))
            if index + 1 < len(sets):
                with scope(f"mirror{index + 1}"):
                    mirror(index + 1)
            with scope(f"shrink{index}"):
                shrink(index)
        with scope("join_last"):
            join(len(sets) - 1)
        backs = {}
        for order, index in enumerate(away_sets):
            with scope(f"gather{index}"):
                home[order] = gather_up(index).astype(bf16)
            for place, step in enumerate(sets[index][0]):
                backs[step, sets[index][1]] = push(
                    home.at[order, pl.ds(place * stretch, stretch)],
                    returned_ref.at[step - 1, pl.ds(sets[index][1] * stretch, stretch)],
                    7, back_sem.at[order, place], group_device(-step),
                )
        with scope("gatherA"):
            combined = [gather_up(index) for index in home_sets]
        with scope("back"):
            for step in range(1, groups):
                for part in range(splits):
                    backs[step, part].wait_recv()
                combined.append(returned_ref[step - 1].astype(f32))
        second_sum = residual_scale * spread_rows.astype(f32) + jnp.concatenate(combined, 0)
        with scope("norm2"):
            result_rows = normalize(second_sum, last_gain_ref[...], 1).astype(bf16)
        out_ref[...] = jnp.dot(back_ref[...], result_rows, preferred_element_type=f32).astype(bf16)
        with scope("sendwait"):
            regions = {
                0: ring_ref.at[pl.ds(1, experts - 1)], 1: weight_recv.at[pl.ds(1, experts - 1)],
                3: stat_recv,
            }
            for phase in range(8):
                region = regions[phase] if phase in regions else stretch_of(sent_bytes[phase])
                size = int(np.prod(region.shape)) * jnp.dtype(region.dtype).itemsize
                assert size == sent_bytes[phase]
                waiter(region, send_sem.at[phase]).wait_send()

    vmem = pl.BlockSpec(memory_space=pltpu.VMEM)
    hbm = pl.BlockSpec(memory_space=pltpu.HBM)
    dma = pltpu.SemaphoreType.DMA
    other = max(lines - 1, 1)
    return pl.pallas_call(
        kernel,
        out_shape=pltpu.VMEM((token_count, width), bf16),
        in_specs=[hbm] * 16,
        out_specs=vmem,
        scratch_shapes=[
            pltpu.VMEM(row_table.shape, f32),
            pltpu.VMEM(column_table.shape, f32),
            pltpu.VMEM((1, HEAD_DIM), f32),
            pltpu.VMEM((1, HEAD_DIM), f32),
            pltpu.VMEM((1, width), f32),
            pltpu.VMEM((TOPK, token_count), jnp.int32),
            pltpu.VMEM((TOPK, token_count), f32),
            pltpu.VMEM((1, width), f32),
            dma((8,)),
            pltpu.VMEM(queries.shape, bf16),
            pltpu.VMEM(key_rows.shape, bf16),
            pltpu.VMEM(value_rows.shape, bf16),
            pltpu.VMEM(residual.shape, bf16),
            pltpu.VMEM(out_weight.shape, bf16),
            pltpu.VMEM(gate_weight.shape[1:], bf16),
            pltpu.VMEM(up_weight.shape[1:], bf16),
            pltpu.VMEM(down_weight.shape[1:], bf16),
            dma((8,)),
            dma((8,)),
            pltpu.VMEM((experts, token_count, key_heads * pair_width), bf16),
            dma((2, ring_half, pieces)),
            pltpu.VMEM((key_heads, query_rows, pair_width), bf16),
            pltpu.VMEM((key_heads, HEAD_DIM, query_rows), f32),
            pltpu.VMEM((key_heads, 1, query_rows), f32),
            pltpu.VMEM((key_heads, 1, query_rows), f32),
            pltpu.VMEM((token_count, key_heads * pair_width), bf16),
            pltpu.VMEM((lines, token_count, width), bf16),
            pltpu.VMEM((lines, token_count, width), bf16),
            pltpu.VMEM((other, token_count, width), bf16),
            pltpu.VMEM((other, token_count, width), bf16),
            dma((lines,)),
            dma((other,)),
            pltpu.VMEM((2, 8, token_count), f32),
            pltpu.VMEM((2, shards - 1, 8, token_count), f32),
            dma((2,)),
            pltpu.VMEM((token_count, token_count), bf16),
            pltpu.VMEM((token_count, token_count), bf16),
            pltpu.VMEM((experts, 8, token_count), f32),
            pltpu.VMEM((experts, 8, token_count), f32),
            dma,
            pltpu.VMEM((row_total, 128), f32),
            pltpu.VMEM((token_count, width), bf16),
            pltpu.VMEM((row_total, hidden_units), bf16),
            dma((splits, max(groups - 1, 1))),
            dma((EXP_GROUP, lines)),
            dma((len(sets),)),
            dma((len(sets),)),
            dma((len(sets), lines)),
            dma((len(sets),)),
            pltpu.VMEM((splits, far_rows, width), bf16),
            pltpu.VMEM((max(groups - 1, 1), capacity, width), bf16),
            dma((splits, max(groups - 1, 1))),
        ]
        + [pltpu.VMEM((shards, rows, width), bf16) for rows in set_rows]
        + [pltpu.VMEM((lines, rows, width), bf16) for rows in set_rows] * 3
        + [pltpu.VMEM((EXP_GROUP, lines, rows, width), bf16) for rows in member_rows]
        + [pltpu.VMEM((rows, width), f32) for rows in set_rows]
        + [pltpu.VMEM((lines, rows, width), f32) for rows in set_rows],
        compiler_params=pltpu.CompilerParams(
            collective_id=0, has_side_effects=True, vmem_limit_bytes=48 << 20
        ),
    )(
        *(
            pltpu.with_memory_space_constraint(array, pltpu.HBM)
            for array in (
                jnp.asarray(row_table), jnp.asarray(column_table), query_gain.reshape(1, -1),
                key_gain.reshape(1, -1), norm_gain.reshape(1, -1), expert_ids.T, route_weights.T,
                final_gain.reshape(1, -1), queries, key_rows, value_rows, residual, out_weight,
                gate_weight, up_weight, down_weight,
            )
        )
    )


def per_device(
    queries,
    projected_key_rows,
    projected_value_rows,
    query_gain,
    key_norm_gain,
    residual,
    out_weight,
    norm_gain,
    expert_ids,
    route_weights,
    gate_weight,
    up_weight,
    down_weight,
    final_gain,
):
    token_total = queries.shape[0] * lax.axis_size("sp")
    row_table, column_table = rotary_tables(-(-token_total // GRID_W))
    return layer(
        queries,
        projected_key_rows,
        projected_value_rows,
        row_table,
        column_table,
        query_gain,
        key_norm_gain,
        out_weight,
        residual,
        norm_gain,
        expert_ids,
        route_weights,
        gate_weight,
        up_weight,
        down_weight,
        final_gain,
        lax.axis_size("sp"),
        lax.axis_size("tp"),
    )


def solution(mesh):
    in_specs = (
        P("sp", "tp"),
        P("sp", "tp"),
        P("sp", "tp"),
        P(),
        P(),
        P("sp", "tp"),
        P("tp", None),
        P("tp"),
        P("sp", None),
        P("sp", None),
        P("sp", None, "tp"),
        P("sp", None, "tp"),
        P("sp", "tp", None),
        P("tp"),
    )
    out_specs = P("sp", "tp")
    return jax.shard_map(
        per_device, mesh=mesh, in_specs=in_specs, out_specs=out_specs, check_vma=False
    )
```

```python
import contextlib

import jax
import jax.numpy as jnp
import numpy as np
from jax import lax
from jax.experimental import pallas as pl
from jax.experimental.pallas import tpu as pltpu
from jax.sharding import PartitionSpec as P

D = 2048
HEAD_DIM = 64
GRID_W = 64
EXP_GROUP = 4
TOPK = 2


theta_base = 10000.0
norm_epsilon = 1e-06
residual_scale = 8.0**0.25
far_below = -1e30
MESH = pl.DeviceIdType.MESH
SCOPES = False


def scope(name):
    return jax.named_scope(name) if SCOPES else contextlib.nullcontext()


def rotary_tables(grid_rows):
    quarter = HEAD_DIM // 4
    lane = np.arange(2 * HEAD_DIM)
    frequency = theta_base ** (-(lane % quarter) * 2.0 / (HEAD_DIM // 2))
    sign = np.where(lane % (2 * quarter) < quarter, -1.0, 1.0)
    by_row = lane % HEAD_DIM < HEAD_DIM // 2

    def tables(positions):
        angles = positions[:, None] * frequency[None, :].astype(np.float32).astype(np.float64)
        return np.stack([np.cos(angles), np.sin(angles) * sign[None, :]]).astype(np.float32)

    rows = np.where(by_row[None, None, :], tables(np.arange(grid_rows)), 0.0)
    columns = np.where(by_row[None, None, :], 0.0, tables(np.arange(GRID_W)))
    return rows.astype(np.float32), columns.astype(np.float32)


def place_of(index, group, group_minor):
    major = group // group_minor
    high, low = index // group_minor, lax.rem(index, group_minor)
    if group_minor == 1:
        return high
    back = major - 1 - high
    odd = lax.rem(back, 2)
    inner = (low - 1) * (1 - odd) + (group_minor - 1 - low) * odd
    first = jnp.where(low == 0, 1, 0)
    return first * high + (1 - first) * (major + back * (group_minor - 1) + inner)


def device_at(place, group, group_minor):
    major = group // group_minor
    if group_minor == 1:
        return place
    first = jnp.where(place < major, 1, 0)
    rest = jnp.maximum(place - major, 0)
    back = rest // (group_minor - 1)
    inner = lax.rem(rest, group_minor - 1)
    odd = lax.rem(back, 2)
    low = 1 + inner * (1 - odd) + (group_minor - 2 - inner) * odd
    other = (major - 1 - back) * group_minor + low
    return first * (place * group_minor) + (1 - first) * other


def layer(
    queries, key_rows, value_rows, row_table, column_table, query_gain, key_gain, out_weight, residual,
    norm_gain, expert_ids, route_weights, gate_weight, up_weight, down_weight, final_gain, experts,
    shards,
):
    token_count, width = residual.shape
    key_heads = key_rows.shape[1] // HEAD_DIM
    pair_width = 2 * HEAD_DIM
    query_rows = 2 * token_count
    ring_minor = 1 << ((experts.bit_length() - 1) // 2)
    ring_half = experts // 2
    pieces = 8
    piece = token_count // pieces
    lines = shards // 2
    groups = experts // EXP_GROUP
    capacity = token_count // groups
    splits = 2 if capacity % 32 == 0 else 1
    stretch = capacity // splits
    near_sets = [([0], part) for part in range(splits)]
    far_sets = [(list(range(1, groups)), part) for part in range(splits)] if groups > 1 else []
    sets = near_sets[:1] + far_sets + near_sets[1:]
    home_sets = [index for index, (steps, _) in enumerate(sets) if steps == [0]]
    away_sets = [index for index, (steps, _) in enumerate(sets) if steps != [0]]
    far_rows = (groups - 1) * stretch if groups > 1 else stretch
    member_rows = [len(steps) * stretch for steps, _ in sets]
    set_rows = [EXP_GROUP * rows for rows in member_rows]
    row_total = sum(set_rows)
    hidden_units = gate_weight.shape[2]
    tile = min(512, hidden_units)
    feature_total = width * shards
    bf16, f32 = jnp.bfloat16, jnp.float32

    def kernel(
        row_hbm, column_hbm, q_gain_hbm, k_gain_hbm, gain_hbm, ids_hbm, rw_hbm, last_gain_hbm,
        q_hbm, k_hbm, v_hbm, res_hbm, ow_hbm, gate_hbm, up_hbm, down_hbm, out_ref,
        row_ref, column_ref, q_gain_ref, k_gain_ref, gain_ref, ids_ref, rw_ref, last_gain_ref,
        small_sem, q_v, k_v, v_v, res_ref, ow_ref, gate_v, up_v, down_v, weight_sem,
        send_sem, ring_ref, ring_recv, q_pad, flash_out, flash_max, flash_sum, att_ref,
        mix_send, mix_pair, line_send, line_recv, mix_sem, line_sem,
        stat_send, stat_recv, stat_sem,
        perm_ref, back_ref, weight_send, weight_recv, share_sem, scale_ref, outgoing, hidden,
        cross_sem, spread_sem, later_sem, mirror_sem, part_sem, return_sem, home, returned_ref, back_sem,
        *per_set,
    ):
        count = len(sets)
        routed, part_send, part_recv, give, take, kept, own_sum = [
            per_set[i * count : (i + 1) * count] for i in range(7)
        ]
        me_s = lax.axis_index("sp")
        me_t = lax.axis_index("tp")
        line = me_t // 2
        core = lax.rem(me_t, 2)
        partner = line * 2 + 1 - core

        def line_at(step):
            return lax.rem(line + step, lines)

        me_g = me_s // EXP_GROUP
        me_m = lax.rem(me_s, EXP_GROUP)

        def member(turn):
            if turn == 0:
                return me_m
            if turn == 1:
                return me_m + 1 - 2 * lax.rem(me_m, 2)
            if turn == 2:
                return me_m + 2 - 4 * (me_m // 2)
            return EXP_GROUP - 1 - me_m

        def line_before(step):
            return lax.rem(line + lines - step, lines)

        def group_device(step):
            return {"sp": lax.rem(me_g + step + groups, groups) * EXP_GROUP + me_m}

        def square_device(turn, step):
            return {"sp": me_g * EXP_GROUP + member(turn), "tp": line_at(step) * 2 + core}

        barrier = pltpu.get_barrier_semaphore()
        for step in range(1, experts):
            pl.semaphore_signal(
                barrier, inc=1, device_id={"sp": lax.rem(me_s + step, experts)},
                device_id_type=MESH,
            )
        for step in range(1, shards):
            pl.semaphore_signal(
                barrier, inc=1, device_id={"tp": lax.rem(me_t + step, shards)},
                device_id_type=MESH,
            )
        for turn in range(1, EXP_GROUP):
            for step in range(1, lines):
                pl.semaphore_signal(
                    barrier, inc=1, device_id=square_device(turn, step), device_id_type=MESH
                )
        greeted = experts - 1 + shards - 1 + (EXP_GROUP - 1) * (lines - 1)
        loads = [
            pltpu.make_async_copy(src, dst, weight_sem.at[i])
            for i, (src, dst) in enumerate(
                (
                    (k_hbm, k_v), (v_hbm, v_v), (q_hbm, q_v), (ow_hbm, ow_ref), (res_hbm, res_ref),
                    (gate_hbm.at[0], gate_v), (up_hbm.at[0], up_v), (down_hbm.at[0], down_v),
                )
            )
        ]
        small_loads = [
            pltpu.make_async_copy(src, dst, small_sem.at[i])
            for i, (src, dst) in enumerate(
                (
                    (row_hbm, row_ref), (column_hbm, column_ref), (q_gain_hbm, q_gain_ref),
                    (k_gain_hbm, k_gain_ref), (gain_hbm, gain_ref), (ids_hbm, ids_ref),
                    (rw_hbm, rw_ref), (last_gain_hbm, last_gain_ref),
                )
            )
        ]
        for load in loads[:3] + small_loads:
            load.start()
        sent_bytes = dict.fromkeys(range(8), 0)

        def push(source, target, phase, recv_sem, device):
            copy = pltpu.make_async_remote_copy(
                src_ref=source, dst_ref=target, send_sem=send_sem.at[phase], recv_sem=recv_sem,
                device_id=device, device_id_type=MESH,
            )
            copy.start()
            sent_bytes[phase] += int(np.prod(source.shape)) * jnp.dtype(source.dtype).itemsize
            return copy

        def stretch_of(size):
            rows = size // (2 * hidden_units)
            assert rows * 2 * hidden_units == size and rows % 8 == 0 and rows <= feature_total
            return gate_v.at[pl.ds(0, rows)]

        def waiter(region, sems):
            return pltpu.make_async_remote_copy(
                src_ref=region, dst_ref=region, send_sem=sems, recv_sem=sems,
                device_id={"tp": partner}, device_id_type=MESH,
            )

        lane_pair = lax.broadcasted_iota(jnp.int32, (token_count, pair_width), 1)
        low_half = lane_pair < HEAD_DIM
        quarter = HEAD_DIM // 4
        turn_low = lane_pair % (2 * quarter) < quarter
        same_head = jnp.where(
            lax.broadcasted_iota(jnp.int32, (pair_width, pair_width), 0) // HEAD_DIM
            == lax.broadcasted_iota(jnp.int32, (pair_width, pair_width), 1) // HEAD_DIM,
            1.0, 0.0,
        ).astype(bf16)
        for load in small_loads:
            load.wait()
        for load in loads[:3]:
            load.wait()
        for load in loads[3:]:
            load.start()

        def rotary(part):
            blocks = []
            for line_of_grid in range(token_count // GRID_W):
                row = row_ref[part, pl.ds(me_s * (token_count // GRID_W) + line_of_grid, 1)]
                blocks.append(column_ref[part] + row)
            return jnp.concatenate(blocks, 0)

        cosine, sine = rotary(0), rotary(1)
        both_gains = [
            jnp.concatenate([ref[...]] * 2, 1) for ref in (q_gain_ref, k_gain_ref)
        ]

        def rotated(rows, gain):
            square = rows * rows
            high = square.astype(bf16)
            rest = (square - high.astype(f32)).astype(bf16)
            total = jnp.dot(high, same_head, preferred_element_type=f32) + jnp.dot(
                rest, same_head, preferred_element_type=f32
            )
            scaled = rows * lax.rsqrt(total / HEAD_DIM + norm_epsilon) * gain
            turned = jnp.where(
                turn_low,
                pltpu.roll(scaled, pair_width - quarter, 1),
                pltpu.roll(scaled, quarter, 1),
            )
            return scaled * cosine + turned * sine

        def swap(rows):
            return pltpu.roll(rows, HEAD_DIM, 1)

        for pair in range((key_heads + 1) // 2):
            if key_heads == 1:
                key_pair = jnp.concatenate([k_v[...]] * 2, 1).astype(f32)
                value_pair = jnp.concatenate([v_v[...]] * 2, 1).astype(f32)
            else:
                lanes = pl.ds(pair * pair_width, pair_width)
                key_pair = k_v[:, lanes].astype(f32)
                value_pair = v_v[:, lanes].astype(f32)
            key_pair = rotated(key_pair, both_gains[1])
            ring_ref[0, :, pl.ds(2 * pair * pair_width, pair_width)] = jnp.where(
                low_half, key_pair, swap(value_pair)
            ).astype(bf16)
            if key_heads > 1:
                ring_ref[0, :, pl.ds((2 * pair + 1) * pair_width, pair_width)] = jnp.where(
                    low_half, swap(key_pair), value_pair
                ).astype(bf16)
        spot = place_of(me_s, experts, ring_minor)
        right = device_at(lax.rem(spot + 1, experts), experts, ring_minor)
        left = device_at(lax.rem(spot + experts - 1, experts), experts, ring_minor)
        with scope("barrier"):
            pl.semaphore_wait(barrier, greeted)

        ring = {}

        def pass_on(hop, part):
            for way in range(2):
                if hop == ring_half and (part < pieces // 2) != (way == 0):
                    continue
                if hop > 1:
                    ring[way, hop - 1, part].wait_recv()
                span = pl.ds(part * piece, piece)
                source_slot = (hop - 1) if way == 0 else (experts - hop + 1) % experts
                target_slot = hop if way == 0 else experts - hop
                copy = push(
                    ring_ref.at[source_slot, span], ring_ref.at[target_slot, span], 0,
                    ring_recv.at[way, hop - 1, part], {"sp": right if way == 0 else left},
                )
                ring[way, hop, part] = copy

        def attend(slot, head, first):
            block = ring_ref[slot, :, pl.ds(head * pair_width, pair_width)]
            scores = lax.dot_general(
                block, q_pad[head], (((1,), (1,)), ((), ())), preferred_element_type=f32
            )
            peak = jnp.max(scores, 0, keepdims=True)
            if not first:
                peak = jnp.maximum(flash_max[head], peak)
            weights = jnp.exp(scores - peak)
            mass = jnp.sum(weights, 0, keepdims=True)
            gathered = lax.dot_general(
                block, weights.astype(bf16), (((0,), (0,)), ((), ())), preferred_element_type=f32
            )[HEAD_DIM:]
            if not first:
                fade = jnp.exp(flash_max[head] - peak)
                mass = mass + flash_sum[head] * fade
                gathered = gathered + flash_out[head] * fade
            flash_max[head] = peak
            flash_sum[head] = mass
            flash_out[head] = gathered

        def prepare(head):
            rows = rotated(
                q_v[:, pl.ds(head * pair_width, pair_width)].astype(f32), both_gains[0]
            ) * HEAD_DIM ** (-0.5)
            rows = jnp.dot(perm_ref[...], rows.astype(bf16), preferred_element_type=f32)
            q_pad[head, pl.ds(0, token_count)] = jnp.where(low_half, rows, 0.0).astype(bf16)
            q_pad[head, pl.ds(token_count, token_count)] = jnp.where(
                low_half, swap(rows), 0.0
            ).astype(bf16)

        def columns_of(rows):
            return jnp.concatenate([rows] * (token_count // TOPK), 0).T

        lane = lax.broadcasted_iota(jnp.int32, (token_count, 128), 1)
        before = jnp.where(
            lax.broadcasted_iota(jnp.int32, (token_count, token_count), 1)
            < lax.broadcasted_iota(jnp.int32, (token_count, token_count), 0),
            1.0, 0.0,
        ).astype(bf16)

        def route():
            ids = columns_of(ids_ref[...].astype(f32)).astype(jnp.int32)
            routing = columns_of(rw_ref[...])
            group_of = ids[:, 0:1] // EXP_GROUP
            inside = jnp.where(lane == group_of, 1.0, 0.0)
            earlier = jnp.dot(before, inside.astype(bf16), preferred_element_type=f32)
            slot = jnp.sum(earlier * inside, 1, keepdims=True)
            away = lax.rem(group_of - me_g + groups, groups)
            place = (away * capacity).astype(f32) + slot
            place_row = jnp.where(lane == 0, place, 0.0).T[0:1].astype(jnp.int32)
            place = place.astype(jnp.int32)
            row_index = lax.broadcasted_iota(jnp.int32, (token_count, token_count), 0)
            picks = jnp.where(row_index == place_row, 1.0, 0.0)
            perm_ref[...] = picks.astype(bf16)
            back_ref[...] = jnp.where(
                lax.broadcasted_iota(jnp.int32, (token_count, token_count), 1) == place, 1.0, 0.0
            ).astype(bf16)
            by_expert = sum(
                jnp.where(lane == ids[:, k : k + 1], routing[:, k : k + 1], 0.0)
                for k in range(TOPK)
            )
            by_slot = jnp.dot(
                picks, by_expert, preferred_element_type=f32, precision=lax.Precision.HIGHEST
            ).T
            for expert in range(experts):
                weight_send[expert] = jnp.broadcast_to(
                    by_slot[expert : expert + 1], (8, token_count)
                )
            weight_recv[me_s] = weight_send[me_s]
            for step in range(1, experts):
                push(
                    weight_send.at[lax.rem(me_s + step, experts)], weight_recv.at[me_s], 1,
                    share_sem, {"sp": lax.rem(me_s + step, experts)},
                )

        waiting = []
        for part in range(pieces):
            pass_on(1, part)
        route()
        for head in range(key_heads):
            prepare(head)
        waiting += [(0, head, True) for head in range(key_heads)]
        for hop in range(2, ring_half + 1):
            if hop == 3:
                loads[4].wait()
                res_ref[...] = jnp.dot(
                    perm_ref[...], res_ref[...], preferred_element_type=f32
                ).astype(bf16)
            for part in range(pieces):
                pass_on(hop, part)
                for _ in range(-(-len(waiting) // (pieces - part))):
                    attend(*waiting.pop(0))
            if hop < ring_half:
                for slot in (hop - 1, experts - hop + 1):
                    waiting += [(slot, head, False) for head in range(key_heads)]
        with scope("ring_tail"):
            for way in range(2):
                for part in range(pieces):
                    if (way, ring_half, part) not in ring:
                        ring[way, ring_half - 1, part].wait_recv()
        for slot in (ring_half - 1, ring_half + 1):
            for head in range(key_heads):
                attend(slot, head, False)
        with scope("ring_last"):
            for way in range(2):
                for part in range(pieces):
                    if (way, ring_half, part) in ring:
                        ring[way, ring_half, part].wait_recv()
        for head in range(key_heads):
            attend(ring_half, head, False)
        for head in range(key_heads):
            result_rows = flash_out[head] / flash_sum[head]
            att_ref[:, pl.ds(head * pair_width, pair_width)] = (
                jnp.concatenate([result_rows[:, :token_count], result_rows[:, token_count:]], 0)
                .T.astype(bf16)
            )
        attended_rows = att_ref[...]
        loads[3].wait()

        def mix(shard):
            return jnp.dot(
                attended_rows,
                ow_ref[:, pl.ds(pl.multiple_of(shard * width, width), width)],
                preferred_element_type=f32,
            )

        across = {}
        pair = {}

        def send_pair(step):
            mix_send[step] = mix(line_at(step) * 2 + 1 - core).astype(bf16)
            pair[step] = push(
                mix_send.at[step], mix_pair.at[step], 2, mix_sem.at[step], {"tp": partner}
            )

        for step in range(1, lines):
            send_pair(step)
        for step in range(1, lines):
            mine = mix(line_at(step) * 2 + core)
            with scope("pairwait"):
                pair[step].wait_recv()
            line_send[step - 1] = (mine + mix_pair[step].astype(f32)).astype(bf16)
            across[step] = push(
                line_send.at[step - 1], line_recv.at[step - 1], 2, line_sem.at[step - 1],
                {"tp": line_at(step) * 2 + core},
            )
        send_pair(0)
        total = mix(me_t)
        pair[0].wait_recv()
        total = total + mix_pair[0].astype(f32)
        total = total + residual_scale * res_ref[...].astype(f32)
        for step in range(1, lines):
            with scope("acrosswait"):
                across[step].wait_recv()
            total = total + line_recv[step - 1].astype(f32)

        def normalize(values, gain, turn):
            sums = jnp.sum(values, 1, keepdims=True)
            squares = jnp.sum(values * values, 1, keepdims=True)
            both = jnp.where(lane == 0, sums, jnp.where(lane == 1, squares, 0.0)).T[:8]
            stat_send[turn] = both
            for step in range(1, shards):
                push(
                    stat_send.at[turn], stat_recv.at[turn, step - 1], 3, stat_sem.at[turn],
                    {"tp": lax.rem(me_t + step, shards)},
                )
            waiter(stat_recv.at[turn], stat_sem.at[turn]).wait_recv()
            for step in range(1, shards):
                both = both + stat_recv[turn, step - 1]
            columns = jnp.concatenate([both] * 16, 0).T
            center = columns[:, 0:1] / feature_total
            spread = columns[:, 1:2] / feature_total - center * center
            return (values - center) * lax.rsqrt(spread + norm_epsilon) * gain

        with scope("norm1"):
            normed = normalize(total, gain_ref[...], 0).astype(bf16)
        spread_rows = normed
        outgoing[...] = spread_rows
        square = [(turn, step) for turn in range(EXP_GROUP) for step in range(lines)]
        square.sort(key=lambda pair: -(pair[0] + 1) // 2 - min(pair[1], lines - pair[1]))
        square.remove((0, 0))

        def member_span(index, owner):
            count = member_rows[index]
            return pl.ds(pl.multiple_of(owner * count, count), count)

        crossings = {}

        def cross(index):
            for place, step in enumerate(sets[index][0]):
                crossings[index, step] = push(
                    outgoing.at[pl.ds(step * capacity + sets[index][1] * stretch, stretch)],
                    routed[index].at[
                        me_t,
                        pl.ds(
                            pl.multiple_of(
                                me_m * member_rows[index] + place * stretch, stretch
                            ),
                            stretch,
                        ),
                    ],
                    4, cross_sem.at[away_sets.index(index), place], group_device(step),
                )

        arrivals = {}

        def spread(index):
            rows = member_span(index, me_m)
            if index in home_sets:
                top = sets[index][1] * stretch
                routed[index][me_t, rows] = spread_rows[top : top + stretch]
                source = outgoing.at[pl.ds(top, stretch)]
            else:
                for step in sets[index][0]:
                    crossings[index, step].wait_recv()
                source = routed[index].at[me_t, rows]
            for turn, step in square:
                arrivals[index, turn, step] = push(
                    source, routed[index].at[me_t, rows], 4, spread_sem.at[turn, step] if index == 0 else later_sem.at[index],
                    square_device(turn, step),
                )
            push(
                source, routed[index].at[me_t, rows], 5, mirror_sem.at[index], {"tp": partner}
            )

        def mirror(index):
            if index > 0:
                size = len(square) * member_rows[index] * width * 2
                waiter(stretch_of(size), later_sem.at[index]).wait_recv()
            for turn, step in square:
                if index == 0:
                    arrivals[index, turn, step].wait_recv()
                block = routed[index].at[
                    line_before(step) * 2 + core, member_span(index, member(turn))
                ]
                push(block, block, 5, mirror_sem.at[index], {"tp": partner})

        def settle(index):
            size = lines * set_rows[index] * width * 2
            waiter(stretch_of(size), mirror_sem.at[index]).wait_recv()

        def expand(index, span):
            base = sum(set_rows[:index])
            rows = set_rows[index]

            def one_tile(number, carry):
                cols = pl.ds(pl.multiple_of(number * tile, tile), tile)
                block = jnp.concatenate([routed[index][shard] for shard in range(shards)], 1)
                gate_sum = jnp.dot(block, gate_v[:, cols], preferred_element_type=f32)
                up_sum = jnp.dot(block, up_v[:, cols], preferred_element_type=f32)
                hidden[pl.ds(base, rows), cols] = (
                    gate_sum / (1.0 + jnp.exp(-gate_sum)) * up_sum
                ).astype(bf16)
                return carry

            lax.fori_loop(*span, one_tile, 0)

        def down(index, shard):
            base = sum(set_rows[:index])
            return scale_ref[pl.ds(base, set_rows[index]), 0:1] * jnp.dot(
                hidden[pl.ds(base, set_rows[index])],
                down_v[:, pl.ds(pl.multiple_of(shard * width, width), width)],
                preferred_element_type=f32,
            )

        parts = {}
        line_order = list(range(1, lines)) + [0]

        def shrink(index):
            for step in line_order:
                part_send[index][step] = down(index, line_at(step) * 2 + 1 - core).astype(bf16)
                parts[index, step] = push(
                    part_send[index].at[step], part_recv[index].at[step], 6,
                    part_sem.at[index, step], {"tp": partner},
                )
            for step in line_order:
                own_sum[index][step] = down(index, line_at(step) * 2 + core)

        def join(index):
            for step in line_order:
                parts[index, step].wait_recv()
                own = own_sum[index][step] + part_recv[index][step].astype(f32)
                give[index][step] = own.astype(bf16)
                for turn in (3, 2, 1, 0):
                    if turn == 0 and step == 0:
                        continue
                    push(
                        give[index].at[step, member_span(index, member(turn))],
                        take[index].at[turn, step], 7, return_sem.at[index],
                        square_device(turn, step),
                    )
                if step == 0:
                    kept[index][...] = own

        def gather_up(index):
            total = kept[index][member_span(index, me_m)]
            size = len(square) * member_rows[index] * width * 2
            waiter(stretch_of(size), return_sem.at[index]).wait_recv()
            for turn, step in square:
                total = total + take[index][turn, step].astype(f32)
            return total

        for index in away_sets[:1]:
            cross(index)
        spread(0)
        for index in away_sets[1:]:
            cross(index)
        with scope("weights_in"):
            waiter(weight_recv.at[pl.ds(0, experts - 1)], share_sem).wait_recv()
        shared = [
            weight_recv[lax.rem(me_g - step + groups, groups) * EXP_GROUP + owner, 0:1]
            for step in range(groups)
            for owner in range(EXP_GROUP)
        ]
        shared.append(jnp.zeros((128 - experts, token_count), f32))
        shared = jnp.concatenate(shared, 0).T
        base = 0
        for steps, part in sets:
            for owner in range(EXP_GROUP):
                for step in steps:
                    column = step * EXP_GROUP + owner
                    top = step * capacity + part * stretch
                    scale_ref[pl.ds(base, stretch)] = jnp.broadcast_to(
                        shared[top : top + stretch, column : column + 1], (stretch, 128)
                    )
                    base += stretch
        for index in away_sets + home_sets[1:]:
            with scope(f"cross{index}"):
                spread(index)
        with scope("mirror0"):
            mirror(0)
        with scope("weights"):
            for load in loads[5:]:
                load.wait()
        tiles = hidden_units // tile
        for index in range(len(sets)):
            with scope(f"settle{index}"):
                settle(index)
            with scope(f"expand{index}a"):
                expand(index, (0, min(1, tiles)))
            if index > 0:
                with scope(f"join{index - 1}"):
                    join(index - 1)
            with scope(f"expand{index}b"):
                expand(index, (min(1, tiles), tiles))
            if index + 1 < len(sets):
                with scope(f"mirror{index + 1}"):
                    mirror(index + 1)
            with scope(f"shrink{index}"):
                shrink(index)
        with scope("join_last"):
            join(len(sets) - 1)
        backs = {}
        for order, index in enumerate(away_sets):
            with scope(f"gather{index}"):
                home[order] = gather_up(index).astype(bf16)
            for place, step in enumerate(sets[index][0]):
                backs[step, sets[index][1]] = push(
                    home.at[order, pl.ds(place * stretch, stretch)],
                    returned_ref.at[step - 1, pl.ds(sets[index][1] * stretch, stretch)],
                    7, back_sem.at[order, place], group_device(-step),
                )
        with scope("gatherA"):
            combined = [gather_up(index) for index in home_sets]
        with scope("back"):
            for step in range(1, groups):
                for part in range(splits):
                    backs[step, part].wait_recv()
                combined.append(returned_ref[step - 1].astype(f32))
        second_sum = residual_scale * spread_rows.astype(f32) + jnp.concatenate(combined, 0)
        with scope("norm2"):
            result_rows = normalize(second_sum, last_gain_ref[...], 1).astype(bf16)
        out_ref[...] = jnp.dot(back_ref[...], result_rows, preferred_element_type=f32).astype(bf16)
        with scope("sendwait"):
            regions = {
                0: ring_ref.at[pl.ds(1, experts - 1)], 1: weight_recv.at[pl.ds(1, experts - 1)],
                3: stat_recv,
            }
            for phase in range(8):
                region = regions[phase] if phase in regions else stretch_of(sent_bytes[phase])
                size = int(np.prod(region.shape)) * jnp.dtype(region.dtype).itemsize
                assert size == sent_bytes[phase]
                waiter(region, send_sem.at[phase]).wait_send()

    vmem = pl.BlockSpec(memory_space=pltpu.VMEM)
    hbm = pl.BlockSpec(memory_space=pltpu.HBM)
    dma = pltpu.SemaphoreType.DMA
    other = max(lines - 1, 1)
    return pl.pallas_call(
        kernel,
        out_shape=pltpu.VMEM((token_count, width), bf16),
        in_specs=[hbm] * 16,
        out_specs=vmem,
        scratch_shapes=[
            pltpu.VMEM(row_table.shape, f32),
            pltpu.VMEM(column_table.shape, f32),
            pltpu.VMEM((1, HEAD_DIM), f32),
            pltpu.VMEM((1, HEAD_DIM), f32),
            pltpu.VMEM((1, width), f32),
            pltpu.VMEM((TOPK, token_count), jnp.int32),
            pltpu.VMEM((TOPK, token_count), f32),
            pltpu.VMEM((1, width), f32),
            dma((8,)),
            pltpu.VMEM(queries.shape, bf16),
            pltpu.VMEM(key_rows.shape, bf16),
            pltpu.VMEM(value_rows.shape, bf16),
            pltpu.VMEM(residual.shape, bf16),
            pltpu.VMEM(out_weight.shape, bf16),
            pltpu.VMEM(gate_weight.shape[1:], bf16),
            pltpu.VMEM(up_weight.shape[1:], bf16),
            pltpu.VMEM(down_weight.shape[1:], bf16),
            dma((8,)),
            dma((8,)),
            pltpu.VMEM((experts, token_count, key_heads * pair_width), bf16),
            dma((2, ring_half, pieces)),
            pltpu.VMEM((key_heads, query_rows, pair_width), bf16),
            pltpu.VMEM((key_heads, HEAD_DIM, query_rows), f32),
            pltpu.VMEM((key_heads, 1, query_rows), f32),
            pltpu.VMEM((key_heads, 1, query_rows), f32),
            pltpu.VMEM((token_count, key_heads * pair_width), bf16),
            pltpu.VMEM((lines, token_count, width), bf16),
            pltpu.VMEM((lines, token_count, width), bf16),
            pltpu.VMEM((other, token_count, width), bf16),
            pltpu.VMEM((other, token_count, width), bf16),
            dma((lines,)),
            dma((other,)),
            pltpu.VMEM((2, 8, token_count), f32),
            pltpu.VMEM((2, shards - 1, 8, token_count), f32),
            dma((2,)),
            pltpu.VMEM((token_count, token_count), bf16),
            pltpu.VMEM((token_count, token_count), bf16),
            pltpu.VMEM((experts, 8, token_count), f32),
            pltpu.VMEM((experts, 8, token_count), f32),
            dma,
            pltpu.VMEM((row_total, 128), f32),
            pltpu.VMEM((token_count, width), bf16),
            pltpu.VMEM((row_total, hidden_units), bf16),
            dma((splits, max(groups - 1, 1))),
            dma((EXP_GROUP, lines)),
            dma((len(sets),)),
            dma((len(sets),)),
            dma((len(sets), lines)),
            dma((len(sets),)),
            pltpu.VMEM((splits, far_rows, width), bf16),
            pltpu.VMEM((max(groups - 1, 1), capacity, width), bf16),
            dma((splits, max(groups - 1, 1))),
        ]
        + [pltpu.VMEM((shards, rows, width), bf16) for rows in set_rows]
        + [pltpu.VMEM((lines, rows, width), bf16) for rows in set_rows] * 3
        + [pltpu.VMEM((EXP_GROUP, lines, rows, width), bf16) for rows in member_rows]
        + [pltpu.VMEM((rows, width), f32) for rows in set_rows]
        + [pltpu.VMEM((lines, rows, width), f32) for rows in set_rows],
        compiler_params=pltpu.CompilerParams(
            collective_id=0, has_side_effects=True, vmem_limit_bytes=48 << 20
        ),
    )(
        *(
            pltpu.with_memory_space_constraint(array, pltpu.HBM)
            for array in (
                jnp.asarray(row_table), jnp.asarray(column_table), query_gain.reshape(1, -1),
                key_gain.reshape(1, -1), norm_gain.reshape(1, -1), expert_ids.T, route_weights.T,
                final_gain.reshape(1, -1), queries, key_rows, value_rows, residual, out_weight,
                gate_weight, up_weight, down_weight,
            )
        )
    )


def per_device(
    queries,
    projected_key_rows,
    projected_value_rows,
    query_gain,
    key_norm_gain,
    residual,
    out_weight,
    norm_gain,
    expert_ids,
    route_weights,
    gate_weight,
    up_weight,
    down_weight,
    final_gain,
):
    token_total = queries.shape[0] * lax.axis_size("sp")
    row_table, column_table = rotary_tables(-(-token_total // GRID_W))
    return layer(
        queries,
        projected_key_rows,
        projected_value_rows,
        row_table,
        column_table,
        query_gain,
        key_norm_gain,
        out_weight,
        residual,
        norm_gain,
        expert_ids,
        route_weights,
        gate_weight,
        up_weight,
        down_weight,
        final_gain,
        lax.axis_size("sp"),
        lax.axis_size("tp"),
    )


def solution(mesh):
    in_specs = (
        P("sp", "tp"),
        P("sp", "tp"),
        P("sp", "tp"),
        P(),
        P(),
        P("sp", "tp"),
        P("tp", None),
        P("tp"),
        P("sp", None),
        P("sp", None),
        P("sp", None, "tp"),
        P("sp", None, "tp"),
        P("sp", "tp", None),
        P("tp"),
    )
    out_specs = P("sp", "tp")
    return jax.shard_map(
        per_device, mesh=mesh, in_specs=in_specs, out_specs=out_specs, check_vma=False
    )
```
